512 devices in a mesh: sp: 32 (over z, x), tp: 16 (over y, core).
Axes of the slice: x: 4, y: 8, z: 8, core: 2. Of those that a mesh axis runs over, the one named last changes fastest.
Arguments:
- queries: bfloat16 [512, 4096], P('tp', 'sp'), may hold values from -6 to 6
- input_key_matrix: bfloat16 [512, 4096], P('tp', 'sp'), may hold values from -6 to 6
- input_value_matrix: bfloat16 [1024, 4096], P('tp', 'sp'), may hold values from -6 to 6
- decay_preactivation: bfloat16 [512, 4096], P('tp', 'sp'), may hold values from -6 to 6
- extra_log_decay: float32 [512, 4096], P('tp', 'sp'), may hold values from -1 to 0, as said below
- channel_decay_speed: float32 [512], P('tp'), may hold values from 0 to 1, as said below
- output_weight_matrix: bfloat16 [2048, 1024], P(None, 'tp'), may hold values from -0.1875 to 0.1875
- stored_expert_rows: bfloat16 [4096, 2048], P('sp', 'tp'), may hold values from -6 to 6
- chosen_expert_index: int32 [4096, 2], P('sp'), may hold values from 0 to 31, all different within a row; in each aligned block of 128 rows (0 to 127, 128 to 255, ...) at most 12 rows name the same one
- expert_combine_weight: float32 [4096, 2], P('sp'), may hold values from 0.2 to 1
- cotangent: bfloat16 [4096, 2048], P('sp', 'tp'), may hold values from -6 to 6
- expert_gate_weight: bfloat16 [32, 2048, 2048], P('sp', None, 'tp'), may hold values from -0.125 to 0.125
- expert_up_weight: bfloat16 [32, 2048, 2048], P('sp', None, 'tp'), may hold values from -0.125 to 0.125
- expert_down_weight: bfloat16 [32, 2048, 2048], P('sp', 'tp'), may hold values from -0.125 to 0.125
Outputs:
- grad_queries: float32 [512, 4096], P('tp', 'sp')
- grad_keys: float32 [512, 4096], P('tp', 'sp')
- grad_values: float32 [1024, 4096], P('tp', 'sp')
- grad_logit: float32 [512, 4096], P('tp', 'sp')
- grad_out_proj: float32 [2048, 1024], P('sp', 'tp')
- grad_gate: bfloat16 [32, 2048, 2048], P('sp', None, 'tp')
- grad_up: bfloat16 [32, 2048, 2048], P('sp', None, 'tp')
- grad_down: bfloat16 [32, 2048, 2048], P('sp', 'tp')
The draws below stay inside these ranges and needn't reach their ends.
Inputs may be any that keep to these rules, and one draw needn't show every extreme that they name: `chosen_expert_index`: each position names two different experts; in the rows of one device no expert is named more than 12 times. `channel_decay_speed`: positive. `extra_log_decay`: zero or negative.
All inputs are finite; a program needn't handle non-finite values.
Results may differ from the reference program's by a relative error of at most 0.023.
Values may be sent and summed in bfloat16 or wider, within the bound.
No kernel may reach another device: no remote copies, remote signals or barrier semaphores. Data moves between devices by JAX's collectives and lax.ppermute only.
A program may use at most 64 MiB of HBM per device.

```python
import math
import jax
import jax.numpy as jnp
import numpy as np
from jax import lax

D = 2048
HEADS = 16
KEY_DIM = 32
VAL_DIM = 64
EXPERT_UNITS = 2048
TOK_DEV = 128
SPAN = 64
SEQUENCE_LENGTH = 4096
EXPERTS = 32
CAP = 12
KEY_CHANNELS = 512
VCH = 1024
N_SP = 32
N_TP = 16


def draw_channel_decay_speed(key, part):
    key_pick, key_spread = jax.random.split(jax.random.fold_in(key, 11))
    slow_share = 0.5
    is_slow = jax.random.uniform(key_pick, (KEY_CHANNELS,), jnp.float32) < slow_share
    spread = jax.random.uniform(key_spread, (KEY_CHANNELS,), jnp.float32)
    slow_rate = jnp.exp(jnp.log(0.2) + spread * (jnp.log(1.0) - jnp.log(0.2))) / SEQUENCE_LENGTH
    fast_rate = jnp.exp(jnp.log(0.02) + spread * (jnp.log(0.06) - jnp.log(0.02)))
    return jnp.where(is_slow, slow_rate, fast_rate).astype(jnp.float32)


def draw_decay_preactivation(key, part):
    key_noise, key_level = jax.random.split(jax.random.fold_in(key, 23))
    noise = jnp.clip(jax.random.normal(key_noise, (KEY_CHANNELS, SEQUENCE_LENGTH), jnp.float32), -4.0, 4.0)
    level = jax.random.uniform(key_level, (SEQUENCE_LENGTH // TOK_DEV,), jnp.float32, -1.5, 1.5)
    return (noise + jnp.repeat(level, TOK_DEV)[None, :]).astype(jnp.bfloat16)


def draw_extra_log_decay(key, part):
    key_channel_index, key_channel_count = jax.random.split(jax.random.fold_in(key, 37))
    jump_location = jax.random.randint(key_channel_index, (KEY_CHANNELS, 3), 0, SEQUENCE_LENGTH)
    jump_magnitude = jax.random.uniform(key_channel_count, (KEY_CHANNELS, 3), jnp.float32, jnp.log(0.6), jnp.log(0.8))
    jump_hit_mask = jnp.arange(SEQUENCE_LENGTH, dtype=jnp.int32)[None, None, :] == jump_location[:, :, None]
    return jnp.sum(jnp.where(jump_hit_mask, jump_magnitude[:, :, None], 0.0), axis=1).astype(jnp.float32)


def raised(values, key, source, target, shards_of, factor):
    def block_of(axis_at):
        return (jnp.arange(values.shape[axis_at]) // (values.shape[axis_at] // shards_of)).reshape((-1,) + (1,) * (values.ndim - 1 - axis_at))

    one_side = jax.random.permutation(key, shards_of)[block_of(target)]
    second = (block_of(target) + shards_of // 2) % shards_of
    return jnp.where((block_of(source) == one_side) | (block_of(source) == second), factor * values, values)


def levels(key, dims, cuts, smallest, top_value):
    level = 1.0
    for axis_at, shards_of in cuts:
        draws = jax.random.uniform(jax.random.fold_in(jax.random.fold_in(key, 6), axis_at), (shards_of,), jnp.float32, smallest / len(cuts), top_value / len(cuts))
        level = level * jnp.repeat(jnp.exp(draws), dims[axis_at] // shards_of).reshape((-1,) + (1,) * (len(dims) - 1 - axis_at))
    return level


def assign_block(key, own, number, rows, number_of, top, most, slope):
    order = jax.random.permutation(key, number_of)
    crowded, ordinary = load_shares(number_of, rows * top, most, slope, True), load_shares(number_of, rows * top, most, slope, False)
    places = jnp.arange(number_of)

    def named(sizes, offset_by):
        used = int((sizes > 0).sum())
        fixed = max(1, used // 4)
        moved = fixed + (places - fixed + offset_by * (used - fixed)) % max(1, number_of - fixed)
        return jnp.zeros((number_of,), jnp.int32).at[order[jnp.where(places < fixed, places, moved)]].set(jnp.asarray(sizes, jnp.int32))

    sizes = jnp.where(number % 4 == 0, named(crowded, number // 4), named(ordinary, number - number // 4 - 1))
    mixed = jax.random.permutation(jax.random.fold_in(own, 3), number_of)
    donor, receiver = mixed[0:number_of // 2 * 2:2], mixed[1:number_of // 2 * 2:2]
    margin = jnp.minimum(sizes[donor] - 1, most - sizes[receiver]) // 2
    margin = jnp.where((donor == order[0]) | (receiver == order[0]) | (sizes[receiver] == 0), 0, jnp.maximum(margin, 0))
    moved = jax.random.randint(jax.random.fold_in(own, 4), (number_of // 2,), 0, 1 << 20) % (margin + 1)
    sizes = sizes.at[donor].add(-moved).at[receiver].add(moved)
    items = jnp.searchsorted(jnp.cumsum(sizes), jnp.arange(rows * top), side="right").astype(jnp.int32)
    table = items.reshape(top, rows).T
    table = table[jax.random.permutation(jax.random.fold_in(own, 1), rows)]
    offset_by = jax.random.randint(jax.random.fold_in(own, 2), (rows, 1), 0, top)
    return jnp.take_along_axis(table, (jnp.arange(top)[None, :] + offset_by) % top, axis=1)


def load_shares(count, total, bound, lean, full):
    portions = [(1 << 20) // math.isqrt(rank ** lean) + 1 for rank in range(1, count + 1)]
    largest = bound if full else min(bound, max(-(-total // count), total * portions[0] // sum(portions)))
    least = 1 if total - largest >= count - 1 else 0
    holding, rest = [largest] + [least] * (count - 1), total - largest - least * (count - 1)
    while rest > 0:
        free = [i for i in range(1, count) if holding[i] < largest] or [i for i in range(1, count) if holding[i] < bound]
        mass, left = sum([portions[i] for i in free]), rest
        for i in free:
            extra = min(bound - holding[i], max(1, left * portions[i] // mass), rest)
            holding[i] = holding[i] + extra
            rest = rest - extra
    return np.array(holding)


def normal_values(rng, shape, deviation, limit, shards=(), kind=jnp.bfloat16):
    factor_of = levels(rng, shape, shards, -0.22, 0.18) if shards else 1.0
    drawn = jax.random.normal(rng, shape, jnp.float32) * deviation * factor_of
    return jnp.minimum(jnp.maximum(drawn, -limit), limit).astype(kind)


def bell_draw_with(rng, extent, width, bound, cuts, heavy, kind=jnp.bfloat16):
    entries = width * jax.random.normal(rng, extent, jnp.float32)
    if cuts:
        entries = entries * levels(rng, extent, cuts, -0.22, 0.18)
    return jnp.clip(raised(entries, jax.random.fold_in(rng, 3), *heavy), -bound, bound).astype(kind)


def setup_inputs(seed: int = 0) -> dict:
    keys = jax.random.split(jax.random.key(seed), 15)
    queries = normal_values(keys[0], (KEY_CHANNELS, SEQUENCE_LENGTH), 1.0, 6.0, ((0, 16), (1, 32)))
    input_key_matrix = normal_values(keys[1], (KEY_CHANNELS, SEQUENCE_LENGTH), 1.0, 6.0, ((0, 16), (1, 32)))
    input_value_matrix = normal_values(keys[2], (VCH, SEQUENCE_LENGTH), 1.0, 6.0, ((0, 16), (1, 32)))
    decay_preactivation = draw_decay_preactivation(jax.random.fold_in(keys[14], 71), 0)
    extra_log_decay = draw_extra_log_decay(jax.random.fold_in(keys[14], 71), 0)
    channel_decay_speed = draw_channel_decay_speed(jax.random.fold_in(keys[14], 71), 0)
    output_weight_matrix = normal_values(keys[6], (D, VCH), VCH ** -0.5, 0.1875, ((1, 16),))
    stored_expert_rows = normal_values(keys[7], (SEQUENCE_LENGTH, D), 1.0, 6.0, ((0, 32), (1, 16)))
    chosen_expert_index_keys = jax.random.split(jax.random.fold_in(keys[8], 1), SEQUENCE_LENGTH // TOK_DEV)
    chosen_expert_index_turns = jax.random.permutation(jax.random.fold_in(keys[8], 3), SEQUENCE_LENGTH // TOK_DEV)
    chosen_expert_index = jax.vmap(lambda own, number: assign_block(jax.random.fold_in(keys[8], 2), own, number, TOK_DEV, EXPERTS, 2, CAP, 1))(chosen_expert_index_keys, chosen_expert_index_turns).reshape((SEQUENCE_LENGTH, 2))
    expert_combine_weight = jnp.clip(0.2 + 0.8 * jax.random.uniform(keys[9], (SEQUENCE_LENGTH, 2), jnp.float32) ** levels(keys[9], (SEQUENCE_LENGTH, 2), ((0, 32),), -0.2, 0.2), 0.2, 1.0)
    cotangent = bell_draw_with(keys[10], (SEQUENCE_LENGTH, D), 1.0, 6.0, ((0, 32), (1, 16)), (0, 1, 32, 2.75))
    expert_gate_weight = normal_values(keys[11], (EXPERTS, D, EXPERT_UNITS), D ** -0.5, 0.125, ((0, 32), (2, 16)))
    expert_up_weight = normal_values(keys[12], (EXPERTS, D, EXPERT_UNITS), D ** -0.5, 0.125, ((0, 32), (2, 16)))
    expert_down_weight = normal_values(keys[13], (EXPERTS, EXPERT_UNITS, D), EXPERT_UNITS ** -0.5, 0.125, ((0, 32), (1, 16)))
    return dict(queries=queries, input_key_matrix=input_key_matrix, input_value_matrix=input_value_matrix, decay_preactivation=decay_preactivation, extra_log_decay=extra_log_decay, channel_decay_speed=channel_decay_speed, output_weight_matrix=output_weight_matrix, stored_expert_rows=stored_expert_rows, chosen_expert_index=chosen_expert_index, expert_combine_weight=expert_combine_weight, cotangent=cotangent, expert_gate_weight=expert_gate_weight, expert_up_weight=expert_up_weight, expert_down_weight=expert_down_weight)


def combine_steps(state, pair):
    factor, addend = pair
    return (factor * state + addend, state)

def head_forward(scaled, key_feats, val_feats, decay_logarithm):
    blocks = decay_logarithm.shape[1] // SPAN

    def split_blocks(array):
        return array.reshape(array.shape[0], blocks, SPAN).transpose(1, 0, 2)
    block_q = split_blocks(scaled)
    block_k = split_blocks(key_feats)
    block_v = split_blocks(val_feats)
    cumulative = jnp.cumsum(split_blocks(decay_logarithm), axis=2)
    total_log = cumulative[:, :, -1:]
    lower_mask = lax.broadcasted_iota(jnp.int32, (SPAN, SPAN), 0) >= lax.broadcasted_iota(jnp.int32, (SPAN, SPAN), 1)
    log_gap = cumulative[:, :, :, None] - cumulative[:, :, None, :]
    weight = jnp.exp(jnp.where(lower_mask, log_gap, -log_gap))
    scores = jnp.einsum('bct,bcs,bcts->bts', block_q, block_k, weight)
    inner_part = jnp.einsum('bts,bvs->bvt', scores, block_v)
    factor = jnp.exp(total_log)
    fwd_sum = jnp.einsum('bcs,bvs->bcv', block_k * jnp.exp(total_log - cumulative), block_v)
    bwd_sum = jnp.einsum('bcs,bvs->bcv', block_k * jnp.exp(cumulative), block_v)
    start_state = jnp.zeros((key_feats.shape[0], val_feats.shape[0]), jnp.float32)
    _, fwd_in = lax.scan(combine_steps, start_state, (factor, fwd_sum))
    _, bwd_in = lax.scan(combine_steps, start_state, (factor, bwd_sum), reverse=True)
    carried = jnp.einsum('bct,bcv->bvt', block_q * jnp.exp(cumulative), fwd_in)
    carried = carried + jnp.einsum('bct,bcv->bvt', block_q * jnp.exp(total_log - cumulative), bwd_in)
    output = inner_part + carried
    return output.transpose(1, 0, 2).reshape(val_feats.shape[0], -1)

def head_mix(query_f, key_feats, val_feats, decay_logarithm):
    return head_forward(query_f * KEY_DIM ** (-0.5), key_feats, val_feats, decay_logarithm)

def head_apply(packed):
    return head_mix(packed[0], packed[1], packed[2], packed[3])

def head_grads(packed):
    _, pull_back = jax.vjp(head_mix, packed[0], packed[1], packed[2], packed[3])
    return pull_back(packed[4])

def expert_grads(packed):
    slot_table, gate_local, up_local, down_local, inputs_pad, grads_pad = packed
    rows_x = inputs_pad[slot_table // 2]
    rows_dy = grads_pad[slot_table]
    gate_pre = jnp.dot(rows_x, gate_local, preferred_element_type=jnp.float32)
    up_pre = jnp.dot(rows_x, up_local, preferred_element_type=jnp.float32)
    gate_sig = jax.nn.sigmoid(gate_pre)
    gate_act = gate_pre * gate_sig
    hidden = (gate_act * up_pre).astype(jnp.bfloat16)
    grad_down = jnp.dot(hidden.T, rows_dy, preferred_element_type=jnp.float32).astype(jnp.bfloat16)
    grad_hidden = jnp.dot(rows_dy, down_local.T, preferred_element_type=jnp.float32)
    grad_gate_pre = (grad_hidden * up_pre * gate_sig * (1.0 + gate_pre * (1.0 - gate_sig))).astype(jnp.bfloat16)
    grad_up_pre = (grad_hidden * gate_act).astype(jnp.bfloat16)
    grad_gate = jnp.dot(rows_x.T, grad_gate_pre, preferred_element_type=jnp.float32).astype(jnp.bfloat16)
    grad_up = jnp.dot(rows_x.T, grad_up_pre, preferred_element_type=jnp.float32).astype(jnp.bfloat16)
    row_count = rows_x.shape[0]
    group_width = EXPERT_UNITS // N_TP
    gate_groups = grad_gate_pre.astype(jnp.float32).reshape(row_count, N_TP, group_width)
    up_groups = grad_up_pre.astype(jnp.float32).reshape(row_count, N_TP, group_width)
    gate_weights = gate_local.astype(jnp.float32).reshape(D, N_TP, group_width)
    up_weights = up_local.astype(jnp.float32).reshape(D, N_TP, group_width)
    partial_value = jnp.einsum('rjh,djh->jrd', gate_groups, gate_weights) + jnp.einsum('rjh,djh->jrd', up_groups, up_weights)
    partial_value = partial_value.astype(jnp.bfloat16).astype(jnp.float32)
    slot_grads = lax.optimization_barrier(jnp.sum(partial_value, axis=0)).astype(jnp.bfloat16)
    return (grad_gate, grad_up, grad_down, slot_grads)

def reference(queries, input_key_matrix, input_value_matrix, decay_preactivation, extra_log_decay, channel_decay_speed, output_weight_matrix, stored_expert_rows, chosen_expert_index, expert_combine_weight, cotangent, expert_gate_weight, expert_up_weight, expert_down_weight):
    preactivation_single = decay_preactivation.astype(jnp.float32)
    decay_logarithm = channel_decay_speed[:, None] * jax.nn.log_sigmoid(preactivation_single) + extra_log_decay
    query_heads = queries.astype(jnp.float32).reshape(HEADS, KEY_DIM, SEQUENCE_LENGTH)
    key_heads = input_key_matrix.astype(jnp.float32).reshape(HEADS, KEY_DIM, SEQUENCE_LENGTH)
    value_heads = input_value_matrix.astype(jnp.float32).reshape(HEADS, VAL_DIM, SEQUENCE_LENGTH)
    decay_heads = decay_logarithm.reshape(HEADS, KEY_DIM, SEQUENCE_LENGTH)
    mixed = lax.map(head_apply, (query_heads, key_heads, value_heads, decay_heads))
    inv_rms = lax.rsqrt(lax.optimization_barrier(jnp.mean(mixed * mixed, axis=1, keepdims=True)) + 1e-06)
    normed = mixed * inv_rms
    mix_rows = normed.astype(jnp.bfloat16).reshape(VCH, SEQUENCE_LENGTH)
    block_ids = chosen_expert_index.reshape(N_SP, 2 * TOK_DEV)
    onehot = (block_ids[:, :, None] == jnp.arange(EXPERTS, dtype=jnp.int32)[None, None, :]).astype(jnp.int32)
    slot_rank = lax.optimization_barrier(jnp.sum((jnp.cumsum(onehot, axis=1) - onehot) * onehot, axis=2))
    source = jnp.arange(N_SP, dtype=jnp.int32)[:, None]
    flat_slot = (block_ids * (N_SP * CAP) + source * CAP + slot_rank).reshape(-1)
    slot_table = jnp.full((EXPERTS * N_SP * CAP,), 2 * SEQUENCE_LENGTH, jnp.int32)
    slot_table = slot_table.at[flat_slot].set(jnp.arange(2 * SEQUENCE_LENGTH, dtype=jnp.int32))
    zero_row = jnp.zeros((1, D), jnp.bfloat16)
    inputs_pad = jnp.concatenate([stored_expert_rows, zero_row], axis=0)
    weighted = (expert_combine_weight.reshape(-1, 1) * jnp.repeat(cotangent, 2, axis=0).astype(jnp.float32)).astype(jnp.bfloat16)
    grads_pad = jnp.concatenate([weighted, zero_row], axis=0)

    def per_expert(packed):
        return expert_grads((packed[0], packed[1], packed[2], packed[3], inputs_pad, grads_pad))
    grad_gate, grad_up, grad_down, slot_grads = lax.map(per_expert, (slot_table.reshape(EXPERTS, N_SP * CAP), expert_gate_weight, expert_up_weight, expert_down_weight))
    picked = slot_grads.reshape(EXPERTS * N_SP * CAP, D)[flat_slot].astype(jnp.float32).reshape(SEQUENCE_LENGTH, 2, D)
    token_grads = (cotangent.astype(jnp.float32) + picked[:, 0] + picked[:, 1]).astype(jnp.bfloat16)
    grad_out_proj = jnp.dot(token_grads.T, mix_rows.T, preferred_element_type=jnp.float32)
    grad_normed = jnp.dot(output_weight_matrix.T, token_grads.T, preferred_element_type=jnp.float32).reshape(HEADS, VAL_DIM, SEQUENCE_LENGTH)
    grad_mixed = inv_rms * (grad_normed - normed * lax.optimization_barrier(jnp.mean(grad_normed * normed, axis=1, keepdims=True)))
    grad_q, grad_k, grad_v, grad_decay = lax.map(head_grads, (query_heads, key_heads, value_heads, decay_heads, grad_mixed))
    grad_logit = grad_decay.reshape(KEY_CHANNELS, SEQUENCE_LENGTH) * channel_decay_speed[:, None] * jax.nn.sigmoid(-preactivation_single)
    return (grad_q.reshape(KEY_CHANNELS, SEQUENCE_LENGTH), grad_k.reshape(KEY_CHANNELS, SEQUENCE_LENGTH), grad_v.reshape(VCH, SEQUENCE_LENGTH), grad_logit, grad_out_proj, grad_gate, grad_up, grad_down)
```

```python
import jax
import jax.numpy as jnp
from jax import lax
from jax.experimental import pallas as pl
from jax.experimental.pallas import tpu as pltpu
from jax.sharding import Mesh
from jax.sharding import PartitionSpec as P

KEY_DIM = 32
VAL_DIM = 64
TOK = 128
PEERS = 32
CAP = 12
PAD = 16
RING = 8
SLOTS = PEERS * PAD
ROWS = PEERS * CAP
WIDTH = 128
MODEL = 2048

F32 = jnp.float32
BF16 = jnp.bfloat16
EXACT = lax.Precision.HIGHEST


def dot(a, b, da, db, precision=None):
    return lax.dot_general(
        a, b, (((da,), (db,)), ((), ())), preferred_element_type=F32, precision=precision
    )


def iota(shape, dim):
    return lax.broadcasted_iota(jnp.int32, shape, dim)


def ones_where(mask, dtype=BF16):
    return jnp.where(mask, 1.0, 0.0).astype(dtype)


def split_two(value):
    high = value.astype(BF16).astype(F32)
    return high, (value - high).astype(BF16).astype(F32)


def split_three(value):
    high, rest = split_two(value)
    return high, rest, (value - high - rest).astype(BF16).astype(F32)


def compact_rows(shape, compact_dim):
    row = iota(shape, compact_dim)
    peer = (row * 5462) >> 16
    return peer * PAD + (row - peer * CAP) == iota(shape, 1 - compact_dim)


def row_of_peer(place):
    return iota((PEERS, SLOTS), 1) == iota((PEERS, SLOTS), 0) * PAD + place


def dispatch_kernel(
    ids_ref, share_ref, x_ref, cot_ref, key_ref, val_ref, pre_ref, extra_ref, speed_ref,
    send_ref, pick_ref, cum_ref,
):
    ids = ids_ref[...]
    expert = iota((TOK, PEERS), 1)
    named = [ones_where(ids[:, k : k + 1] == expert) for k in range(2)]
    row, col = iota((TOK, TOK), 0), iota((TOK, TOK), 1)
    earlier, same = ones_where(row < col), ones_where(row == col)
    rank = dot(named[0] + named[1], earlier, 0, 0)
    place = iota((PEERS, PAD, TOK), 1).astype(F32)
    cot = cot_ref[...].astype(F32)
    picks, grads = [], None
    for k in range(2):
        mine = dot(named[k], same, 0, 0)
        at = jnp.where(mine > 0.5, rank, -1.0)
        pick = jnp.where(at[:, None, :] == place, 1.0, 0.0).reshape(SLOTS, TOK).astype(BF16)
        weighted = (share_ref[:, k : k + 1] * cot).astype(BF16)
        part = dot(pick, weighted, 1, 0)
        grads = part if grads is None else grads + part
        picks.append(pick)
    pick = picks[0] + picks[1]
    pick_ref[...] = pick
    rows = jnp.concatenate([dot(pick, x_ref[...], 1, 0), grads], axis=1)

    pre = pre_ref[...].astype(F32)
    log_sig = jnp.minimum(pre, 0.0) - jnp.log1p(jnp.exp(-jnp.abs(pre)))
    diagonal = iota((KEY_DIM, KEY_DIM), 0) == iota((KEY_DIM, KEY_DIM), 1)
    speed = jnp.sum(jnp.where(diagonal, speed_ref[...], 0.0), axis=1, keepdims=True)
    decay = speed * log_sig + extra_ref[...]
    cum = dot(decay, ones_where(row <= col, F32), 1, 0, EXACT)
    cum_ref[...] = cum
    total = cum[:, TOK - 1 : TOK]
    keys, vals = key_ref[...].astype(F32), val_ref[...].astype(F32)
    sums = jnp.concatenate(
        [
            dot(keys * jnp.exp(total - cum), vals, 1, 1, EXACT),
            dot(keys * jnp.exp(cum), vals, 1, 1, EXACT),
        ],
        axis=1,
    )
    state = jnp.concatenate(split_two(sums), axis=1)
    lane = iota((KEY_DIM, 2 * WIDTH), 1)
    logs = jnp.zeros((KEY_DIM, 2 * WIDTH), F32)
    for k, part in enumerate(split_three(total)):
        logs = jnp.where(lane == k, part, logs)
    place = iota((PEERS, PAD, 2 * WIDTH), 1)
    block = rows.reshape(PEERS, PAD, 2 * WIDTH)
    block = jnp.where(place == CAP, state[:, None, :], block)
    block = jnp.where(place == CAP + 1, logs[:, None, :], block)
    send_ref[...] = block.astype(BF16)


def arrival_kernel(got_ref, copies_ref, back_ref):
    got = got_ref[...].reshape(SLOTS, 2 * WIDTH)
    rows = dot(ones_where(compact_rows((ROWS, SLOTS), 0)), got, 1, 0).astype(BF16)
    for k in range(RING):
        copies_ref[k] = rows
    both = dot(ones_where(row_of_peer(CAP)), got, 1, 0)
    state = both[:, :WIDTH] + both[:, WIDTH:]
    logs = dot(ones_where(row_of_peer(CAP + 1)), got, 1, 0)
    log = jnp.sum(logs, axis=1, keepdims=True)
    a, b = iota((PEERS, PEERS), 0), iota((PEERS, PEERS), 1)
    gap_fwd = dot(ones_where(b < a, F32), jnp.where(a > b, log, 0.0), 1, 0, EXACT)
    gap_bwd = dot(ones_where(b > a, F32), jnp.where(a < b, log, 0.0), 1, 0, EXACT)
    fwd = dot(jnp.where(b < a, jnp.exp(gap_fwd), 0.0), state, 1, 0, EXACT)
    bwd = dot(jnp.where(b > a, jnp.exp(gap_bwd), 0.0), state, 1, 0, EXACT)
    lane = iota((PEERS, WIDTH), 1)
    high, low = split_two(jnp.where(lane < VAL_DIM, fwd, bwd))
    peer = iota((PEERS, WIDTH), 0)
    spread = jnp.zeros((PEERS, WIDTH), F32)
    for k, part in enumerate(split_three(log)):
        spread = jnp.where(lane == peer + k * PEERS, part, spread)
    all_logs = jnp.sum(spread, axis=0, keepdims=True)
    place = iota((PEERS, PAD, WIDTH), 1)
    block = jnp.where(place == CAP, high[:, None, :], 0.0)
    block = jnp.where(place == CAP + 1, low[:, None, :], block)
    block = jnp.where(place == CAP + 2, all_logs[:, None, :], block)
    back_ref[...] = block.astype(BF16)


def expert_kernel(
    core_ref, own_ref, other_ref, gate_ref, up_ref, down_ref,
    x_ref, y_ref, grads_ref, hidden_ref,
):
    core = core_ref[0]
    for mine in range(2):

        @pl.when(core == mine)
        def _():
            for side, ref in ((mine, own_ref), (1 - mine, other_ref)):
                for k in range(RING):
                    at = slice((2 * k + side) * WIDTH, (2 * k + side + 1) * WIDTH)
                    x_ref[:, at] = ref[k, :, :WIDTH]
                    y_ref[:, at] = ref[k, :, WIDTH:]

    x, y = x_ref[...], y_ref[...]
    gate_pre = dot(x, gate_ref[...], 1, 0)
    up_pre = dot(x, up_ref[...], 1, 0)
    grad_hidden = dot(y, down_ref[...], 1, 1)
    gate_sig = jax.nn.sigmoid(gate_pre)
    gate_act = gate_pre * gate_sig
    hidden_ref[...] = (gate_act * up_pre).astype(BF16)
    grads_ref[:, :WIDTH] = (
        grad_hidden * up_pre * gate_sig * (1.0 + gate_pre * (1.0 - gate_sig))
    ).astype(BF16)
    grads_ref[:, WIDTH:] = (grad_hidden * gate_act).astype(BF16)


def partial_kernel(core_ref, grads_ref, gate_ref, up_ref, swapped_ref, out_ref):
    core = core_ref[0]
    both = jnp.concatenate([grads_ref[core], grads_ref[1 - core]], axis=1)
    for k in range(RING):
        at = 2 * k + core
        weights = jnp.concatenate(
            [gate_ref[at], up_ref[at], swapped_ref[0, k], swapped_ref[1, k]], axis=1
        )
        out_ref[k] = dot(both, weights, 1, 1).astype(BF16)


def return_kernel(parts_ref, back_ref, send_ref):
    total = parts_ref[0].astype(F32)
    for k in range(1, RING):
        total = total + parts_ref[k].astype(F32)
    rows = dot(ones_where(compact_rows((SLOTS, ROWS), 1)), total.astype(BF16), 1, 0)
    rows = rows.astype(BF16).reshape(PEERS, PAD, WIDTH)
    send_ref[...] = rows + back_ref[...]


def token_kernel(got_ref, pick_ref, cot_ref, copies_ref):
    got = got_ref[...].reshape(SLOTS, WIDTH)
    rows = (cot_ref[...].astype(F32) + dot(pick_ref[...], got, 0, 0)).astype(BF16)
    for k in range(RING):
        copies_ref[k] = rows


def state_kernel(place_ref, got_ref, state_ref, reach_ref):
    got = got_ref[...].reshape(SLOTS, WIDTH)
    state_ref[...] = dot(ones_where(row_of_peer(CAP) | row_of_peer(CAP + 1)), got, 1, 0)
    spread = dot(ones_where(row_of_peer(CAP + 2)), got, 1, 0).astype(BF16)
    lane, peer = iota((WIDTH, PEERS), 0), iota((WIDTH, PEERS), 1)
    fold = (lane == peer) | (lane == peer + PEERS) | (lane == peer + 2 * PEERS)
    logs = dot(spread, ones_where(fold), 1, 0)
    here = place_ref[0]
    a, b = iota((PEERS, PEERS), 0), iota((PEERS, PEERS), 1)
    later = dot(jnp.where(b > here, logs, 0.0), ones_where(a < b, F32), 1, 0, EXACT)
    before = dot(jnp.where(b < here, logs, 0.0), ones_where(a > b, F32), 1, 0, EXACT)
    later = jnp.where(b > here, jnp.exp(later), 0.0)
    before = jnp.where(b < here, jnp.exp(before), 0.0)
    lane = iota((KEY_DIM, WIDTH), 1)
    for k in range(PEERS):
        reach_ref[k] = jnp.where(lane < VAL_DIM, later[:, k : k + 1], before[:, k : k + 1])


def source_kernel(
    rows_ref, weight_ref, normed_ref, inv_ref, mix_ref, query_fwd_ref, query_bwd_ref,
    send_ref, grad_ref,
):
    rows = jnp.concatenate([rows_ref[c, k] for k in range(RING) for c in range(2)], axis=1)
    grad = dot(rows, weight_ref[...], 1, 0)
    normed = normed_ref[...]
    mean = jnp.mean(grad * normed, axis=1, keepdims=True)
    grad = inv_ref[...] * (grad - normed * mean)
    grad_ref[...] = grad
    state = jnp.concatenate(
        [
            dot(query_fwd_ref[...], grad, 1, 0, EXACT),
            dot(query_bwd_ref[...], grad, 1, 0, EXACT),
        ],
        axis=1,
    ).astype(BF16)
    lane = iota((KEY_DIM, WIDTH), 1)
    for k in range(2 * RING):
        part = dot(rows[:, k * WIDTH : (k + 1) * WIDTH], mix_ref[...], 0, 0)
        for half in range(2):
            at = half * VAL_DIM
            both = jnp.where(lane < VAL_DIM, part[at : at + 32], part[at + 32 : at + 64])
            send_ref[2 * k + half, :KEY_DIM] = both.astype(BF16)
            send_ref[2 * k + half, KEY_DIM:] = state


def final_kernel(
    got_ref, reach_ref, state_ref, cum_ref, key_ref, val_ref, pre_ref, speed_ref,
    keys_mix_ref, vals_mix_ref, decay_mix_ref,
    proj_ref, keys_ref, vals_ref, logit_ref,
):
    proj = got_ref[0, :KEY_DIM].astype(F32)
    flow = got_ref[0, KEY_DIM:].astype(F32) * reach_ref[0]
    for k in range(1, PEERS):
        proj = proj + got_ref[k, :KEY_DIM].astype(F32)
        flow = flow + got_ref[k, KEY_DIM:].astype(F32) * reach_ref[k]
    proj_ref[:KEY_DIM] = proj[:, :VAL_DIM]
    proj_ref[KEY_DIM:] = proj[:, VAL_DIM:]
    cum = cum_ref[...]
    total = cum[:, TOK - 1 : TOK]
    keys, vals = key_ref[...].astype(F32), val_ref[...].astype(F32)
    scale_fwd, scale_bwd = jnp.exp(total - cum), jnp.exp(cum)
    flow_fwd, flow_bwd = flow[:, :VAL_DIM], flow[:, VAL_DIM:]
    grad_fwd = dot(flow_fwd, vals, 1, 0, EXACT) * scale_fwd
    grad_bwd = dot(flow_bwd, vals, 1, 0, EXACT) * scale_bwd
    keys_ref[...] = keys_mix_ref[...] + grad_fwd + grad_bwd
    vals_ref[...] = (
        vals_mix_ref[...]
        + dot(flow_fwd, keys * scale_fwd, 0, 0, EXACT)
        + dot(flow_bwd, keys * scale_bwd, 0, 0, EXACT)
    )
    factor = jnp.exp(total) * jnp.sum(flow * state_ref[...], axis=1, keepdims=True)
    grad_fwd, grad_bwd = grad_fwd * keys, grad_bwd * keys
    at_end = factor + jnp.sum(grad_fwd, axis=1, keepdims=True)
    row, col = iota((TOK, TOK), 0), iota((TOK, TOK), 1)
    tail = dot(grad_bwd - grad_fwd, ones_where(row >= col, F32), 1, 0, EXACT)
    decay = decay_mix_ref[...] + tail + at_end
    diagonal = iota((KEY_DIM, KEY_DIM), 0) == iota((KEY_DIM, KEY_DIM), 1)
    speed = jnp.sum(jnp.where(diagonal, speed_ref[...], 0.0), axis=1, keepdims=True)
    pre = pre_ref[...].astype(F32)
    logit_ref[...] = decay * speed * jax.nn.sigmoid(-pre)


SCALAR = pl.BlockSpec(memory_space=pltpu.SMEM)
WHOLE = pl.BlockSpec(memory_space=pltpu.VMEM)


def call(kernel, outs, *args, scalars=0):
    shapes = [jax.ShapeDtypeStruct(shape, dtype) for shape, dtype in outs]
    return pl.pallas_call(
        kernel,
        out_shape=shapes,
        in_specs=[SCALAR] * scalars + [WHOLE] * (len(args) - scalars),
        out_specs=[WHOLE] * len(shapes),
    )(*args)


def inner(scaled, keys, vals, cum):
    row, col = iota((TOK, TOK), 0), iota((TOK, TOK), 1)
    gap = cum[:, :, None] - cum[:, None, :]
    weight = jnp.exp(jnp.where(row >= col, gap, -gap))
    scores = jnp.einsum("ct,cs,cts->ts", scaled, keys, weight)
    return jnp.einsum("ts,vs->vt", scores, vals)


def carried(scaled, cum, fwd_in, bwd_in):
    total = cum[:, -1:]
    return jnp.einsum("ct,cv->vt", scaled * jnp.exp(cum), fwd_in) + jnp.einsum(
        "ct,cv->vt", scaled * jnp.exp(total - cum), bwd_in
    )


def body(
    queries,
    input_key_matrix,
    input_value_matrix,
    decay_preactivation,
    extra_log_decay,
    channel_decay_speed,
    output_weight_matrix,
    stored_expert_rows,
    chosen_expert_index,
    expert_combine_weight,
    cotangent,
    expert_gate_weight,
    expert_up_weight,
    expert_down_weight,
):
    sp = ("z", "x")
    core = lax.axis_index("core")
    core_at = core.reshape(1).astype(jnp.int32)
    place_at = lax.axis_index(sp).reshape(1).astype(jnp.int32)
    speed = channel_decay_speed.reshape(1, KEY_DIM)
    swap = [(0, 1), (1, 0)]

    def exchanged(array, axis):
        return lax.all_to_all(array, axis, split_axis=0, concat_axis=0, tiled=True)

    gate, up, down = expert_gate_weight[0], expert_up_weight[0], expert_down_weight[0]
    gate_blocks = gate.reshape(2 * RING, WIDTH, WIDTH)
    up_blocks = up.reshape(2 * RING, WIDTH, WIDTH)
    send, pick, cum = call(
        dispatch_kernel,
        [((PEERS, PAD, 2 * WIDTH), BF16), ((SLOTS, TOK), BF16), ((KEY_DIM, TOK), F32)],
        chosen_expert_index,
        expert_combine_weight,
        stored_expert_rows,
        cotangent,
        input_key_matrix,
        input_value_matrix,
        decay_preactivation,
        extra_log_decay,
        speed,
    )
    got = exchanged(send, sp)
    copies, back = call(
        arrival_kernel,
        [((RING, ROWS, 2 * WIDTH), BF16), ((PEERS, PAD, WIDTH), BF16)],
        got,
    )
    own = exchanged(copies, "y")

    theirs = jnp.stack(
        [
            lax.dynamic_index_in_dim(
                w.reshape(RING, 2, WIDTH, WIDTH), 1 - core, axis=1, keepdims=False
            )
            for w in (gate, up)
        ]
    )
    swapped = lax.ppermute(theirs, "core", swap)

    other = lax.ppermute(own, "core", swap)
    rows_x, rows_dy, grads, hidden = call(
        expert_kernel,
        [
            ((ROWS, MODEL), BF16),
            ((ROWS, MODEL), BF16),
            ((ROWS, 2 * WIDTH), BF16),
            ((ROWS, WIDTH), BF16),
        ],
        core_at,
        own,
        other,
        gate,
        up,
        down,
        scalars=1,
    )
    grads_both = lax.all_gather(grads, "core", axis=0, tiled=False)
    (partials,) = call(
        partial_kernel,
        [((RING, ROWS, WIDTH), BF16)],
        core_at,
        grads_both,
        gate_blocks,
        up_blocks,
        swapped,
        scalars=1,
    )
    parts = exchanged(partials, "y")
    grad_both = dot(rows_x, grads, 0, 0).astype(BF16)
    grad_gate, grad_up = grad_both[:, :WIDTH], grad_both[:, WIDTH:]
    grad_down = dot(hidden, rows_dy, 0, 0).astype(BF16)
    (send,) = call(return_kernel, [((PEERS, PAD, WIDTH), BF16)], parts, back)
    returned = exchanged(send, sp)
    (copies,) = call(
        token_kernel, [((RING, TOK, WIDTH), BF16)], returned, pick, cotangent
    )
    full_rows = exchanged(copies, "y")
    full_rows = lax.all_gather(full_rows, "core", axis=0, tiled=False)

    state, reach = call(
        state_kernel,
        [((KEY_DIM, WIDTH), F32), ((PEERS, KEY_DIM, WIDTH), F32)],
        place_at,
        returned,
        scalars=1,
    )
    scaled = queries.astype(F32) * KEY_DIM ** (-0.5)
    keys = input_key_matrix.astype(F32)
    vals = input_value_matrix.astype(F32)
    fwd_in, bwd_in = state[:, :VAL_DIM], state[:, VAL_DIM:]
    inner_out, pull_inner = jax.vjp(inner, scaled, keys, vals, cum)
    carried_out, pull_carried = jax.vjp(
        lambda s, c: carried(s, c, fwd_in, bwd_in), scaled, cum
    )
    mixed = inner_out + carried_out
    inv_rms = lax.rsqrt(jnp.mean(mixed * mixed, axis=0, keepdims=True) + 1e-06)
    normed = mixed * inv_rms
    normed_t = normed.T
    mix_t = normed_t.astype(BF16)
    send, grad_mixed_t = call(
        source_kernel,
        [((PEERS, 2 * KEY_DIM, WIDTH), BF16), ((TOK, VAL_DIM), F32)],
        full_rows,
        output_weight_matrix,
        normed_t,
        inv_rms.reshape(TOK, 1),
        jnp.concatenate([mix_t, mix_t], axis=1),
        scaled * jnp.exp(cum),
        scaled * jnp.exp(cum[:, -1:] - cum),
    )
    got = exchanged(send, sp)
    grad_mixed = grad_mixed_t.T
    grad_scaled, grad_keys, grad_vals, grad_cum = pull_inner(grad_mixed)
    grad_scaled_in, grad_cum_in = pull_carried(grad_mixed)
    grad_queries = (grad_scaled + grad_scaled_in) * KEY_DIM ** (-0.5)
    tail_mask = ones_where(iota((TOK, TOK), 0) >= iota((TOK, TOK), 1), F32)
    grad_decay = dot(grad_cum + grad_cum_in, tail_mask, 1, 0, EXACT)
    grad_out_proj, grad_keys, grad_values, grad_logit = call(
        final_kernel,
        [
            ((2 * KEY_DIM, VAL_DIM), F32),
            ((KEY_DIM, TOK), F32),
            ((VAL_DIM, TOK), F32),
            ((KEY_DIM, TOK), F32),
        ],
        got,
        reach,
        state,
        cum,
        input_key_matrix,
        input_value_matrix,
        decay_preactivation,
        speed,
        grad_keys,
        grad_vals,
        grad_decay,
    )
    return (
        grad_queries,
        grad_keys,
        grad_values,
        grad_logit,
        grad_out_proj,
        grad_gate[None],
        grad_up[None],
        grad_down[None],
    )


def solution(mesh):
    fine = Mesh(mesh.devices.reshape(8, 4, 8, 2), ("z", "x", "y", "core"))
    sp, tp = ("z", "x"), ("y", "core")
    in_specs = (
        P(tp, sp),
        P(tp, sp),
        P(tp, sp),
        P(tp, sp),
        P(tp, sp),
        P(tp),
        P(None, tp),
        P(sp, tp),
        P(sp, None),
        P(sp, None),
        P(sp, tp),
        P(sp, None, tp),
        P(sp, None, tp),
        P(sp, tp, None),
    )
    out_specs = (
        P(tp, sp),
        P(tp, sp),
        P(tp, sp),
        P(tp, sp),
        P(sp, tp),
        P(sp, None, tp),
        P(sp, None, tp),
        P(sp, tp, None),
    )
    return jax.shard_map(body, mesh=fine, in_specs=in_specs, out_specs=out_specs, check_vma=False)
```

```python
import jax
import jax.numpy as jnp
from jax import lax
from jax.experimental import pallas as pl
from jax.experimental.pallas import tpu as pltpu
from jax.sharding import Mesh
from jax.sharding import PartitionSpec as P

KEY_DIM = 32
VAL_DIM = 64
TOK = 128
PEERS = 32
CAP = 12
PAD = 16
RING = 8
SLOTS = PEERS * PAD
ROWS = PEERS * CAP
WIDTH = 128
MODEL = 2048

F32 = jnp.float32
BF16 = jnp.bfloat16
EXACT = lax.Precision.HIGHEST


def dot(a, b, da, db, precision=None):
    return lax.dot_general(
        a, b, (((da,), (db,)), ((), ())), preferred_element_type=F32, precision=precision
    )


def iota(shape, dim):
    return lax.broadcasted_iota(jnp.int32, shape, dim)


def ones_where(mask, dtype=BF16):
    return jnp.where(mask, 1.0, 0.0).astype(dtype)


def split_two(value):
    high = value.astype(BF16).astype(F32)
    return high, (value - high).astype(BF16).astype(F32)


def split_three(value):
    high, rest = split_two(value)
    return high, rest, (value - high - rest).astype(BF16).astype(F32)


def compact_rows(shape, compact_dim):
    row = iota(shape, compact_dim)
    peer = (row * 5462) >> 16
    return peer * PAD + (row - peer * CAP) == iota(shape, 1 - compact_dim)


def row_of_peer(place):
    return iota((PEERS, SLOTS), 1) == iota((PEERS, SLOTS), 0) * PAD + place


def dispatch_kernel(
    ids_ref, share_ref, x_ref, cot_ref, key_ref, val_ref, pre_ref, extra_ref, speed_ref,
    send_ref, pick_ref, cum_ref,
):
    ids = ids_ref[...]
    expert = iota((TOK, PEERS), 1)
    named = [ones_where(ids[:, k : k + 1] == expert) for k in range(2)]
    row, col = iota((TOK, TOK), 0), iota((TOK, TOK), 1)
    earlier, same = ones_where(row < col), ones_where(row == col)
    rank = dot(named[0] + named[1], earlier, 0, 0)
    place = iota((PEERS, PAD, TOK), 1).astype(F32)
    cot = cot_ref[...].astype(F32)
    picks, grads = [], None
    for k in range(2):
        mine = dot(named[k], same, 0, 0)
        at = jnp.where(mine > 0.5, rank, -1.0)
        pick = jnp.where(at[:, None, :] == place, 1.0, 0.0).reshape(SLOTS, TOK).astype(BF16)
        weighted = (share_ref[:, k : k + 1] * cot).astype(BF16)
        part = dot(pick, weighted, 1, 0)
        grads = part if grads is None else grads + part
        picks.append(pick)
    pick = picks[0] + picks[1]
    pick_ref[...] = pick
    rows = jnp.concatenate([dot(pick, x_ref[...], 1, 0), grads], axis=1)

    pre = pre_ref[...].astype(F32)
    log_sig = jnp.minimum(pre, 0.0) - jnp.log1p(jnp.exp(-jnp.abs(pre)))
    diagonal = iota((KEY_DIM, KEY_DIM), 0) == iota((KEY_DIM, KEY_DIM), 1)
    speed = jnp.sum(jnp.where(diagonal, speed_ref[...], 0.0), axis=1, keepdims=True)
    decay = speed * log_sig + extra_ref[...]
    cum = dot(decay, ones_where(row <= col, F32), 1, 0, EXACT)
    cum_ref[...] = cum
    total = cum[:, TOK - 1 : TOK]
    keys, vals = key_ref[...].astype(F32), val_ref[...].astype(F32)
    sums = jnp.concatenate(
        [
            dot(keys * jnp.exp(total - cum), vals, 1, 1, EXACT),
            dot(keys * jnp.exp(cum), vals, 1, 1, EXACT),
        ],
        axis=1,
    )
    state = jnp.concatenate(split_two(sums), axis=1)
    lane = iota((KEY_DIM, 2 * WIDTH), 1)
    logs = jnp.zeros((KEY_DIM, 2 * WIDTH), F32)
    for k, part in enumerate(split_three(total)):
        logs = jnp.where(lane == k, part, logs)
    place = iota((PEERS, PAD, 2 * WIDTH), 1)
    block = rows.reshape(PEERS, PAD, 2 * WIDTH)
    block = jnp.where(place == CAP, state[:, None, :], block)
    block = jnp.where(place == CAP + 1, logs[:, None, :], block)
    send_ref[...] = block.astype(BF16)


def arrival_kernel(got_ref, copies_ref, back_ref):
    got = got_ref[...].reshape(SLOTS, 2 * WIDTH)
    rows = dot(ones_where(compact_rows((ROWS, SLOTS), 0)), got, 1, 0).astype(BF16)
    for k in range(RING):
        copies_ref[k] = rows
    both = dot(ones_where(row_of_peer(CAP)), got, 1, 0)
    state = both[:, :WIDTH] + both[:, WIDTH:]
    logs = dot(ones_where(row_of_peer(CAP + 1)), got, 1, 0)
    log = jnp.sum(logs, axis=1, keepdims=True)
    a, b = iota((PEERS, PEERS), 0), iota((PEERS, PEERS), 1)
    gap_fwd = dot(ones_where(b < a, F32), jnp.where(a > b, log, 0.0), 1, 0, EXACT)
    gap_bwd = dot(ones_where(b > a, F32), jnp.where(a < b, log, 0.0), 1, 0, EXACT)
    fwd = dot(jnp.where(b < a, jnp.exp(gap_fwd), 0.0), state, 1, 0, EXACT)
    bwd = dot(jnp.where(b > a, jnp.exp(gap_bwd), 0.0), state, 1, 0, EXACT)
    lane = iota((PEERS, WIDTH), 1)
    high, low = split_two(jnp.where(lane < VAL_DIM, fwd, bwd))
    peer = iota((PEERS, WIDTH), 0)
    spread = jnp.zeros((PEERS, WIDTH), F32)
    for k, part in enumerate(split_three(log)):
        spread = jnp.where(lane == peer + k * PEERS, part, spread)
    all_logs = jnp.sum(spread, axis=0, keepdims=True)
    place = iota((PEERS, PAD, WIDTH), 1)
    block = jnp.where(place == CAP, high[:, None, :], 0.0)
    block = jnp.where(place == CAP + 1, low[:, None, :], block)
    block = jnp.where(place == CAP + 2, all_logs[:, None, :], block)
    back_ref[...] = block.astype(BF16)


def expert_kernel(
    core_ref, own_ref, other_ref, gate_ref, up_ref, down_ref,
    x_ref, y_ref, grads_ref, hidden_ref,
):
    core = core_ref[0]
    for mine in range(2):

        @pl.when(core == mine)
        def _():
            for side, ref in ((mine, own_ref), (1 - mine, other_ref)):
                for k in range(RING):
                    at = slice((2 * k + side) * WIDTH, (2 * k + side + 1) * WIDTH)
                    x_ref[:, at] = ref[k, :, :WIDTH]
                    y_ref[:, at] = ref[k, :, WIDTH:]

    x, y = x_ref[...], y_ref[...]
    gate_pre = dot(x, gate_ref[...], 1, 0)
    up_pre = dot(x, up_ref[...], 1, 0)
    grad_hidden = dot(y, down_ref[...], 1, 1)
    gate_sig = jax.nn.sigmoid(gate_pre)
    gate_act = gate_pre * gate_sig
    hidden_ref[...] = (gate_act * up_pre).astype(BF16)
    grads_ref[:, :WIDTH] = (
        grad_hidden * up_pre * gate_sig * (1.0 + gate_pre * (1.0 - gate_sig))
    ).astype(BF16)
    grads_ref[:, WIDTH:] = (grad_hidden * gate_act).astype(BF16)


def partial_kernel(core_ref, grads_ref, gate_ref, up_ref, swapped_ref, out_ref):
    core = core_ref[0]
    both = jnp.concatenate([grads_ref[core], grads_ref[1 - core]], axis=1)
    for k in range(RING):
        at = 2 * k + core
        weights = jnp.concatenate(
            [gate_ref[at], up_ref[at], swapped_ref[0, k], swapped_ref[1, k]], axis=1
        )
        out_ref[k] = dot(both, weights, 1, 1).astype(BF16)


def return_kernel(parts_ref, back_ref, send_ref):
    total = parts_ref[0].astype(F32)
    for k in range(1, RING):
        total = total + parts_ref[k].astype(F32)
    rows = dot(ones_where(compact_rows((SLOTS, ROWS), 1)), total.astype(BF16), 1, 0)
    rows = rows.astype(BF16).reshape(PEERS, PAD, WIDTH)
    send_ref[...] = rows + back_ref[...]


def token_kernel(got_ref, pick_ref, cot_ref, copies_ref):
    got = got_ref[...].reshape(SLOTS, WIDTH)
    rows = (cot_ref[...].astype(F32) + dot(pick_ref[...], got, 0, 0)).astype(BF16)
    for k in range(RING):
        copies_ref[k] = rows


def state_kernel(place_ref, got_ref, state_ref, reach_ref):
    got = got_ref[...].reshape(SLOTS, WIDTH)
    state_ref[...] = dot(ones_where(row_of_peer(CAP) | row_of_peer(CAP + 1)), got, 1, 0)
    spread = dot(ones_where(row_of_peer(CAP + 2)), got, 1, 0).astype(BF16)
    lane, peer = iota((WIDTH, PEERS), 0), iota((WIDTH, PEERS), 1)
    fold = (lane == peer) | (lane == peer + PEERS) | (lane == peer + 2 * PEERS)
    logs = dot(spread, ones_where(fold), 1, 0)
    here = place_ref[0]
    a, b = iota((PEERS, PEERS), 0), iota((PEERS, PEERS), 1)
    later = dot(jnp.where(b > here, logs, 0.0), ones_where(a < b, F32), 1, 0, EXACT)
    before = dot(jnp.where(b < here, logs, 0.0), ones_where(a > b, F32), 1, 0, EXACT)
    later = jnp.where(b > here, jnp.exp(later), 0.0)
    before = jnp.where(b < here, jnp.exp(before), 0.0)
    lane = iota((KEY_DIM, WIDTH), 1)
    for k in range(PEERS):
        reach_ref[k] = jnp.where(lane < VAL_DIM, later[:, k : k + 1], before[:, k : k + 1])


def source_kernel(
    rows_ref, weight_ref, normed_ref, inv_ref, mix_ref, query_fwd_ref, query_bwd_ref,
    send_ref, grad_ref,
):
    rows = jnp.concatenate([rows_ref[c, k] for k in range(RING) for c in range(2)], axis=1)
    grad = dot(rows, weight_ref[...], 1, 0)
    normed = normed_ref[...]
    mean = jnp.mean(grad * normed, axis=1, keepdims=True)
    grad = inv_ref[...] * (grad - normed * mean)
    grad_ref[...] = grad
    state = jnp.concatenate(
        [
            dot(query_fwd_ref[...], grad, 1, 0, EXACT),
            dot(query_bwd_ref[...], grad, 1, 0, EXACT),
        ],
        axis=1,
    ).astype(BF16)
    lane = iota((KEY_DIM, WIDTH), 1)
    for k in range(2 * RING):
        part = dot(rows[:, k * WIDTH : (k + 1) * WIDTH], mix_ref[...], 0, 0)
        for half in range(2):
            at = half * VAL_DIM
            both = jnp.where(lane < VAL_DIM, part[at : at + 32], part[at + 32 : at + 64])
            send_ref[2 * k + half, :KEY_DIM] = both.astype(BF16)
            send_ref[2 * k + half, KEY_DIM:] = state


def final_kernel(
    got_ref, reach_ref, state_ref, cum_ref, key_ref, val_ref, pre_ref, speed_ref,
    keys_mix_ref, vals_mix_ref, decay_mix_ref,
    proj_ref, keys_ref, vals_ref, logit_ref,
):
    proj = got_ref[0, :KEY_DIM].astype(F32)
    flow = got_ref[0, KEY_DIM:].astype(F32) * reach_ref[0]
    for k in range(1, PEERS):
        proj = proj + got_ref[k, :KEY_DIM].astype(F32)
        flow = flow + got_ref[k, KEY_DIM:].astype(F32) * reach_ref[k]
    proj_ref[:KEY_DIM] = proj[:, :VAL_DIM]
    proj_ref[KEY_DIM:] = proj[:, VAL_DIM:]
    cum = cum_ref[...]
    total = cum[:, TOK - 1 : TOK]
    keys, vals = key_ref[...].astype(F32), val_ref[...].astype(F32)
    scale_fwd, scale_bwd = jnp.exp(total - cum), jnp.exp(cum)
    flow_fwd, flow_bwd = flow[:, :VAL_DIM], flow[:, VAL_DIM:]
    grad_fwd = dot(flow_fwd, vals, 1, 0, EXACT) * scale_fwd
    grad_bwd = dot(flow_bwd, vals, 1, 0, EXACT) * scale_bwd
    keys_ref[...] = keys_mix_ref[...] + grad_fwd + grad_bwd
    vals_ref[...] = (
        vals_mix_ref[...]
        + dot(flow_fwd, keys * scale_fwd, 0, 0, EXACT)
        + dot(flow_bwd, keys * scale_bwd, 0, 0, EXACT)
    )
    factor = jnp.exp(total) * jnp.sum(flow * state_ref[...], axis=1, keepdims=True)
    grad_fwd, grad_bwd = grad_fwd * keys, grad_bwd * keys
    at_end = factor + jnp.sum(grad_fwd, axis=1, keepdims=True)
    row, col = iota((TOK, TOK), 0), iota((TOK, TOK), 1)
    tail = dot(grad_bwd - grad_fwd, ones_where(row >= col, F32), 1, 0, EXACT)
    decay = decay_mix_ref[...] + tail + at_end
    diagonal = iota((KEY_DIM, KEY_DIM), 0) == iota((KEY_DIM, KEY_DIM), 1)
    speed = jnp.sum(jnp.where(diagonal, speed_ref[...], 0.0), axis=1, keepdims=True)
    pre = pre_ref[...].astype(F32)
    logit_ref[...] = decay * speed * jax.nn.sigmoid(-pre)


SCALAR = pl.BlockSpec(memory_space=pltpu.SMEM)
WHOLE = pl.BlockSpec(memory_space=pltpu.VMEM)


def on_chip(array):
    return pltpu.with_memory_space_constraint(array, pltpu.VMEM)


def call(kernel, outs, *args, scalars=0, stored=()):
    shapes = [
        (jax.ShapeDtypeStruct if k in stored else pltpu.VMEM)(shape, dtype)
        for k, (shape, dtype) in enumerate(outs)
    ]
    return pl.pallas_call(
        kernel,
        out_shape=shapes,
        in_specs=[SCALAR] * scalars + [WHOLE] * (len(args) - scalars),
        out_specs=[WHOLE] * len(shapes),
        compiler_params=pltpu.CompilerParams(vmem_limit_bytes=24 << 20),
    )(*args)


def inner(scaled, keys, vals, cum):
    row, col = iota((TOK, TOK), 0), iota((TOK, TOK), 1)
    gap = cum[:, :, None] - cum[:, None, :]
    weight = jnp.exp(jnp.where(row >= col, gap, -gap))
    scores = jnp.einsum("ct,cs,cts->ts", scaled, keys, weight)
    return jnp.einsum("ts,vs->vt", scores, vals)


def carried(scaled, cum, fwd_in, bwd_in):
    total = cum[:, -1:]
    return jnp.einsum("ct,cv->vt", scaled * jnp.exp(cum), fwd_in) + jnp.einsum(
        "ct,cv->vt", scaled * jnp.exp(total - cum), bwd_in
    )


def body(
    queries,
    input_key_matrix,
    input_value_matrix,
    decay_preactivation,
    extra_log_decay,
    channel_decay_speed,
    output_weight_matrix,
    stored_expert_rows,
    chosen_expert_index,
    expert_combine_weight,
    cotangent,
    expert_gate_weight,
    expert_up_weight,
    expert_down_weight,
):
    sp = ("z", "x")
    core = lax.axis_index("core")
    core_at = core.reshape(1).astype(jnp.int32)
    place_at = lax.axis_index(sp).reshape(1).astype(jnp.int32)
    speed = channel_decay_speed.reshape(1, KEY_DIM)
    swap = [(0, 1), (1, 0)]

    def exchanged(array, axis):
        return lax.all_to_all(array, axis, split_axis=0, concat_axis=0, tiled=True)

    gate, up, down = expert_gate_weight[0], expert_up_weight[0], expert_down_weight[0]
    gate_blocks = gate.reshape(2 * RING, WIDTH, WIDTH)
    up_blocks = up.reshape(2 * RING, WIDTH, WIDTH)
    send, pick, cum = call(
        dispatch_kernel,
        [((PEERS, PAD, 2 * WIDTH), BF16), ((SLOTS, TOK), BF16), ((KEY_DIM, TOK), F32)],
        chosen_expert_index,
        expert_combine_weight,
        stored_expert_rows,
        cotangent,
        input_key_matrix,
        input_value_matrix,
        decay_preactivation,
        extra_log_decay,
        speed,
    )
    got = on_chip(exchanged(send, sp))
    copies, back = call(
        arrival_kernel,
        [((RING, ROWS, 2 * WIDTH), BF16), ((PEERS, PAD, WIDTH), BF16)],
        got,
    )
    own = exchanged(copies, "y")

    theirs = jnp.stack(
        [
            lax.dynamic_index_in_dim(
                w.reshape(RING, 2, WIDTH, WIDTH), 1 - core, axis=1, keepdims=False
            )
            for w in (gate, up)
        ]
    )
    swapped = lax.ppermute(theirs, "core", swap)

    other = lax.ppermute(own, "core", swap)
    rows_x, rows_dy, grads, hidden = call(
        expert_kernel,
        [
            ((ROWS, MODEL), BF16),
            ((ROWS, MODEL), BF16),
            ((ROWS, 2 * WIDTH), BF16),
            ((ROWS, WIDTH), BF16),
        ],
        core_at,
        on_chip(own),
        on_chip(other),
        gate,
        up,
        down,
        scalars=1,
        stored=(0, 1),
    )
    grads_both = lax.all_gather(grads, "core", axis=0, tiled=False)
    (partials,) = call(
        partial_kernel,
        [((RING, ROWS, WIDTH), BF16)],
        core_at,
        on_chip(grads_both),
        gate_blocks,
        up_blocks,
        on_chip(swapped),
        scalars=1,
    )
    parts = exchanged(partials, "y")
    grad_both = dot(rows_x, grads, 0, 0).astype(BF16)
    grad_gate, grad_up = grad_both[:, :WIDTH], grad_both[:, WIDTH:]
    grad_down = dot(hidden, rows_dy, 0, 0).astype(BF16)
    (send,) = call(return_kernel, [((PEERS, PAD, WIDTH), BF16)], on_chip(parts), on_chip(back))
    returned = on_chip(exchanged(send, sp))
    (copies,) = call(
        token_kernel, [((RING, TOK, WIDTH), BF16)], returned, pick, cotangent
    )
    full_rows = exchanged(copies, "y")
    full_rows = lax.all_gather(full_rows, "core", axis=0, tiled=False)

    state, reach = call(
        state_kernel,
        [((KEY_DIM, WIDTH), F32), ((PEERS, KEY_DIM, WIDTH), F32)],
        place_at,
        returned,
        scalars=1,
    )
    scaled = queries.astype(F32) * KEY_DIM ** (-0.5)
    keys = input_key_matrix.astype(F32)
    vals = input_value_matrix.astype(F32)
    fwd_in, bwd_in = state[:, :VAL_DIM], state[:, VAL_DIM:]
    inner_out, pull_inner = jax.vjp(inner, scaled, keys, vals, cum)
    carried_out, pull_carried = jax.vjp(
        lambda s, c: carried(s, c, fwd_in, bwd_in), scaled, cum
    )
    mixed = inner_out + carried_out
    inv_rms = lax.rsqrt(jnp.mean(mixed * mixed, axis=0, keepdims=True) + 1e-06)
    normed = mixed * inv_rms
    normed_t = normed.T
    mix_t = normed_t.astype(BF16)
    send, grad_mixed_t = call(
        source_kernel,
        [((PEERS, 2 * KEY_DIM, WIDTH), BF16), ((TOK, VAL_DIM), F32)],
        on_chip(full_rows),
        output_weight_matrix,
        normed_t,
        inv_rms.reshape(TOK, 1),
        jnp.concatenate([mix_t, mix_t], axis=1),
        scaled * jnp.exp(cum),
        scaled * jnp.exp(cum[:, -1:] - cum),
    )
    got = exchanged(send, sp)
    grad_mixed = grad_mixed_t.T
    grad_scaled, grad_keys, grad_vals, grad_cum = pull_inner(grad_mixed)
    grad_scaled_in, grad_cum_in = pull_carried(grad_mixed)
    grad_queries = (grad_scaled + grad_scaled_in) * KEY_DIM ** (-0.5)
    tail_mask = ones_where(iota((TOK, TOK), 0) >= iota((TOK, TOK), 1), F32)
    grad_decay = dot(grad_cum + grad_cum_in, tail_mask, 1, 0, EXACT)
    grad_out_proj, grad_keys, grad_values, grad_logit = call(
        final_kernel,
        [
            ((2 * KEY_DIM, VAL_DIM), F32),
            ((KEY_DIM, TOK), F32),
            ((VAL_DIM, TOK), F32),
            ((KEY_DIM, TOK), F32),
        ],
        on_chip(got),
        reach,
        state,
        cum,
        input_key_matrix,
        input_value_matrix,
        decay_preactivation,
        speed,
        grad_keys,
        grad_vals,
        grad_decay,
        stored=range(4),
    )
    return (
        grad_queries,
        grad_keys,
        grad_values,
        grad_logit,
        grad_out_proj,
        grad_gate[None],
        grad_up[None],
        grad_down[None],
    )


def solution(mesh):
    fine = Mesh(mesh.devices.reshape(8, 4, 8, 2), ("z", "x", "y", "core"))
    sp, tp = ("z", "x"), ("y", "core")
    in_specs = (
        P(tp, sp),
        P(tp, sp),
        P(tp, sp),
        P(tp, sp),
        P(tp, sp),
        P(tp),
        P(None, tp),
        P(sp, tp),
        P(sp, None),
        P(sp, None),
        P(sp, tp),
        P(sp, None, tp),
        P(sp, None, tp),
        P(sp, tp, None),
    )
    out_specs = (
        P(tp, sp),
        P(tp, sp),
        P(tp, sp),
        P(tp, sp),
        P(sp, tp),
        P(sp, None, tp),
        P(sp, None, tp),
        P(sp, tp, None),
    )
    return jax.shard_map(body, mesh=fine, in_specs=in_specs, out_specs=out_specs, check_vma=False)
```

```python
import jax
import jax.numpy as jnp
from jax import lax
from jax.experimental import pallas as pl
from jax.experimental.pallas import tpu as pltpu
from jax.sharding import Mesh
from jax.sharding import PartitionSpec as P

KEY_DIM = 32
VAL_DIM = 64
TOK = 128
PEERS = 32
CAP = 12
PAD = 16
RING = 8
SLOTS = PEERS * PAD
ROWS = PEERS * CAP
WIDTH = 128
MODEL = 2048

F32 = jnp.float32
BF16 = jnp.bfloat16
EXACT = lax.Precision.HIGHEST


def dot(a, b, da, db, precision=None):
    return lax.dot_general(
        a, b, (((da,), (db,)), ((), ())), preferred_element_type=F32, precision=precision
    )


def iota(shape, dim):
    return lax.broadcasted_iota(jnp.int32, shape, dim)


def ones_where(mask, dtype=BF16):
    return jnp.where(mask, 1.0, 0.0).astype(dtype)


def split_two(value):
    high = value.astype(BF16).astype(F32)
    return high, (value - high).astype(BF16).astype(F32)


def split_three(value):
    high, rest = split_two(value)
    return high, rest, (value - high - rest).astype(BF16).astype(F32)


def compact_rows(shape, compact_dim):
    row = iota(shape, compact_dim)
    peer = (row * 5462) >> 16
    return peer * PAD + (row - peer * CAP) == iota(shape, 1 - compact_dim)


def row_of_peer(place):
    return iota((PEERS, SLOTS), 1) == iota((PEERS, SLOTS), 0) * PAD + place


def dispatch_kernel(
    ids_ref, share_ref, x_ref, cot_ref, key_ref, val_ref, pre_ref, extra_ref, speed_ref,
    send_ref, pick_ref, cum_ref,
):
    expert = iota((PEERS, TOK), 0)
    named = [ids_ref[k : k + 1, :] == expert for k in range(2)]
    row, col = iota((TOK, TOK), 0), iota((TOK, TOK), 1)
    rank = dot(ones_where(named[0] | named[1]), ones_where(row < col), 1, 0)
    place = iota((PEERS, PAD, TOK), 1).astype(F32)
    cot = cot_ref[...].astype(F32)
    picks, grads = [], None
    for k in range(2):
        at = jnp.where(named[k], rank, -1.0)
        pick = jnp.where(at[:, None, :] == place, 1.0, 0.0).reshape(SLOTS, TOK).astype(BF16)
        share = jnp.sum(jnp.where(row == col, share_ref[k : k + 1, :], 0.0), axis=1, keepdims=True)
        part = dot(pick, (share * cot).astype(BF16), 1, 0)
        grads = part if grads is None else grads + part
        picks.append(pick)
    pick = picks[0] + picks[1]
    pick_ref[...] = pick
    rows = jnp.concatenate([dot(pick, x_ref[...], 1, 0), grads], axis=1)

    pre = pre_ref[...].astype(F32)
    log_sig = jnp.minimum(pre, 0.0) - jnp.log1p(jnp.exp(-jnp.abs(pre)))
    diagonal = iota((KEY_DIM, KEY_DIM), 0) == iota((KEY_DIM, KEY_DIM), 1)
    speed = jnp.sum(jnp.where(diagonal, speed_ref[...], 0.0), axis=1, keepdims=True)
    decay = speed * log_sig + extra_ref[...]
    cum = dot(decay, ones_where(row <= col, F32), 1, 0, EXACT)
    cum_ref[...] = cum
    total = cum[:, TOK - 1 : TOK]
    keys, vals = key_ref[...].astype(F32), val_ref[...].astype(F32)
    sums = jnp.concatenate(
        [
            dot(keys * jnp.exp(total - cum), vals, 1, 1, EXACT),
            dot(keys * jnp.exp(cum), vals, 1, 1, EXACT),
        ],
        axis=1,
    )
    state = jnp.concatenate(split_two(sums), axis=1)
    lane = iota((KEY_DIM, 2 * WIDTH), 1)
    logs = jnp.zeros((KEY_DIM, 2 * WIDTH), F32)
    for k, part in enumerate(split_three(total)):
        logs = jnp.where(lane == k, part, logs)
    place = iota((PEERS, PAD, 2 * WIDTH), 1)
    block = rows.reshape(PEERS, PAD, 2 * WIDTH)
    block = jnp.where(place == CAP, state[:, None, :], block)
    block = jnp.where(place == CAP + 1, logs[:, None, :], block)
    send_ref[...] = block.astype(BF16)


def arrival_kernel(got_ref, x_ref, copies_ref, back_ref):
    got = got_ref[...].reshape(SLOTS, 2 * WIDTH)
    rows = dot(ones_where(compact_rows((ROWS, SLOTS), 0)), got, 1, 0).astype(BF16)
    x_ref[...] = rows[:, :WIDTH]
    for k in range(RING):
        copies_ref[k] = rows[:, WIDTH:]
    both = dot(ones_where(row_of_peer(CAP)), got, 1, 0)
    state = both[:, :WIDTH] + both[:, WIDTH:]
    logs = dot(ones_where(row_of_peer(CAP + 1)), got, 1, 0)
    log = jnp.sum(logs, axis=1, keepdims=True)
    a, b = iota((PEERS, PEERS), 0), iota((PEERS, PEERS), 1)
    gap_fwd = dot(ones_where(b < a, F32), jnp.where(a > b, log, 0.0), 1, 0, EXACT)
    gap_bwd = dot(ones_where(b > a, F32), jnp.where(a < b, log, 0.0), 1, 0, EXACT)
    fwd = dot(jnp.where(b < a, jnp.exp(gap_fwd), 0.0), state, 1, 0, EXACT)
    bwd = dot(jnp.where(b > a, jnp.exp(gap_bwd), 0.0), state, 1, 0, EXACT)
    lane = iota((PEERS, WIDTH), 1)
    high, low = split_two(jnp.where(lane < VAL_DIM, fwd, bwd))
    peer = iota((PEERS, WIDTH), 0)
    spread = jnp.zeros((PEERS, WIDTH), F32)
    for k, part in enumerate(split_three(log)):
        spread = jnp.where(lane == peer + k * PEERS, part, spread)
    all_logs = jnp.sum(spread, axis=0, keepdims=True)
    place = iota((PEERS, PAD, WIDTH), 1)
    block = jnp.where(place == CAP, high[:, None, :], 0.0)
    block = jnp.where(place == CAP + 1, low[:, None, :], block)
    block = jnp.where(place == CAP + 2, all_logs[:, None, :], block)
    back_ref[...] = block.astype(BF16)


def forward_kernel(core_ref, own_ref, other_ref, gate_ref, up_ref, pre_ref):
    core = core_ref[0]
    total = jnp.zeros((ROWS, 2 * WIDTH), F32)
    for k in range(RING):
        for side, ref in ((core, own_ref), (1 - core, other_ref)):
            at = 2 * k + side
            weights = jnp.concatenate([gate_ref[at], up_ref[at]], axis=1)
            total = total + dot(ref[k], weights, 1, 0)
    pre_ref[...] = total


def hidden_kernel(core_ref, own_ref, other_ref, down_ref, pre_ref, grads_ref, hidden_ref):
    core = core_ref[0]
    grad_hidden = jnp.zeros((ROWS, WIDTH), F32)
    for k in range(RING):
        for side, ref in ((core, own_ref), (1 - core, other_ref)):
            at = pl.multiple_of((2 * k + side) * WIDTH, WIDTH)
            grad_hidden = grad_hidden + dot(ref[k], down_ref[:, pl.ds(at, WIDTH)], 1, 1)
    gate_pre, up_pre = pre_ref[:, :WIDTH], pre_ref[:, WIDTH:]
    gate_sig = jax.nn.sigmoid(gate_pre)
    gate_act = gate_pre * gate_sig
    hidden_ref[...] = (gate_act * up_pre).astype(BF16)
    grads_ref[:, :WIDTH] = (
        grad_hidden * up_pre * gate_sig * (1.0 + gate_pre * (1.0 - gate_sig))
    ).astype(BF16)
    grads_ref[:, WIDTH:] = (grad_hidden * gate_act).astype(BF16)


def weight_kernel(
    core_ref, x_ref, other_x_ref, y_ref, other_y_ref, grads_ref, hidden_ref,
    gate_ref, up_ref, down_ref,
):
    core = core_ref[0]
    grads, hidden = grads_ref[...], hidden_ref[...]
    for k in range(RING):
        for side, x, y in ((core, x_ref, y_ref), (1 - core, other_x_ref, other_y_ref)):
            at = 2 * k + side
            both = dot(x[k], grads, 0, 0).astype(BF16)
            gate_ref[at] = both[:, :WIDTH]
            up_ref[at] = both[:, WIDTH:]
            lanes = pl.ds(pl.multiple_of(at * WIDTH, WIDTH), WIDTH)
            down_ref[:, lanes] = dot(hidden, y[k], 0, 0).astype(BF16)


def partial_kernel(core_ref, grads_ref, gate_ref, up_ref, swapped_ref, out_ref):
    core = core_ref[0]
    both = jnp.concatenate([grads_ref[core], grads_ref[1 - core]], axis=1)
    for k in range(RING):
        at = 2 * k + core
        weights = jnp.concatenate(
            [gate_ref[at], up_ref[at], swapped_ref[0, k], swapped_ref[1, k]], axis=1
        )
        out_ref[k] = dot(both, weights, 1, 1).astype(BF16)


def return_kernel(parts_ref, back_ref, send_ref):
    total = parts_ref[0].astype(F32)
    for k in range(1, RING):
        total = total + parts_ref[k].astype(F32)
    rows = dot(ones_where(compact_rows((SLOTS, ROWS), 1)), total.astype(BF16), 1, 0)
    rows = rows.astype(BF16).reshape(PEERS, PAD, WIDTH)
    send_ref[...] = rows + back_ref[...]


def token_kernel(got_ref, pick_ref, cot_ref, copies_ref):
    got = got_ref[...].reshape(SLOTS, WIDTH)
    rows = (cot_ref[...].astype(F32) + dot(pick_ref[...], got, 0, 0)).astype(BF16)
    for k in range(RING):
        copies_ref[k] = rows


def state_kernel(place_ref, got_ref, state_ref, reach_ref):
    got = got_ref[...].reshape(SLOTS, WIDTH)
    state_ref[...] = dot(ones_where(row_of_peer(CAP) | row_of_peer(CAP + 1)), got, 1, 0)
    spread = dot(ones_where(row_of_peer(CAP + 2)), got, 1, 0).astype(BF16)
    lane, peer = iota((WIDTH, PEERS), 0), iota((WIDTH, PEERS), 1)
    fold = (lane == peer) | (lane == peer + PEERS) | (lane == peer + 2 * PEERS)
    logs = dot(spread, ones_where(fold), 1, 0)
    here = place_ref[0]
    a, b = iota((PEERS, PEERS), 0), iota((PEERS, PEERS), 1)
    later = dot(jnp.where(b > here, logs, 0.0), ones_where(a < b, F32), 1, 0, EXACT)
    before = dot(jnp.where(b < here, logs, 0.0), ones_where(a > b, F32), 1, 0, EXACT)
    later = jnp.where(b > here, jnp.exp(later), 0.0)
    before = jnp.where(b < here, jnp.exp(before), 0.0)
    lane = iota((KEY_DIM, WIDTH), 1)
    for k in range(PEERS):
        reach_ref[k] = jnp.where(lane < VAL_DIM, later[:, k : k + 1], before[:, k : k + 1])


def source_kernel(
    rows_ref, weight_ref, normed_ref, inv_ref, mix_ref, query_fwd_ref, query_bwd_ref,
    send_ref, grad_ref,
):
    rows = jnp.concatenate([rows_ref[c, k] for k in range(RING) for c in range(2)], axis=1)
    grad = dot(rows, weight_ref[...], 1, 1)
    normed = normed_ref[...]
    mean = jnp.mean(grad * normed, axis=1, keepdims=True)
    grad = inv_ref[...] * (grad - normed * mean)
    grad_ref[...] = grad
    state = jnp.concatenate(
        [
            dot(query_fwd_ref[...], grad, 1, 0, EXACT),
            dot(query_bwd_ref[...], grad, 1, 0, EXACT),
        ],
        axis=1,
    ).astype(BF16)
    lane = iota((KEY_DIM, WIDTH), 1)
    for k in range(2 * RING):
        part = dot(rows[:, k * WIDTH : (k + 1) * WIDTH], mix_ref[...], 0, 0)
        for half in range(2):
            at = half * VAL_DIM
            both = jnp.where(lane < VAL_DIM, part[at : at + 32], part[at + 32 : at + 64])
            send_ref[2 * k + half, :KEY_DIM] = both.astype(BF16)
            send_ref[2 * k + half, KEY_DIM:] = state


def final_kernel(
    got_ref, reach_ref, state_ref, cum_ref, key_ref, val_ref, pre_ref, speed_ref,
    keys_mix_ref, vals_mix_ref, decay_mix_ref,
    proj_ref, keys_ref, vals_ref, logit_ref,
):
    proj = got_ref[0, :KEY_DIM].astype(F32)
    flow = got_ref[0, KEY_DIM:].astype(F32) * reach_ref[0]
    for k in range(1, PEERS):
        proj = proj + got_ref[k, :KEY_DIM].astype(F32)
        flow = flow + got_ref[k, KEY_DIM:].astype(F32) * reach_ref[k]
    proj_ref[:KEY_DIM] = proj[:, :VAL_DIM]
    proj_ref[KEY_DIM:] = proj[:, VAL_DIM:]
    cum = cum_ref[...]
    total = cum[:, TOK - 1 : TOK]
    keys, vals = key_ref[...].astype(F32), val_ref[...].astype(F32)
    scale_fwd, scale_bwd = jnp.exp(total - cum), jnp.exp(cum)
    flow_fwd, flow_bwd = flow[:, :VAL_DIM], flow[:, VAL_DIM:]
    grad_fwd = dot(flow_fwd, vals, 1, 0, EXACT) * scale_fwd
    grad_bwd = dot(flow_bwd, vals, 1, 0, EXACT) * scale_bwd
    keys_ref[...] = keys_mix_ref[...] + grad_fwd + grad_bwd
    vals_ref[...] = (
        vals_mix_ref[...]
        + dot(flow_fwd, keys * scale_fwd, 0, 0, EXACT)
        + dot(flow_bwd, keys * scale_bwd, 0, 0, EXACT)
    )
    factor = jnp.exp(total) * jnp.sum(flow * state_ref[...], axis=1, keepdims=True)
    grad_fwd, grad_bwd = grad_fwd * keys, grad_bwd * keys
    at_end = factor + jnp.sum(grad_fwd, axis=1, keepdims=True)
    row, col = iota((TOK, TOK), 0), iota((TOK, TOK), 1)
    tail = dot(grad_bwd - grad_fwd, ones_where(row >= col, F32), 1, 0, EXACT)
    decay = decay_mix_ref[...] + tail + at_end
    diagonal = iota((KEY_DIM, KEY_DIM), 0) == iota((KEY_DIM, KEY_DIM), 1)
    speed = jnp.sum(jnp.where(diagonal, speed_ref[...], 0.0), axis=1, keepdims=True)
    pre = pre_ref[...].astype(F32)
    logit_ref[...] = decay * speed * jax.nn.sigmoid(-pre)


SCALAR = pl.BlockSpec(memory_space=pltpu.SMEM)
WHOLE = pl.BlockSpec(memory_space=pltpu.VMEM)


def on_chip(array):
    return pltpu.with_memory_space_constraint(array, pltpu.VMEM)


def off_chip(array):
    return pltpu.with_memory_space_constraint(array, pltpu.HBM)


def call(kernel, outs, *args, scalars=0, stored=()):
    shapes = [
        (jax.ShapeDtypeStruct if k in stored else pltpu.VMEM)(shape, dtype)
        for k, (shape, dtype) in enumerate(outs)
    ]
    return pl.pallas_call(
        kernel,
        out_shape=shapes,
        in_specs=[SCALAR] * scalars + [WHOLE] * (len(args) - scalars),
        out_specs=[WHOLE] * len(shapes),
        compiler_params=pltpu.CompilerParams(vmem_limit_bytes=24 << 20),
    )(*args)


def inner(scaled, keys, vals, cum):
    row, col = iota((TOK, TOK), 0), iota((TOK, TOK), 1)
    gap = cum[:, :, None] - cum[:, None, :]
    weight = jnp.exp(jnp.where(row >= col, gap, -gap))
    scores = jnp.einsum("ct,cs,cts->ts", scaled, keys, weight)
    return jnp.einsum("ts,vs->vt", scores, vals)


def carried(scaled, cum, fwd_in, bwd_in):
    total = cum[:, -1:]
    return jnp.einsum("ct,cv->vt", scaled * jnp.exp(cum), fwd_in) + jnp.einsum(
        "ct,cv->vt", scaled * jnp.exp(total - cum), bwd_in
    )


def body(
    queries,
    input_key_matrix,
    input_value_matrix,
    decay_preactivation,
    extra_log_decay,
    channel_decay_speed,
    output_weight_matrix,
    stored_expert_rows,
    chosen_expert_index,
    expert_combine_weight,
    cotangent,
    expert_gate_weight,
    expert_up_weight,
    expert_down_weight,
):
    sp = ("z", "x")
    core = lax.axis_index("core")
    core_at = core.reshape(1).astype(jnp.int32)
    place_at = lax.axis_index(sp).reshape(1).astype(jnp.int32)
    speed = channel_decay_speed.reshape(1, KEY_DIM)
    swap = [(0, 1), (1, 0)]

    def exchanged(array, axis):
        return lax.all_to_all(array, axis, split_axis=0, concat_axis=0, tiled=True)

    gate, up, down = expert_gate_weight[0], expert_up_weight[0], expert_down_weight[0]
    gate_blocks = gate.reshape(2 * RING, WIDTH, WIDTH)
    up_blocks = up.reshape(2 * RING, WIDTH, WIDTH)
    send, pick, cum = call(
        dispatch_kernel,
        [((PEERS, PAD, 2 * WIDTH), BF16), ((SLOTS, TOK), BF16), ((KEY_DIM, TOK), F32)],
        off_chip(chosen_expert_index.T),
        off_chip(expert_combine_weight.T),
        off_chip(stored_expert_rows),
        off_chip(cotangent),
        off_chip(input_key_matrix),
        off_chip(input_value_matrix),
        off_chip(decay_preactivation),
        off_chip(extra_log_decay),
        off_chip(speed),
    )
    got = on_chip(exchanged(send, sp))
    rows_x, copies, back = call(
        arrival_kernel,
        [((ROWS, WIDTH), BF16), ((RING, ROWS, WIDTH), BF16), ((PEERS, PAD, WIDTH), BF16)],
        got,
    )
    own_y = exchanged(copies, "y")
    own_x = lax.all_gather(rows_x, "y", axis=0, tiled=False)

    theirs = jnp.stack(
        [
            lax.dynamic_index_in_dim(
                w.reshape(RING, 2, WIDTH, WIDTH), 1 - core, axis=1, keepdims=False
            )
            for w in (gate, up)
        ]
    )
    swapped = lax.ppermute(theirs, "core", swap)

    other_x = lax.ppermute(own_x, "core", swap)
    other_y = lax.ppermute(own_y, "core", swap)
    (pre,) = call(
        forward_kernel,
        [((ROWS, 2 * WIDTH), F32)],
        core_at,
        own_x,
        other_x,
        gate_blocks,
        up_blocks,
        scalars=1,
    )
    grads, hidden = call(
        hidden_kernel,
        [((ROWS, 2 * WIDTH), BF16), ((ROWS, WIDTH), BF16)],
        core_at,
        own_y,
        other_y,
        down,
        pre,
        scalars=1,
    )
    grads_both = lax.all_gather(grads, "core", axis=0, tiled=False)
    (partials,) = call(
        partial_kernel,
        [((RING, ROWS, WIDTH), BF16)],
        core_at,
        on_chip(grads_both),
        gate_blocks,
        up_blocks,
        swapped,
        scalars=1,
    )
    parts = exchanged(partials, "y")
    (send,) = call(return_kernel, [((PEERS, PAD, WIDTH), BF16)], on_chip(parts), on_chip(back))
    returned = on_chip(exchanged(send, sp))
    (copies,) = call(
        token_kernel, [((RING, TOK, WIDTH), BF16)], returned, pick, cotangent
    )
    cum, copies = lax.optimization_barrier((cum, copies))
    full_rows = exchanged(copies, "y")
    full_rows = lax.all_gather(full_rows, "core", axis=0, tiled=False)

    state, reach = call(
        state_kernel,
        [((KEY_DIM, WIDTH), F32), ((PEERS, KEY_DIM, WIDTH), F32)],
        place_at,
        returned,
        scalars=1,
    )
    scaled = queries.astype(F32) * KEY_DIM ** (-0.5)
    keys = input_key_matrix.astype(F32)
    vals = input_value_matrix.astype(F32)
    fwd_in, bwd_in = state[:, :VAL_DIM], state[:, VAL_DIM:]
    inner_out, pull_inner = jax.vjp(inner, scaled, keys, vals, cum)
    carried_out, pull_carried = jax.vjp(
        lambda s, c: carried(s, c, fwd_in, bwd_in), scaled, cum
    )
    mixed = inner_out + carried_out
    inv_rms = lax.rsqrt(jnp.mean(mixed * mixed, axis=0, keepdims=True) + 1e-06)
    normed = mixed * inv_rms
    normed_t = normed.T
    mix_t = normed_t.astype(BF16)
    send, grad_mixed_t = call(
        source_kernel,
        [((PEERS, 2 * KEY_DIM, WIDTH), BF16), ((TOK, VAL_DIM), F32)],
        on_chip(full_rows),
        output_weight_matrix.T,
        normed_t,
        inv_rms.reshape(TOK, 1),
        jnp.concatenate([mix_t, mix_t], axis=1),
        scaled * jnp.exp(cum),
        scaled * jnp.exp(cum[:, -1:] - cum),
    )
    send, grads, hidden = lax.optimization_barrier((send, grads, hidden))
    got = exchanged(send, sp)
    grad_gate, grad_up, grad_down = call(
        weight_kernel,
        [
            ((2 * RING, WIDTH, WIDTH), BF16),
            ((2 * RING, WIDTH, WIDTH), BF16),
            ((WIDTH, MODEL), BF16),
        ],
        core_at,
        own_x,
        other_x,
        own_y,
        other_y,
        grads,
        hidden,
        scalars=1,
        stored=range(3),
    )
    grad_mixed = grad_mixed_t.T
    grad_scaled, grad_keys, grad_vals, grad_cum = pull_inner(grad_mixed)
    grad_scaled_in, grad_cum_in = pull_carried(grad_mixed)
    grad_queries = (grad_scaled + grad_scaled_in) * KEY_DIM ** (-0.5)
    tail_mask = ones_where(iota((TOK, TOK), 0) >= iota((TOK, TOK), 1), F32)
    grad_decay = dot(grad_cum + grad_cum_in, tail_mask, 1, 0, EXACT)
    grad_out_proj, grad_keys, grad_values, grad_logit = call(
        final_kernel,
        [
            ((2 * KEY_DIM, VAL_DIM), F32),
            ((KEY_DIM, TOK), F32),
            ((VAL_DIM, TOK), F32),
            ((KEY_DIM, TOK), F32),
        ],
        on_chip(got),
        reach,
        state,
        cum,
        input_key_matrix,
        input_value_matrix,
        decay_preactivation,
        speed,
        grad_keys,
        grad_vals,
        grad_decay,
        stored=range(4),
    )
    return (
        grad_queries,
        grad_keys,
        grad_values,
        grad_logit,
        grad_out_proj,
        grad_gate.reshape(1, MODEL, WIDTH),
        grad_up.reshape(1, MODEL, WIDTH),
        grad_down[None],
    )


def solution(mesh):
    fine = Mesh(mesh.devices.reshape(8, 4, 8, 2), ("z", "x", "y", "core"))
    sp, tp = ("z", "x"), ("y", "core")
    in_specs = (
        P(tp, sp),
        P(tp, sp),
        P(tp, sp),
        P(tp, sp),
        P(tp, sp),
        P(tp),
        P(None, tp),
        P(sp, tp),
        P(sp, None),
        P(sp, None),
        P(sp, tp),
        P(sp, None, tp),
        P(sp, None, tp),
        P(sp, tp, None),
    )
    out_specs = (
        P(tp, sp),
        P(tp, sp),
        P(tp, sp),
        P(tp, sp),
        P(sp, tp),
        P(sp, None, tp),
        P(sp, None, tp),
        P(sp, tp, None),
    )
    return jax.shard_map(body, mesh=fine, in_specs=in_specs, out_specs=out_specs, check_vma=False)
```

```python
import jax
import jax.numpy as jnp
from jax import lax
from jax.experimental import pallas as pl
from jax.experimental.pallas import tpu as pltpu
from jax.sharding import Mesh
from jax.sharding import PartitionSpec as P

KEY_DIM = 32
VAL_DIM = 64
TOK = 128
PEERS = 32
CAP = 12
PAD = 16
RING = 8
SLOTS = PEERS * PAD
ROWS = PEERS * CAP
HALF = ROWS // 2
WIDTH = 128
MODEL = 2048

F32 = jnp.float32
BF16 = jnp.bfloat16
EXACT = lax.Precision.HIGHEST


def dot(a, b, da, db, precision=None):
    return lax.dot_general(
        a, b, (((da,), (db,)), ((), ())), preferred_element_type=F32, precision=precision
    )


def iota(shape, dim):
    return lax.broadcasted_iota(jnp.int32, shape, dim)


def ones_where(mask, dtype=BF16):
    return jnp.where(mask, 1.0, 0.0).astype(dtype)


def split_two(value):
    high = value.astype(BF16).astype(F32)
    return high, (value - high).astype(BF16).astype(F32)


def split_three(value):
    high, rest = split_two(value)
    return high, rest, (value - high - rest).astype(BF16).astype(F32)


def compact_rows(shape, compact_dim):
    row = iota(shape, compact_dim)
    peer = (row * 5462) >> 16
    return peer * PAD + (row - peer * CAP) == iota(shape, 1 - compact_dim)


def row_of_peer(place):
    return iota((PEERS, SLOTS), 1) == iota((PEERS, SLOTS), 0) * PAD + place


def dispatch_kernel(
    ids_ref, share_ref, x_ref, cot_ref, key_ref, val_ref, pre_ref, extra_ref, speed_ref,
    send_ref, pick_ref, cum_ref,
):
    expert = iota((PEERS, TOK), 0)
    named = [ids_ref[k : k + 1, :] == expert for k in range(2)]
    row, col = iota((TOK, TOK), 0), iota((TOK, TOK), 1)
    rank = dot(ones_where(named[0] | named[1]), ones_where(row < col), 1, 0)
    place = iota((PEERS, PAD, TOK), 1).astype(F32)
    cot = cot_ref[...].astype(F32)
    picks, grads = [], None
    for k in range(2):
        at = jnp.where(named[k], rank, -1.0)
        pick = jnp.where(at[:, None, :] == place, 1.0, 0.0).reshape(SLOTS, TOK).astype(BF16)
        share = jnp.sum(jnp.where(row == col, share_ref[k : k + 1, :], 0.0), axis=1, keepdims=True)
        part = dot(pick, (share * cot).astype(BF16), 1, 0)
        grads = part if grads is None else grads + part
        picks.append(pick)
    pick = picks[0] + picks[1]
    pick_ref[...] = pick
    rows = jnp.concatenate([dot(pick, x_ref[...], 1, 0), grads], axis=1)

    pre = pre_ref[...].astype(F32)
    log_sig = jnp.minimum(pre, 0.0) - jnp.log1p(jnp.exp(-jnp.abs(pre)))
    diagonal = iota((KEY_DIM, KEY_DIM), 0) == iota((KEY_DIM, KEY_DIM), 1)
    speed = jnp.sum(jnp.where(diagonal, speed_ref[...], 0.0), axis=1, keepdims=True)
    decay = speed * log_sig + extra_ref[...]
    cum = dot(decay, ones_where(row <= col, F32), 1, 0, EXACT)
    cum_ref[...] = cum
    total = cum[:, TOK - 1 : TOK]
    keys, vals = key_ref[...].astype(F32), val_ref[...].astype(F32)
    sums = jnp.concatenate(
        [
            dot(keys * jnp.exp(total - cum), vals, 1, 1, EXACT),
            dot(keys * jnp.exp(cum), vals, 1, 1, EXACT),
        ],
        axis=1,
    )
    state = jnp.concatenate(split_two(sums), axis=1)
    lane = iota((KEY_DIM, 2 * WIDTH), 1)
    logs = jnp.zeros((KEY_DIM, 2 * WIDTH), F32)
    for k, part in enumerate(split_three(total)):
        logs = jnp.where(lane == k, part, logs)
    place = iota((PEERS, PAD, 2 * WIDTH), 1)
    block = rows.reshape(PEERS, PAD, 2 * WIDTH)
    block = jnp.where(place == CAP, state[:, None, :], block)
    block = jnp.where(place == CAP + 1, logs[:, None, :], block)
    send_ref[...] = block.astype(BF16)


def arrival_kernel(got_ref, first_ref, second_ref, back_ref):
    got = got_ref[...].reshape(SLOTS, 2 * WIDTH)
    rows = dot(ones_where(compact_rows((ROWS, SLOTS), 0)), got, 1, 0).astype(BF16)
    for k in range(RING):
        first_ref[k] = rows[:HALF]
        second_ref[k] = rows[HALF:]
    both = dot(ones_where(row_of_peer(CAP)), got, 1, 0)
    state = both[:, :WIDTH] + both[:, WIDTH:]
    logs = dot(ones_where(row_of_peer(CAP + 1)), got, 1, 0)
    log = jnp.sum(logs, axis=1, keepdims=True)
    a, b = iota((PEERS, PEERS), 0), iota((PEERS, PEERS), 1)
    gap_fwd = dot(ones_where(b < a, F32), jnp.where(a > b, log, 0.0), 1, 0, EXACT)
    gap_bwd = dot(ones_where(b > a, F32), jnp.where(a < b, log, 0.0), 1, 0, EXACT)
    fwd = dot(jnp.where(b < a, jnp.exp(gap_fwd), 0.0), state, 1, 0, EXACT)
    bwd = dot(jnp.where(b > a, jnp.exp(gap_bwd), 0.0), state, 1, 0, EXACT)
    lane = iota((PEERS, WIDTH), 1)
    high, low = split_two(jnp.where(lane < VAL_DIM, fwd, bwd))
    peer = iota((PEERS, WIDTH), 0)
    spread = jnp.zeros((PEERS, WIDTH), F32)
    for k, part in enumerate(split_three(log)):
        spread = jnp.where(lane == peer + k * PEERS, part, spread)
    all_logs = jnp.sum(spread, axis=0, keepdims=True)
    place = iota((PEERS, PAD, WIDTH), 1)
    block = jnp.where(place == CAP, high[:, None, :], 0.0)
    block = jnp.where(place == CAP + 1, low[:, None, :], block)
    block = jnp.where(place == CAP + 2, all_logs[:, None, :], block)
    back_ref[...] = block.astype(BF16)


def expert_kernel(
    core_ref, own_ref, other_ref, gate_ref, up_ref, down_ref, grads_ref, hidden_ref
):
    core = core_ref[0]
    pre = jnp.zeros((HALF, 2 * WIDTH), F32)
    grad_hidden = jnp.zeros((HALF, WIDTH), F32)
    for k in range(RING):
        for side, ref in ((core, own_ref), (1 - core, other_ref)):
            at = 2 * k + side
            weights = jnp.concatenate([gate_ref[at], up_ref[at]], axis=1)
            pre = pre + dot(ref[k, :, :WIDTH], weights, 1, 0)
            lanes = pl.ds(pl.multiple_of(at * WIDTH, WIDTH), WIDTH)
            grad_hidden = grad_hidden + dot(ref[k, :, WIDTH:], down_ref[:, lanes], 1, 1)
    gate_pre, up_pre = pre[:, :WIDTH], pre[:, WIDTH:]
    gate_sig = jax.nn.sigmoid(gate_pre)
    gate_act = gate_pre * gate_sig
    hidden_ref[...] = (gate_act * up_pre).astype(BF16)
    grads_ref[:, :WIDTH] = (
        grad_hidden * up_pre * gate_sig * (1.0 + gate_pre * (1.0 - gate_sig))
    ).astype(BF16)
    grads_ref[:, WIDTH:] = (grad_hidden * gate_act).astype(BF16)


def weight_kernel(
    core_ref, own_a_ref, other_a_ref, own_b_ref, other_b_ref,
    grads_a_ref, grads_b_ref, hidden_a_ref, hidden_b_ref,
    gate_ref, up_ref, down_ref,
):
    core = core_ref[0]
    grads = (grads_a_ref[...], grads_b_ref[...])
    hidden = (hidden_a_ref[...], hidden_b_ref[...])
    for k in range(RING):
        for side, rows in (
            (core, (own_a_ref, own_b_ref)),
            (1 - core, (other_a_ref, other_b_ref)),
        ):
            at = 2 * k + side
            both, down = (
                sum(dot(r[k, :, :WIDTH], g, 0, 0) for r, g in zip(rows, grads)),
                sum(dot(h, r[k, :, WIDTH:], 0, 0) for r, h in zip(rows, hidden)),
            )
            gate_ref[at] = both[:, :WIDTH].astype(BF16)
            up_ref[at] = both[:, WIDTH:].astype(BF16)
            lanes = pl.ds(pl.multiple_of(at * WIDTH, WIDTH), WIDTH)
            down_ref[:, lanes] = down.astype(BF16)


def partial_kernel(core_ref, grads_ref, gate_ref, up_ref, swapped_ref, out_ref):
    core = core_ref[0]
    both = jnp.concatenate([grads_ref[core], grads_ref[1 - core]], axis=1)
    for k in range(RING):
        at = 2 * k + core
        weights = jnp.concatenate(
            [gate_ref[at], up_ref[at], swapped_ref[0, k], swapped_ref[1, k]], axis=1
        )
        out_ref[k] = dot(both, weights, 1, 1).astype(BF16)


def return_kernel(first_ref, second_ref, back_ref, send_ref):
    halves = []
    for ref in (first_ref, second_ref):
        total = ref[0].astype(F32)
        for k in range(1, RING):
            total = total + ref[k].astype(F32)
        halves.append(total.astype(BF16))
    total = jnp.concatenate(halves, axis=0)
    rows = dot(ones_where(compact_rows((SLOTS, ROWS), 1)), total, 1, 0)
    rows = rows.astype(BF16).reshape(PEERS, PAD, WIDTH)
    send_ref[...] = rows + back_ref[...]


def token_kernel(got_ref, pick_ref, cot_ref, copies_ref):
    got = got_ref[...].reshape(SLOTS, WIDTH)
    rows = (cot_ref[...].astype(F32) + dot(pick_ref[...], got, 0, 0)).astype(BF16)
    for k in range(RING):
        copies_ref[k] = rows


def state_kernel(place_ref, got_ref, state_ref, reach_ref):
    got = got_ref[...].reshape(SLOTS, WIDTH)
    state_ref[...] = dot(ones_where(row_of_peer(CAP) | row_of_peer(CAP + 1)), got, 1, 0)
    spread = dot(ones_where(row_of_peer(CAP + 2)), got, 1, 0).astype(BF16)
    lane, peer = iota((WIDTH, PEERS), 0), iota((WIDTH, PEERS), 1)
    fold = (lane == peer) | (lane == peer + PEERS) | (lane == peer + 2 * PEERS)
    logs = dot(spread, ones_where(fold), 1, 0)
    here = place_ref[0]
    a, b = iota((PEERS, PEERS), 0), iota((PEERS, PEERS), 1)
    later = dot(jnp.where(b > here, logs, 0.0), ones_where(a < b, F32), 1, 0, EXACT)
    before = dot(jnp.where(b < here, logs, 0.0), ones_where(a > b, F32), 1, 0, EXACT)
    later = jnp.where(b > here, jnp.exp(later), 0.0)
    before = jnp.where(b < here, jnp.exp(before), 0.0)
    lane = iota((KEY_DIM, WIDTH), 1)
    for k in range(PEERS):
        reach_ref[k] = jnp.where(lane < VAL_DIM, later[:, k : k + 1], before[:, k : k + 1])


def source_kernel(
    rows_ref, weight_ref, normed_ref, inv_ref, mix_ref, query_fwd_ref, query_bwd_ref,
    send_ref, grad_ref,
):
    rows = jnp.concatenate([rows_ref[c, k] for k in range(RING) for c in range(2)], axis=1)
    grad = dot(rows, weight_ref[...], 1, 1)
    normed = normed_ref[...]
    mean = jnp.mean(grad * normed, axis=1, keepdims=True)
    grad = inv_ref[...] * (grad - normed * mean)
    grad_ref[...] = grad
    state = jnp.concatenate(
        [
            dot(query_fwd_ref[...], grad, 1, 0, EXACT),
            dot(query_bwd_ref[...], grad, 1, 0, EXACT),
        ],
        axis=1,
    ).astype(BF16)
    lane = iota((KEY_DIM, WIDTH), 1)
    for k in range(2 * RING):
        part = dot(rows[:, k * WIDTH : (k + 1) * WIDTH], mix_ref[...], 0, 0)
        for half in range(2):
            at = half * VAL_DIM
            both = jnp.where(lane < VAL_DIM, part[at : at + 32], part[at + 32 : at + 64])
            send_ref[2 * k + half, :KEY_DIM] = both.astype(BF16)
            send_ref[2 * k + half, KEY_DIM:] = state


def final_kernel(
    got_ref, reach_ref, state_ref, cum_ref, key_ref, val_ref, pre_ref, speed_ref,
    keys_mix_ref, vals_mix_ref, decay_mix_ref,
    proj_ref, keys_ref, vals_ref, logit_ref,
):
    proj = got_ref[0, :KEY_DIM].astype(F32)
    flow = got_ref[0, KEY_DIM:].astype(F32) * reach_ref[0]
    for k in range(1, PEERS):
        proj = proj + got_ref[k, :KEY_DIM].astype(F32)
        flow = flow + got_ref[k, KEY_DIM:].astype(F32) * reach_ref[k]
    proj_ref[:KEY_DIM] = proj[:, :VAL_DIM]
    proj_ref[KEY_DIM:] = proj[:, VAL_DIM:]
    cum = cum_ref[...]
    total = cum[:, TOK - 1 : TOK]
    keys, vals = key_ref[...].astype(F32), val_ref[...].astype(F32)
    scale_fwd, scale_bwd = jnp.exp(total - cum), jnp.exp(cum)
    flow_fwd, flow_bwd = flow[:, :VAL_DIM], flow[:, VAL_DIM:]
    grad_fwd = dot(flow_fwd, vals, 1, 0, EXACT) * scale_fwd
    grad_bwd = dot(flow_bwd, vals, 1, 0, EXACT) * scale_bwd
    keys_ref[...] = keys_mix_ref[...] + grad_fwd + grad_bwd
    vals_ref[...] = (
        vals_mix_ref[...]
        + dot(flow_fwd, keys * scale_fwd, 0, 0, EXACT)
        + dot(flow_bwd, keys * scale_bwd, 0, 0, EXACT)
    )
    factor = jnp.exp(total) * jnp.sum(flow * state_ref[...], axis=1, keepdims=True)
    grad_fwd, grad_bwd = grad_fwd * keys, grad_bwd * keys
    at_end = factor + jnp.sum(grad_fwd, axis=1, keepdims=True)
    row, col = iota((TOK, TOK), 0), iota((TOK, TOK), 1)
    tail = dot(grad_bwd - grad_fwd, ones_where(row >= col, F32), 1, 0, EXACT)
    decay = decay_mix_ref[...] + tail + at_end
    diagonal = iota((KEY_DIM, KEY_DIM), 0) == iota((KEY_DIM, KEY_DIM), 1)
    speed = jnp.sum(jnp.where(diagonal, speed_ref[...], 0.0), axis=1, keepdims=True)
    pre = pre_ref[...].astype(F32)
    logit_ref[...] = decay * speed * jax.nn.sigmoid(-pre)


SCALAR = pl.BlockSpec(memory_space=pltpu.SMEM)
WHOLE = pl.BlockSpec(memory_space=pltpu.VMEM)


def on_chip(array):
    return pltpu.with_memory_space_constraint(array, pltpu.VMEM)


def off_chip(array):
    return pltpu.with_memory_space_constraint(array, pltpu.HBM)


def call(kernel, outs, *args, scalars=0, stored=()):
    shapes = [
        (pltpu.HBM if k in stored else pltpu.VMEM)(shape, dtype)
        for k, (shape, dtype) in enumerate(outs)
    ]
    return pl.pallas_call(
        kernel,
        out_shape=shapes,
        in_specs=[SCALAR] * scalars + [WHOLE] * (len(args) - scalars),
        out_specs=[WHOLE] * len(shapes),
        compiler_params=pltpu.CompilerParams(vmem_limit_bytes=24 << 20),
    )(*args)


def inner(scaled, keys, vals, cum):
    row, col = iota((TOK, TOK), 0), iota((TOK, TOK), 1)
    gap = cum[:, :, None] - cum[:, None, :]
    weight = jnp.exp(jnp.where(row >= col, gap, -gap))
    scores = jnp.einsum("ct,cs,cts->ts", scaled, keys, weight)
    return jnp.einsum("ts,vs->vt", scores, vals)


def carried(scaled, cum, fwd_in, bwd_in):
    total = cum[:, -1:]
    return jnp.einsum("ct,cv->vt", scaled * jnp.exp(cum), fwd_in) + jnp.einsum(
        "ct,cv->vt", scaled * jnp.exp(total - cum), bwd_in
    )


def body(
    queries,
    input_key_matrix,
    input_value_matrix,
    decay_preactivation,
    extra_log_decay,
    channel_decay_speed,
    output_weight_matrix,
    stored_expert_rows,
    chosen_expert_index,
    expert_combine_weight,
    cotangent,
    expert_gate_weight,
    expert_up_weight,
    expert_down_weight,
):
    sp = ("z", "x")
    core = lax.axis_index("core")
    core_at = core.reshape(1).astype(jnp.int32)
    place_at = lax.axis_index(sp).reshape(1).astype(jnp.int32)
    speed = channel_decay_speed.reshape(1, KEY_DIM)
    swap = [(0, 1), (1, 0)]

    def exchanged(array, axis):
        return lax.all_to_all(array, axis, split_axis=0, concat_axis=0, tiled=True)

    gate, up, down = expert_gate_weight[0], expert_up_weight[0], expert_down_weight[0]
    gate_blocks = gate.reshape(2 * RING, WIDTH, WIDTH)
    up_blocks = up.reshape(2 * RING, WIDTH, WIDTH)
    send, pick, cum = call(
        dispatch_kernel,
        [((PEERS, PAD, 2 * WIDTH), BF16), ((SLOTS, TOK), BF16), ((KEY_DIM, TOK), F32)],
        off_chip(chosen_expert_index.T),
        off_chip(expert_combine_weight.T),
        off_chip(stored_expert_rows),
        off_chip(cotangent),
        off_chip(input_key_matrix),
        off_chip(input_value_matrix),
        off_chip(decay_preactivation),
        off_chip(extra_log_decay),
        off_chip(speed),
        stored=(1,),
    )
    got = on_chip(exchanged(send, sp))
    first, second, back = call(
        arrival_kernel,
        [
            ((RING, HALF, 2 * WIDTH), BF16),
            ((RING, HALF, 2 * WIDTH), BF16),
            ((PEERS, PAD, WIDTH), BF16),
        ],
        got,
        stored=range(3),
    )
    own_a = exchanged(first, "y")
    own_b = exchanged(second, "y")
    theirs = jnp.stack(
        [
            lax.dynamic_index_in_dim(
                w.reshape(RING, 2, WIDTH, WIDTH), 1 - core, axis=1, keepdims=False
            )
            for w in (gate, up)
        ]
    )
    swapped = lax.ppermute(theirs, "core", swap)

    def expert(own):
        other = lax.ppermute(own, "core", swap)
        grads, hidden = call(
            expert_kernel,
            [((HALF, 2 * WIDTH), BF16), ((HALF, WIDTH), BF16)],
            core_at,
            off_chip(own),
            off_chip(other),
            gate_blocks,
            up_blocks,
            down,
            scalars=1,
            stored=range(2),
        )
        grads_both = lax.all_gather(grads, "core", axis=0, tiled=False)
        (partials,) = call(
            partial_kernel,
            [((RING, HALF, WIDTH), BF16)],
            core_at,
            on_chip(grads_both),
            gate_blocks,
            up_blocks,
            swapped,
            scalars=1,
            stored=(0,),
        )
        return other, grads, hidden, partials

    other_a, grads_a, hidden_a, partials_a = expert(own_a)
    own_b, partials_a = lax.optimization_barrier((own_b, partials_a))
    parts_a = exchanged(partials_a, "y")
    other_b, grads_b, hidden_b, partials_b = expert(own_b)
    parts_b = exchanged(partials_b, "y")
    (send,) = call(
        return_kernel,
        [((PEERS, PAD, WIDTH), BF16)],
        on_chip(parts_a),
        on_chip(parts_b),
        off_chip(back),
    )
    returned = on_chip(exchanged(send, sp))
    (copies,) = call(
        token_kernel, [((RING, TOK, WIDTH), BF16)], returned, off_chip(pick), off_chip(cotangent)
    )
    cum, copies = lax.optimization_barrier((cum, copies))
    full_rows = exchanged(copies, "y")
    full_rows = lax.all_gather(full_rows, "core", axis=0, tiled=False)

    state, reach = call(
        state_kernel,
        [((KEY_DIM, WIDTH), F32), ((PEERS, KEY_DIM, WIDTH), F32)],
        place_at,
        returned,
        scalars=1,
    )
    scaled = queries.astype(F32) * KEY_DIM ** (-0.5)
    keys = input_key_matrix.astype(F32)
    vals = input_value_matrix.astype(F32)
    fwd_in, bwd_in = state[:, :VAL_DIM], state[:, VAL_DIM:]
    inner_out, pull_inner = jax.vjp(inner, scaled, keys, vals, cum)
    carried_out, pull_carried = jax.vjp(
        lambda s, c: carried(s, c, fwd_in, bwd_in), scaled, cum
    )
    mixed = inner_out + carried_out
    inv_rms = lax.rsqrt(jnp.mean(mixed * mixed, axis=0, keepdims=True) + 1e-06)
    normed = mixed * inv_rms
    normed_t = normed.T
    mix_t = normed_t.astype(BF16)
    send, grad_mixed_t = call(
        source_kernel,
        [((PEERS, 2 * KEY_DIM, WIDTH), BF16), ((TOK, VAL_DIM), F32)],
        on_chip(full_rows),
        off_chip(output_weight_matrix.T),
        normed_t,
        inv_rms.reshape(TOK, 1),
        jnp.concatenate([mix_t, mix_t], axis=1),
        scaled * jnp.exp(cum),
        scaled * jnp.exp(cum[:, -1:] - cum),
    )
    send, grads_a, grads_b = lax.optimization_barrier((send, grads_a, grads_b))
    got = exchanged(send, sp)
    grad_gate, grad_up, grad_down = call(
        weight_kernel,
        [
            ((2 * RING, WIDTH, WIDTH), BF16),
            ((2 * RING, WIDTH, WIDTH), BF16),
            ((WIDTH, MODEL), BF16),
        ],
        core_at,
        off_chip(own_a),
        off_chip(other_a),
        off_chip(own_b),
        off_chip(other_b),
        off_chip(grads_a),
        off_chip(grads_b),
        off_chip(hidden_a),
        off_chip(hidden_b),
        scalars=1,
        stored=range(3),
    )
    grad_mixed = grad_mixed_t.T
    grad_scaled, grad_keys, grad_vals, grad_cum = pull_inner(grad_mixed)
    grad_scaled_in, grad_cum_in = pull_carried(grad_mixed)
    grad_queries = (grad_scaled + grad_scaled_in) * KEY_DIM ** (-0.5)
    tail_mask = ones_where(iota((TOK, TOK), 0) >= iota((TOK, TOK), 1), F32)
    grad_decay = dot(grad_cum + grad_cum_in, tail_mask, 1, 0, EXACT)
    grad_out_proj, grad_keys, grad_values, grad_logit = call(
        final_kernel,
        [
            ((2 * KEY_DIM, VAL_DIM), F32),
            ((KEY_DIM, TOK), F32),
            ((VAL_DIM, TOK), F32),
            ((KEY_DIM, TOK), F32),
        ],
        on_chip(got),
        reach,
        state,
        cum,
        input_key_matrix,
        input_value_matrix,
        decay_preactivation,
        speed,
        grad_keys,
        grad_vals,
        grad_decay,
        stored=range(4),
    )
    return (
        grad_queries,
        grad_keys,
        grad_values,
        grad_logit,
        grad_out_proj,
        grad_gate.reshape(1, MODEL, WIDTH),
        grad_up.reshape(1, MODEL, WIDTH),
        grad_down[None],
    )


def solution(mesh):
    fine = Mesh(mesh.devices.reshape(8, 4, 8, 2), ("z", "x", "y", "core"))
    sp, tp = ("z", "x"), ("y", "core")
    in_specs = (
        P(tp, sp),
        P(tp, sp),
        P(tp, sp),
        P(tp, sp),
        P(tp, sp),
        P(tp),
        P(None, tp),
        P(sp, tp),
        P(sp, None),
        P(sp, None),
        P(sp, tp),
        P(sp, None, tp),
        P(sp, None, tp),
        P(sp, tp, None),
    )
    out_specs = (
        P(tp, sp),
        P(tp, sp),
        P(tp, sp),
        P(tp, sp),
        P(sp, tp),
        P(sp, None, tp),
        P(sp, None, tp),
        P(sp, tp, None),
    )
    return jax.shard_map(body, mesh=fine, in_specs=in_specs, out_specs=out_specs, check_vma=False)
```

```python
import jax
import jax.numpy as jnp
from jax import lax
from jax.experimental import pallas as pl
from jax.experimental.pallas import tpu as pltpu
from jax.sharding import Mesh
from jax.sharding import PartitionSpec as P


KEY_DIM = 32
VAL_DIM = 64
TOK = 128
PEERS = 32
CAP = 12
PAD = 16
RING = 8
SLOTS = PEERS * PAD
ROWS = PEERS * CAP
WIDTH = 128
MODEL = 2048

F32 = jnp.float32
BF16 = jnp.bfloat16
EXACT = lax.Precision.HIGHEST


def dot(a, b, da, db, precision=None):
    return lax.dot_general(
        a, b, (((da,), (db,)), ((), ())), preferred_element_type=F32, precision=precision
    )


def iota(shape, dim):
    return lax.broadcasted_iota(jnp.int32, shape, dim)


def ones_where(mask, dtype=BF16):
    return jnp.where(mask, 1.0, 0.0).astype(dtype)


def split_two(value):
    high = value.astype(BF16).astype(F32)
    return high, (value - high).astype(BF16).astype(F32)


def split_three(value):
    high, rest = split_two(value)
    return high, rest, (value - high - rest).astype(BF16).astype(F32)


def compact_rows(shape, compact_dim):
    row = iota(shape, compact_dim)
    peer = (row * 5462) >> 16
    return peer * PAD + (row - peer * CAP) == iota(shape, 1 - compact_dim)


def row_of_peer(place):
    return iota((PEERS, SLOTS), 1) == iota((PEERS, SLOTS), 0) * PAD + place


def dispatch_kernel(
    ids_ref, share_ref, x_ref, cot_ref, key_ref, val_ref, pre_ref, extra_ref, speed_ref,
    send_ref, pick_ref, cum_ref,
):
    expert = iota((PEERS, TOK), 0)
    named = [ids_ref[k : k + 1, :] == expert for k in range(2)]
    row, col = iota((TOK, TOK), 0), iota((TOK, TOK), 1)
    rank = dot(ones_where(named[0] | named[1]), ones_where(row < col), 1, 0)
    place = iota((PEERS, PAD, TOK), 1).astype(F32)
    cot = cot_ref[...].astype(F32)
    picks, grads = [], None
    for k in range(2):
        at = jnp.where(named[k], rank, -1.0)
        pick = jnp.where(at[:, None, :] == place, 1.0, 0.0).reshape(SLOTS, TOK).astype(BF16)
        share = jnp.sum(jnp.where(row == col, share_ref[k : k + 1, :], 0.0), axis=1, keepdims=True)
        part = dot(pick, (share * cot).astype(BF16), 1, 0)
        grads = part if grads is None else grads + part
        picks.append(pick)
    pick = picks[0] + picks[1]
    pick_ref[...] = pick
    rows = jnp.concatenate([dot(pick, x_ref[...], 1, 0), grads], axis=1)

    pre = pre_ref[...].astype(F32)
    log_sig = jnp.minimum(pre, 0.0) - jnp.log1p(jnp.exp(-jnp.abs(pre)))
    diagonal = iota((KEY_DIM, KEY_DIM), 0) == iota((KEY_DIM, KEY_DIM), 1)
    speed = jnp.sum(jnp.where(diagonal, speed_ref[...], 0.0), axis=1, keepdims=True)
    decay = speed * log_sig + extra_ref[...]
    cum = dot(decay, ones_where(row <= col, F32), 1, 0, EXACT)
    cum_ref[...] = cum
    total = cum[:, TOK - 1 : TOK]
    keys, vals = key_ref[...].astype(F32), val_ref[...].astype(F32)
    sums = jnp.concatenate(
        [
            dot(keys * jnp.exp(total - cum), vals, 1, 1, EXACT),
            dot(keys * jnp.exp(cum), vals, 1, 1, EXACT),
        ],
        axis=1,
    )
    state = jnp.concatenate(split_two(sums), axis=1)
    lane = iota((KEY_DIM, 2 * WIDTH), 1)
    logs = jnp.zeros((KEY_DIM, 2 * WIDTH), F32)
    for k, part in enumerate(split_three(total)):
        logs = jnp.where(lane == k, part, logs)
    place = iota((PEERS, PAD, 2 * WIDTH), 1)
    block = rows.reshape(PEERS, PAD, 2 * WIDTH)
    block = jnp.where(place == CAP, state[:, None, :], block)
    block = jnp.where(place == CAP + 1, logs[:, None, :], block)
    send_ref[...] = block.astype(BF16)


def arrival_kernel(got_ref, copies_ref, back_ref):
    got = got_ref[...].reshape(SLOTS, 2 * WIDTH)
    rows = dot(ones_where(compact_rows((ROWS, SLOTS), 0)), got, 1, 0).astype(BF16)
    for k in range(RING):
        copies_ref[k] = rows
    both = dot(ones_where(row_of_peer(CAP)), got, 1, 0)
    state = both[:, :WIDTH] + both[:, WIDTH:]
    logs = dot(ones_where(row_of_peer(CAP + 1)), got, 1, 0)
    log = jnp.sum(logs, axis=1, keepdims=True)
    a, b = iota((PEERS, PEERS), 0), iota((PEERS, PEERS), 1)
    gap_fwd = dot(ones_where(b < a, F32), jnp.where(a > b, log, 0.0), 1, 0, EXACT)
    gap_bwd = dot(ones_where(b > a, F32), jnp.where(a < b, log, 0.0), 1, 0, EXACT)
    fwd = dot(jnp.where(b < a, jnp.exp(gap_fwd), 0.0), state, 1, 0, EXACT)
    bwd = dot(jnp.where(b > a, jnp.exp(gap_bwd), 0.0), state, 1, 0, EXACT)
    lane = iota((PEERS, WIDTH), 1)
    high, low = split_two(jnp.where(lane < VAL_DIM, fwd, bwd))
    peer = iota((PEERS, WIDTH), 0)
    spread = jnp.zeros((PEERS, WIDTH), F32)
    for k, part in enumerate(split_three(log)):
        spread = jnp.where(lane == peer + k * PEERS, part, spread)
    all_logs = jnp.sum(spread, axis=0, keepdims=True)
    place = iota((PEERS, PAD, WIDTH), 1)
    block = jnp.where(place == CAP, high[:, None, :], 0.0)
    block = jnp.where(place == CAP + 1, low[:, None, :], block)
    block = jnp.where(place == CAP + 2, all_logs[:, None, :], block)
    back_ref[...] = block.astype(BF16)


def slice_kernel(core_ref, gate_ref, up_ref, down_ref, out_ref):
    other = 1 - core_ref[0]
    for k in range(RING):
        at = 2 * k + other
        out_ref[0, k] = gate_ref[at]
        out_ref[1, k] = up_ref[at]
        out_ref[2, k] = down_ref[:, pl.ds(pl.multiple_of(at * WIDTH, WIDTH), WIDTH)]


def forward_kernel(core_ref, rows_ref, gate_ref, up_ref, down_ref, swapped_ref, out_ref, send_ref):
    core = core_ref[0]
    pre = jnp.zeros((ROWS, 4 * WIDTH), F32)
    grad = jnp.zeros((ROWS, 2 * WIDTH), F32)
    for k in range(0, RING, 2):
        weights, downs = [], []
        for j in (k, k + 1):
            at = 2 * j + core
            parts = [gate_ref[at], up_ref[at], swapped_ref[0, j], swapped_ref[1, j]]
            weights.append(jnp.concatenate(parts, axis=1))
            lanes = pl.ds(pl.multiple_of(at * WIDTH, WIDTH), WIDTH)
            downs.append(jnp.concatenate([down_ref[:, lanes], swapped_ref[2, j]], axis=0))
        x = jnp.concatenate([rows_ref[k, :, :WIDTH], rows_ref[k + 1, :, :WIDTH]], axis=1)
        y = jnp.concatenate([rows_ref[k, :, WIDTH:], rows_ref[k + 1, :, WIDTH:]], axis=1)
        pre = pre + dot(x, jnp.concatenate(weights, axis=0), 1, 0)
        grad = grad + dot(y, jnp.concatenate(downs, axis=1), 1, 1)
    mine = jnp.concatenate([pre[:, : 2 * WIDTH], grad[:, :WIDTH]], axis=1)
    theirs = jnp.concatenate([pre[:, 2 * WIDTH :], grad[:, WIDTH:]], axis=1)
    out_ref[0] = mine
    out_ref[1] = theirs
    send_ref[0] = theirs.astype(BF16)
    send_ref[1] = mine.astype(BF16)


def partial_kernel(
    core_ref, own_ref, got_ref, gate_ref, up_ref, swapped_ref, out_ref, grads_ref, hidden_ref
):
    core = core_ref[0]
    grads = []
    for half in range(2):
        total = own_ref[half] + got_ref[half].astype(F32)
        gate_pre, up_pre = total[:, :WIDTH], total[:, WIDTH : 2 * WIDTH]
        grad_hidden = total[:, 2 * WIDTH :]
        gate_sig = jax.nn.sigmoid(gate_pre)
        gate_act = gate_pre * gate_sig
        hidden_ref[:, half * WIDTH : (half + 1) * WIDTH] = (gate_act * up_pre).astype(BF16)
        slope = gate_sig * (1.0 + gate_pre * (1.0 - gate_sig))
        grads.append((grad_hidden * up_pre * slope).astype(BF16))
        grads.append((grad_hidden * gate_act).astype(BF16))
    grads = jnp.concatenate(grads, axis=1)
    grads_ref[...] = grads
    for k in range(RING):
        at = 2 * k + core
        weights = jnp.concatenate(
            [gate_ref[at], up_ref[at], swapped_ref[0, k], swapped_ref[1, k]], axis=1
        )
        out_ref[k] = dot(grads, weights, 1, 1).astype(BF16)


def weight_kernel(rows_ref, grads_ref, hidden_ref, own_ref, send_ref):
    grads, hidden = grads_ref[...], hidden_ref[...]
    for k in range(RING):
        both = dot(rows_ref[k, :, :WIDTH], grads, 0, 0).astype(BF16)
        down = dot(hidden, rows_ref[k, :, WIDTH:], 0, 0).astype(BF16)
        for half, ref in enumerate((own_ref, send_ref)):
            at = 2 * half * WIDTH
            ref[0, k] = both[:, at : at + WIDTH]
            ref[1, k] = both[:, at + WIDTH : at + 2 * WIDTH]
            ref[2, k] = down[half * WIDTH : (half + 1) * WIDTH]


def joined_kernel(core_ref, own_ref, got_ref, gate_ref, up_ref, down_ref):
    core = core_ref[0]
    for k in range(RING):
        for side, ref in ((core, own_ref), (1 - core, got_ref)):
            at = 2 * k + side
            gate_ref[at] = ref[0, k]
            up_ref[at] = ref[1, k]
            down_ref[:, pl.ds(pl.multiple_of(at * WIDTH, WIDTH), WIDTH)] = ref[2, k]


def return_kernel(parts_ref, back_ref, send_ref):
    total = parts_ref[0].astype(F32)
    for k in range(1, RING):
        total = total + parts_ref[k].astype(F32)
    rows = dot(ones_where(compact_rows((SLOTS, ROWS), 1)), total.astype(BF16), 1, 0)
    rows = rows.astype(BF16).reshape(PEERS, PAD, WIDTH)
    send_ref[...] = rows + back_ref[...]


def token_kernel(got_ref, pick_ref, cot_ref, copies_ref):
    got = got_ref[...].reshape(SLOTS, WIDTH)
    rows = (cot_ref[...].astype(F32) + dot(pick_ref[...], got, 0, 0)).astype(BF16)
    for k in range(RING):
        copies_ref[k] = rows


def state_kernel(place_ref, got_ref, state_ref, reach_ref):
    got = got_ref[...].reshape(SLOTS, WIDTH)
    state_ref[...] = dot(ones_where(row_of_peer(CAP) | row_of_peer(CAP + 1)), got, 1, 0)
    spread = dot(ones_where(row_of_peer(CAP + 2)), got, 1, 0).astype(BF16)
    lane, peer = iota((WIDTH, PEERS), 0), iota((WIDTH, PEERS), 1)
    fold = (lane == peer) | (lane == peer + PEERS) | (lane == peer + 2 * PEERS)
    logs = dot(spread, ones_where(fold), 1, 0)
    here = place_ref[0]
    a, b = iota((PEERS, PEERS), 0), iota((PEERS, PEERS), 1)
    later = dot(jnp.where(b > here, logs, 0.0), ones_where(a < b, F32), 1, 0, EXACT)
    before = dot(jnp.where(b < here, logs, 0.0), ones_where(a > b, F32), 1, 0, EXACT)
    later = jnp.where(b > here, jnp.exp(later), 0.0)
    before = jnp.where(b < here, jnp.exp(before), 0.0)
    half = KEY_DIM // 2
    first = iota((half, WIDTH), 1) < VAL_DIM
    for k in range(PEERS):
        for side, value in enumerate((later, before)):
            column = value[:, k : k + 1]
            reach_ref[side, k] = jnp.where(first, column[:half], column[half:])


def source_kernel(
    place_ref, rows_ref, weight_ref, normed_ref, inv_ref, mix_ref, query_fwd_ref, query_bwd_ref,
    send_ref, grad_ref,
):
    here = place_ref[0]
    rows = jnp.concatenate([rows_ref[c, k] for k in range(RING) for c in range(2)], axis=1)
    grad = dot(rows, weight_ref[...], 1, 1)
    normed = normed_ref[...]
    mean = jnp.mean(grad * normed, axis=1, keepdims=True)
    grad = inv_ref[...] * (grad - normed * mean)
    grad_ref[...] = grad
    twice = jnp.concatenate([grad, grad], axis=1)
    half = KEY_DIM // 2
    first = iota((half, WIDTH), 1) < VAL_DIM
    states = []
    for ref in (query_fwd_ref, query_bwd_ref):
        state = dot(ref[...], twice, 1, 0, EXACT)
        states.append(jnp.where(first, state[:half], state[half:]))
    lane = iota((KEY_DIM, WIDTH), 1)
    for k in range(2 * RING):
        part = dot(rows[:, k * WIDTH : (k + 1) * WIDTH], mix_ref[...], 0, 0)
        for side in range(2):
            at, peer = side * VAL_DIM, 2 * k + side
            both = jnp.where(lane < VAL_DIM, part[at : at + 32], part[at + 32 : at + 64])
            send_ref[peer, :KEY_DIM] = both.astype(BF16)
            send_ref[peer, KEY_DIM:] = jnp.where(peer < here, states[0], states[1]).astype(BF16)


def final_kernel(
    got_ref, reach_ref, state_ref, cum_ref, key_ref, val_ref, pre_ref, speed_ref,
    keys_mix_ref, vals_mix_ref, decay_mix_ref,
    proj_ref, keys_ref, vals_ref, logit_ref,
):
    proj = got_ref[0, :KEY_DIM].astype(F32)
    flow = got_ref[0, KEY_DIM:].astype(F32)
    packed = [flow * reach_ref[0, 0], flow * reach_ref[1, 0]]
    for k in range(1, PEERS):
        proj = proj + got_ref[k, :KEY_DIM].astype(F32)
        flow = got_ref[k, KEY_DIM:].astype(F32)
        packed = [total + flow * reach_ref[side, k] for side, total in enumerate(packed)]
    flow_fwd, flow_bwd = (
        jnp.concatenate([total[:, :VAL_DIM], total[:, VAL_DIM:]], axis=0) for total in packed
    )
    proj_ref[:KEY_DIM] = proj[:, :VAL_DIM]
    proj_ref[KEY_DIM:] = proj[:, VAL_DIM:]
    cum = cum_ref[...]
    total = cum[:, TOK - 1 : TOK]
    keys, vals = key_ref[...].astype(F32), val_ref[...].astype(F32)
    scale_fwd, scale_bwd = jnp.exp(total - cum), jnp.exp(cum)
    grad_fwd = dot(flow_fwd, vals, 1, 0, EXACT) * scale_fwd
    grad_bwd = dot(flow_bwd, vals, 1, 0, EXACT) * scale_bwd
    keys_ref[...] = keys_mix_ref[...] + grad_fwd + grad_bwd
    vals_ref[...] = (
        vals_mix_ref[...]
        + dot(flow_fwd, keys * scale_fwd, 0, 0, EXACT)
        + dot(flow_bwd, keys * scale_bwd, 0, 0, EXACT)
    )
    state = state_ref[...]
    flow = flow_fwd * state[:, :VAL_DIM] + flow_bwd * state[:, VAL_DIM:]
    factor = jnp.exp(total) * jnp.sum(flow, axis=1, keepdims=True)
    grad_fwd, grad_bwd = grad_fwd * keys, grad_bwd * keys
    at_end = factor + jnp.sum(grad_fwd, axis=1, keepdims=True)
    row, col = iota((TOK, TOK), 0), iota((TOK, TOK), 1)
    tail = dot(grad_bwd - grad_fwd, ones_where(row >= col, F32), 1, 0, EXACT)
    decay = decay_mix_ref[...] + tail + at_end
    diagonal = iota((KEY_DIM, KEY_DIM), 0) == iota((KEY_DIM, KEY_DIM), 1)
    speed = jnp.sum(jnp.where(diagonal, speed_ref[...], 0.0), axis=1, keepdims=True)
    pre = pre_ref[...].astype(F32)
    logit_ref[...] = decay * speed * jax.nn.sigmoid(-pre)


SCALAR = pl.BlockSpec(memory_space=pltpu.SMEM)
WHOLE = pl.BlockSpec(memory_space=pltpu.VMEM)


def on_chip(array):
    return pltpu.with_memory_space_constraint(array, pltpu.VMEM)


def off_chip(array):
    return pltpu.with_memory_space_constraint(array, pltpu.HBM)


def call(kernel, outs, *args, scalars=0, stored=()):
    shapes = [
        (pltpu.HBM if k in stored else pltpu.VMEM)(shape, dtype)
        for k, (shape, dtype) in enumerate(outs)
    ]
    return pl.pallas_call(
        kernel,
        out_shape=shapes,
        in_specs=[SCALAR] * scalars + [WHOLE] * (len(args) - scalars),
        out_specs=[WHOLE] * len(shapes),
        compiler_params=pltpu.CompilerParams(vmem_limit_bytes=24 << 20),
    )(*args)


def inner(scaled, keys, vals, cum, lower):
    gap = cum[:, :, None] - cum[:, None, :]
    weight = jnp.exp(jnp.where(lower, gap, -gap))
    scores = jnp.einsum("ct,cs,cts->ts", scaled, keys, weight)
    return jnp.einsum("ts,vs->vt", scores, vals)


def carried(scaled, cum, fwd_in, bwd_in):
    total = cum[:, -1:]
    return jnp.einsum("ct,cv->vt", scaled * jnp.exp(cum), fwd_in) + jnp.einsum(
        "ct,cv->vt", scaled * jnp.exp(total - cum), bwd_in
    )


def body(
    queries,
    input_key_matrix,
    input_value_matrix,
    decay_preactivation,
    extra_log_decay,
    channel_decay_speed,
    output_weight_matrix,
    stored_expert_rows,
    chosen_expert_index,
    expert_combine_weight,
    cotangent,
    expert_gate_weight,
    expert_up_weight,
    expert_down_weight,
):
    sp = ("z", "x")
    core = lax.axis_index("core")
    core_at = core.reshape(1).astype(jnp.int32)
    place_at = lax.axis_index(sp).reshape(1).astype(jnp.int32)
    speed = channel_decay_speed.reshape(1, KEY_DIM)
    swap = [(0, 1), (1, 0)]

    def exchanged(array, axis):
        return lax.all_to_all(array, axis, split_axis=0, concat_axis=0, tiled=True)

    gate, up, down = expert_gate_weight[0], expert_up_weight[0], expert_down_weight[0]
    gate_blocks = gate.reshape(2 * RING, WIDTH, WIDTH)
    up_blocks = up.reshape(2 * RING, WIDTH, WIDTH)
    send, pick, cum = call(
        dispatch_kernel,
        [((PEERS, PAD, 2 * WIDTH), BF16), ((SLOTS, TOK), BF16), ((KEY_DIM, TOK), F32)],
        off_chip(chosen_expert_index.T),
        off_chip(expert_combine_weight.T),
        off_chip(stored_expert_rows),
        off_chip(cotangent),
        off_chip(input_key_matrix),
        off_chip(input_value_matrix),
        off_chip(decay_preactivation),
        off_chip(extra_log_decay),
        off_chip(speed),
        stored=(1,),
    )
    got = exchanged(send, sp)
    (theirs,) = call(
        slice_kernel,
        [((3, RING, WIDTH, WIDTH), BF16)],
        core_at,
        off_chip(gate_blocks),
        off_chip(up_blocks),
        off_chip(down),
        scalars=1,
        stored=(0,),
    )
    swapped = lax.ppermute(theirs, "core", swap)
    copies, back = call(
        arrival_kernel,
        [((RING, ROWS, 2 * WIDTH), BF16), ((PEERS, PAD, WIDTH), BF16)],
        on_chip(got),
        stored=(0, 1),
    )
    rows = exchanged(copies, "y")
    own, send = call(
        forward_kernel,
        [((2, ROWS, 3 * WIDTH), F32), ((2, ROWS, 3 * WIDTH), BF16)],
        core_at,
        rows,
        gate_blocks,
        up_blocks,
        down,
        swapped,
        scalars=1,
    )
    crossed = lax.ppermute(send, "core", swap)
    partials, grads, hidden = call(
        partial_kernel,
        [
            ((RING, ROWS, WIDTH), BF16),
            ((ROWS, 4 * WIDTH), BF16),
            ((ROWS, 2 * WIDTH), BF16),
        ],
        core_at,
        on_chip(own),
        on_chip(crossed),
        gate_blocks,
        up_blocks,
        swapped,
        scalars=1,
        stored=(1, 2),
    )
    parts = exchanged(partials, "y")
    (send,) = call(
        return_kernel, [((PEERS, PAD, WIDTH), BF16)], on_chip(parts), off_chip(back)
    )
    returned = on_chip(exchanged(send, sp))
    (copies,) = call(
        token_kernel, [((RING, TOK, WIDTH), BF16)], returned, off_chip(pick), off_chip(cotangent)
    )
    row = iota((TOK, TOK), 0)
    cum, queries, key_in, val_in, row, copies = lax.optimization_barrier(
        (cum, queries, input_key_matrix, input_value_matrix, row, copies)
    )
    full_rows = exchanged(copies, "y")
    full_rows = lax.all_gather(full_rows, "core", axis=0, tiled=False)

    state, reach = call(
        state_kernel,
        [((KEY_DIM, WIDTH), F32), ((2, PEERS, KEY_DIM // 2, WIDTH), F32)],
        place_at,
        returned,
        scalars=1,
    )
    scaled = queries.astype(F32) * KEY_DIM ** (-0.5)
    keys = key_in.astype(F32)
    vals = val_in.astype(F32)
    lower = row >= iota((TOK, TOK), 1)
    fwd_in, bwd_in = state[:, :VAL_DIM], state[:, VAL_DIM:]
    inner_out, pull_inner = jax.vjp(
        lambda *args: inner(*args, lower), scaled, keys, vals, cum
    )
    carried_out, pull_carried = jax.vjp(
        lambda s, c: carried(s, c, fwd_in, bwd_in), scaled, cum
    )
    mixed = inner_out + carried_out
    inv_rms = lax.rsqrt(jnp.mean(mixed * mixed, axis=0, keepdims=True) + 1e-06)
    normed = mixed * inv_rms
    normed_t = normed.T
    mix_t = normed_t.astype(BF16)
    mix_twice = jnp.concatenate([mix_t, mix_t], axis=1)
    query_fwd = scaled * jnp.exp(cum)
    query_bwd = scaled * jnp.exp(cum[:, -1:] - cum)
    send, grad_mixed_t = call(
        source_kernel,
        [((PEERS, 3 * KEY_DIM // 2, WIDTH), BF16), ((TOK, VAL_DIM), F32)],
        place_at,
        on_chip(full_rows),
        off_chip(output_weight_matrix.T),
        normed_t,
        inv_rms.reshape(TOK, 1),
        mix_twice,
        query_fwd,
        query_bwd,
        scalars=1,
    )
    send, grads, hidden = lax.optimization_barrier((send, grads, hidden))
    got = exchanged(send, sp)
    own, send = call(
        weight_kernel,
        [((3, RING, WIDTH, WIDTH), BF16)] * 2,
        off_chip(rows),
        off_chip(grads),
        off_chip(hidden),
        stored=range(2),
    )
    crossed = lax.ppermute(send, "core", swap)
    grad_gate, grad_up, grad_down = call(
        joined_kernel,
        [
            ((2 * RING, WIDTH, WIDTH), BF16),
            ((2 * RING, WIDTH, WIDTH), BF16),
            ((WIDTH, MODEL), BF16),
        ],
        core_at,
        off_chip(own),
        off_chip(crossed),
        scalars=1,
        stored=range(3),
    )
    grad_mixed = grad_mixed_t.T
    grad_scaled, grad_keys, grad_vals, grad_cum = pull_inner(grad_mixed)
    grad_scaled_in, grad_cum_in = pull_carried(grad_mixed)
    grad_queries = (grad_scaled + grad_scaled_in) * KEY_DIM ** (-0.5)
    tail_mask = ones_where(iota((TOK, TOK), 0) >= iota((TOK, TOK), 1), F32)
    grad_decay = dot(grad_cum + grad_cum_in, tail_mask, 1, 0, EXACT)
    grad_out_proj, grad_keys, grad_values, grad_logit = call(
        final_kernel,
        [
            ((2 * KEY_DIM, VAL_DIM), F32),
            ((KEY_DIM, TOK), F32),
            ((VAL_DIM, TOK), F32),
            ((KEY_DIM, TOK), F32),
        ],
        on_chip(got),
        reach,
        state,
        cum,
        input_key_matrix,
        input_value_matrix,
        decay_preactivation,
        speed,
        grad_keys,
        grad_vals,
        grad_decay,
        stored=range(4),
    )
    return (
        grad_queries,
        grad_keys,
        grad_values,
        grad_logit,
        grad_out_proj,
        grad_gate.reshape(1, MODEL, WIDTH),
        grad_up.reshape(1, MODEL, WIDTH),
        grad_down[None],
    )


def solution(mesh):
    fine = Mesh(mesh.devices.reshape(8, 4, 8, 2), ("z", "x", "y", "core"))
    sp, tp = ("z", "x"), ("y", "core")
    in_specs = (
        P(tp, sp),
        P(tp, sp),
        P(tp, sp),
        P(tp, sp),
        P(tp, sp),
        P(tp),
        P(None, tp),
        P(sp, tp),
        P(sp, None),
        P(sp, None),
        P(sp, tp),
        P(sp, None, tp),
        P(sp, None, tp),
        P(sp, tp, None),
    )
    out_specs = (
        P(tp, sp),
        P(tp, sp),
        P(tp, sp),
        P(tp, sp),
        P(sp, tp),
        P(sp, None, tp),
        P(sp, None, tp),
        P(sp, tp, None),
    )

    return jax.shard_map(body, mesh=fine, in_specs=in_specs, out_specs=out_specs, check_vma=False)
```

```python
import jax
import jax.numpy as jnp
from jax import lax
from jax.experimental import pallas as pl
from jax.experimental.pallas import tpu as pltpu
from jax.sharding import Mesh
from jax.sharding import PartitionSpec as P


KEY_DIM = 32
VAL_DIM = 64
TOK = 128
PEERS = 32
CAP = 12
PAD = 16
RING = 8
SLOTS = PEERS * PAD
ROWS = PEERS * CAP
WIDTH = 128
MODEL = 2048

F32 = jnp.float32
BF16 = jnp.bfloat16
EXACT = lax.Precision.HIGHEST


def dot(a, b, da, db, precision=None):
    return lax.dot_general(
        a, b, (((da,), (db,)), ((), ())), preferred_element_type=F32, precision=precision
    )


def iota(shape, dim):
    return lax.broadcasted_iota(jnp.int32, shape, dim)


def ones_where(mask, dtype=BF16):
    return jnp.where(mask, 1.0, 0.0).astype(dtype)


def split_two(value):
    high = value.astype(BF16).astype(F32)
    return high, (value - high).astype(BF16).astype(F32)


def split_three(value):
    high, rest = split_two(value)
    return high, rest, (value - high - rest).astype(BF16).astype(F32)


def compact_rows(shape, compact_dim):
    row = iota(shape, compact_dim)
    peer = (row * 5462) >> 16
    return peer * PAD + (row - peer * CAP) == iota(shape, 1 - compact_dim)


def row_of_peer(place):
    return iota((PEERS, SLOTS), 1) == iota((PEERS, SLOTS), 0) * PAD + place


def dispatch_kernel(
    ids_ref, share_ref, x_ref, cot_ref, key_ref, val_ref, pre_ref, extra_ref, speed_ref,
    send_ref, pick_ref, cum_ref,
):
    expert = iota((PEERS, TOK), 0)
    named = [ids_ref[k : k + 1, :] == expert for k in range(2)]
    row, col = iota((TOK, TOK), 0), iota((TOK, TOK), 1)
    rank = dot(ones_where(named[0] | named[1]), ones_where(row < col), 1, 0)
    place = iota((PEERS, PAD, TOK), 1).astype(F32)
    cot = cot_ref[...].astype(F32)
    picks, grads = [], None
    for k in range(2):
        at = jnp.where(named[k], rank, -1.0)
        pick = jnp.where(at[:, None, :] == place, 1.0, 0.0).reshape(SLOTS, TOK).astype(BF16)
        share = jnp.sum(jnp.where(row == col, share_ref[k : k + 1, :], 0.0), axis=1, keepdims=True)
        part = dot(pick, (share * cot).astype(BF16), 1, 0)
        grads = part if grads is None else grads + part
        picks.append(pick)
    pick = picks[0] + picks[1]
    pick_ref[...] = pick
    rows = jnp.concatenate([dot(pick, x_ref[...], 1, 0), grads], axis=1)

    pre = pre_ref[...].astype(F32)
    log_sig = jnp.minimum(pre, 0.0) - jnp.log1p(jnp.exp(-jnp.abs(pre)))
    diagonal = iota((KEY_DIM, KEY_DIM), 0) == iota((KEY_DIM, KEY_DIM), 1)
    speed = jnp.sum(jnp.where(diagonal, speed_ref[...], 0.0), axis=1, keepdims=True)
    decay = speed * log_sig + extra_ref[...]
    cum = dot(decay, ones_where(row <= col, F32), 1, 0, EXACT)
    cum_ref[...] = cum
    total = cum[:, TOK - 1 : TOK]
    keys, vals = key_ref[...].astype(F32), val_ref[...].astype(F32)
    sums = jnp.concatenate(
        [
            dot(keys * jnp.exp(total - cum), vals, 1, 1, EXACT),
            dot(keys * jnp.exp(cum), vals, 1, 1, EXACT),
        ],
        axis=1,
    )
    state = jnp.concatenate(split_two(sums), axis=1)
    lane = iota((KEY_DIM, 2 * WIDTH), 1)
    logs = jnp.zeros((KEY_DIM, 2 * WIDTH), F32)
    for k, part in enumerate(split_three(total)):
        logs = jnp.where(lane == k, part, logs)
    place = iota((PEERS, PAD, 2 * WIDTH), 1)
    block = rows.reshape(PEERS, PAD, 2 * WIDTH)
    block = jnp.where(place == CAP, state[:, None, :], block)
    block = jnp.where(place == CAP + 1, logs[:, None, :], block)
    send_ref[...] = block.astype(BF16)


def arrival_kernel(got_ref, copies_ref, back_ref):
    got = got_ref[...].reshape(SLOTS, 2 * WIDTH)
    rows = dot(ones_where(compact_rows((ROWS, SLOTS), 0)), got, 1, 0).astype(BF16)
    for k in range(RING):
        copies_ref[k] = rows
    both = dot(ones_where(row_of_peer(CAP)), got, 1, 0)
    state = both[:, :WIDTH] + both[:, WIDTH:]
    logs = dot(ones_where(row_of_peer(CAP + 1)), got, 1, 0)
    log = jnp.sum(logs, axis=1, keepdims=True)
    a, b = iota((PEERS, PEERS), 0), iota((PEERS, PEERS), 1)
    gap_fwd = dot(ones_where(b < a, F32), jnp.where(a > b, log, 0.0), 1, 0, EXACT)
    gap_bwd = dot(ones_where(b > a, F32), jnp.where(a < b, log, 0.0), 1, 0, EXACT)
    fwd = dot(jnp.where(b < a, jnp.exp(gap_fwd), 0.0), state, 1, 0, EXACT)
    bwd = dot(jnp.where(b > a, jnp.exp(gap_bwd), 0.0), state, 1, 0, EXACT)
    lane = iota((PEERS, WIDTH), 1)
    high, low = split_two(jnp.where(lane < VAL_DIM, fwd, bwd))
    peer = iota((PEERS, WIDTH), 0)
    spread = jnp.zeros((PEERS, WIDTH), F32)
    for k, part in enumerate(split_three(log)):
        spread = jnp.where(lane == peer + k * PEERS, part, spread)
    all_logs = jnp.sum(spread, axis=0, keepdims=True)
    place = iota((PEERS, PAD, WIDTH), 1)
    block = jnp.where(place == CAP, high[:, None, :], 0.0)
    block = jnp.where(place == CAP + 1, low[:, None, :], block)
    block = jnp.where(place == CAP + 2, all_logs[:, None, :], block)
    back_ref[...] = block.astype(BF16)


def slice_kernel(core_ref, place_ref, gate_ref, up_ref, down_ref, own_ref, out_ref):
    core = core_ref[0]
    for side, ref in ((core, own_ref), (1 - core, out_ref)):
        for k in range(RING):
            at = 2 * k + side
            ref[0, k] = gate_ref[at]
            ref[1, k] = up_ref[at]
            ref[2, k] = down_ref[:, pl.ds(pl.multiple_of(at * WIDTH, WIDTH), WIDTH)]


def forward_kernel(rows_ref, own_ref, swapped_ref, out_ref, send_ref):
    pre = jnp.zeros((ROWS, 4 * WIDTH), F32)
    grad = jnp.zeros((ROWS, 2 * WIDTH), F32)
    for k in range(0, RING, 2):
        weights, downs = [], []
        for j in (k, k + 1):
            parts = [own_ref[0, j], own_ref[1, j], swapped_ref[0, j], swapped_ref[1, j]]
            weights.append(jnp.concatenate(parts, axis=1))
            downs.append(jnp.concatenate([own_ref[2, j], swapped_ref[2, j]], axis=0))
        x = jnp.concatenate([rows_ref[k, :, :WIDTH], rows_ref[k + 1, :, :WIDTH]], axis=1)
        y = jnp.concatenate([rows_ref[k, :, WIDTH:], rows_ref[k + 1, :, WIDTH:]], axis=1)
        pre = pre + dot(x, jnp.concatenate(weights, axis=0), 1, 0)
        grad = grad + dot(y, jnp.concatenate(downs, axis=1), 1, 1)
    mine = jnp.concatenate([pre[:, : 2 * WIDTH], grad[:, :WIDTH]], axis=1)
    theirs = jnp.concatenate([pre[:, 2 * WIDTH :], grad[:, WIDTH:]], axis=1)
    out_ref[0] = mine
    out_ref[1] = theirs
    send_ref[0] = theirs.astype(BF16)
    send_ref[1] = mine.astype(BF16)


def partial_kernel(
    own_ref, got_ref, kept_ref, swapped_ref, out_ref, grads_ref, hidden_ref
):
    grads = []
    for half in range(2):
        total = own_ref[half] + got_ref[half].astype(F32)
        gate_pre, up_pre = total[:, :WIDTH], total[:, WIDTH : 2 * WIDTH]
        grad_hidden = total[:, 2 * WIDTH :]
        gate_sig = jax.nn.sigmoid(gate_pre)
        gate_act = gate_pre * gate_sig
        hidden_ref[:, half * WIDTH : (half + 1) * WIDTH] = (gate_act * up_pre).astype(BF16)
        slope = gate_sig * (1.0 + gate_pre * (1.0 - gate_sig))
        grads.append((grad_hidden * up_pre * slope).astype(BF16))
        grads.append((grad_hidden * gate_act).astype(BF16))
    grads = jnp.concatenate(grads, axis=1)
    grads_ref[...] = grads
    for k in range(RING):
        weights = jnp.concatenate(
            [kept_ref[0, k], kept_ref[1, k], swapped_ref[0, k], swapped_ref[1, k]], axis=1
        )
        out_ref[k] = dot(grads, weights, 1, 1).astype(BF16)


def weight_kernel(rows_ref, grads_ref, hidden_ref, own_ref, send_ref):
    grads, hidden = grads_ref[...], hidden_ref[...]
    for k in range(RING):
        both = dot(rows_ref[k, :, :WIDTH], grads, 0, 0).astype(BF16)
        down = dot(hidden, rows_ref[k, :, WIDTH:], 0, 0).astype(BF16)
        for half, ref in enumerate((own_ref, send_ref)):
            at = 2 * half * WIDTH
            ref[0, k] = both[:, at : at + WIDTH]
            ref[1, k] = both[:, at + WIDTH : at + 2 * WIDTH]
            ref[2, k] = down[half * WIDTH : (half + 1) * WIDTH]


def joined_kernel(core_ref, own_ref, got_ref, gate_ref, up_ref, down_ref):
    core = core_ref[0]
    for k in range(RING):
        for side, ref in ((core, own_ref), (1 - core, got_ref)):
            at = 2 * k + side
            gate_ref[at] = ref[0, k]
            up_ref[at] = ref[1, k]
            down_ref[:, pl.ds(pl.multiple_of(at * WIDTH, WIDTH), WIDTH)] = ref[2, k]


def return_kernel(parts_ref, back_ref, send_ref):
    total = parts_ref[0].astype(F32)
    for k in range(1, RING):
        total = total + parts_ref[k].astype(F32)
    rows = dot(ones_where(compact_rows((SLOTS, ROWS), 1)), total.astype(BF16), 1, 0)
    rows = rows.astype(BF16).reshape(PEERS, PAD, WIDTH)
    send_ref[...] = rows + back_ref[...]


def token_kernel(got_ref, pick_ref, cot_ref, copies_ref):
    got = got_ref[...].reshape(SLOTS, WIDTH)
    rows = (cot_ref[...].astype(F32) + dot(pick_ref[...], got, 0, 0)).astype(BF16)
    for k in range(RING):
        copies_ref[k] = rows


def state_kernel(place_ref, got_ref, state_ref, reach_ref):
    got = got_ref[...].reshape(SLOTS, WIDTH)
    state_ref[...] = dot(ones_where(row_of_peer(CAP) | row_of_peer(CAP + 1)), got, 1, 0)
    spread = dot(ones_where(row_of_peer(CAP + 2)), got, 1, 0).astype(BF16)
    lane, peer = iota((WIDTH, PEERS), 0), iota((WIDTH, PEERS), 1)
    fold = (lane == peer) | (lane == peer + PEERS) | (lane == peer + 2 * PEERS)
    logs = dot(spread, ones_where(fold), 1, 0)
    here = place_ref[0]
    a, b = iota((PEERS, PEERS), 0), iota((PEERS, PEERS), 1)
    later = dot(jnp.where(b > here, logs, 0.0), ones_where(a < b, F32), 1, 0, EXACT)
    before = dot(jnp.where(b < here, logs, 0.0), ones_where(a > b, F32), 1, 0, EXACT)
    later = jnp.where(b > here, jnp.exp(later), 0.0)
    before = jnp.where(b < here, jnp.exp(before), 0.0)
    half = KEY_DIM // 2
    first = iota((half, WIDTH), 1) < VAL_DIM
    for k in range(PEERS):
        for side, value in enumerate((later, before)):
            column = value[:, k : k + 1]
            reach_ref[side, k] = jnp.where(first, column[:half], column[half:])


def source_kernel(
    place_ref, rows_ref, weight_ref, normed_ref, inv_ref, mix_ref, query_fwd_ref, query_bwd_ref,
    send_ref, grad_ref,
):
    here = place_ref[0]
    rows = jnp.concatenate([rows_ref[c, k] for k in range(RING) for c in range(2)], axis=1)
    grad = dot(rows, weight_ref[...], 1, 1)
    normed = normed_ref[...]
    mean = jnp.mean(grad * normed, axis=1, keepdims=True)
    grad = inv_ref[...] * (grad - normed * mean)
    grad_ref[...] = grad
    twice = jnp.concatenate([grad, grad], axis=1)
    half = KEY_DIM // 2
    first = iota((half, WIDTH), 1) < VAL_DIM
    states = []
    for ref in (query_fwd_ref, query_bwd_ref):
        state = dot(ref[...], twice, 1, 0, EXACT)
        states.append(jnp.where(first, state[:half], state[half:]))
    lane = iota((KEY_DIM, WIDTH), 1)
    for k in range(2 * RING):
        part = dot(rows[:, k * WIDTH : (k + 1) * WIDTH], mix_ref[...], 0, 0)
        for side in range(2):
            at, peer = side * VAL_DIM, 2 * k + side
            both = jnp.where(lane < VAL_DIM, part[at : at + 32], part[at + 32 : at + 64])
            send_ref[peer, :KEY_DIM] = both.astype(BF16)
            send_ref[peer, KEY_DIM:] = jnp.where(peer < here, states[0], states[1]).astype(BF16)


def final_kernel(
    got_ref, reach_ref, state_ref, cum_ref, key_ref, val_ref, pre_ref, speed_ref,
    keys_mix_ref, vals_mix_ref, decay_mix_ref,
    proj_ref, keys_ref, vals_ref, logit_ref,
):
    proj = got_ref[0, :KEY_DIM].astype(F32)
    flow = got_ref[0, KEY_DIM:].astype(F32)
    packed = [flow * reach_ref[0, 0], flow * reach_ref[1, 0]]
    for k in range(1, PEERS):
        proj = proj + got_ref[k, :KEY_DIM].astype(F32)
        flow = got_ref[k, KEY_DIM:].astype(F32)
        packed = [total + flow * reach_ref[side, k] for side, total in enumerate(packed)]
    flow_fwd, flow_bwd = (
        jnp.concatenate([total[:, :VAL_DIM], total[:, VAL_DIM:]], axis=0) for total in packed
    )
    proj_ref[:KEY_DIM] = proj[:, :VAL_DIM]
    proj_ref[KEY_DIM:] = proj[:, VAL_DIM:]
    cum = cum_ref[...]
    total = cum[:, TOK - 1 : TOK]
    keys, vals = key_ref[...].astype(F32), val_ref[...].astype(F32)
    scale_fwd, scale_bwd = jnp.exp(total - cum), jnp.exp(cum)
    grad_fwd = dot(flow_fwd, vals, 1, 0, EXACT) * scale_fwd
    grad_bwd = dot(flow_bwd, vals, 1, 0, EXACT) * scale_bwd
    keys_ref[...] = keys_mix_ref[...] + grad_fwd + grad_bwd
    vals_ref[...] = (
        vals_mix_ref[...]
        + dot(flow_fwd, keys * scale_fwd, 0, 0, EXACT)
        + dot(flow_bwd, keys * scale_bwd, 0, 0, EXACT)
    )
    state = state_ref[...]
    flow = flow_fwd * state[:, :VAL_DIM] + flow_bwd * state[:, VAL_DIM:]
    factor = jnp.exp(total) * jnp.sum(flow, axis=1, keepdims=True)
    grad_fwd, grad_bwd = grad_fwd * keys, grad_bwd * keys
    at_end = factor + jnp.sum(grad_fwd, axis=1, keepdims=True)
    row, col = iota((TOK, TOK), 0), iota((TOK, TOK), 1)
    tail = dot(grad_bwd - grad_fwd, ones_where(row >= col, F32), 1, 0, EXACT)
    decay = decay_mix_ref[...] + tail + at_end
    diagonal = iota((KEY_DIM, KEY_DIM), 0) == iota((KEY_DIM, KEY_DIM), 1)
    speed = jnp.sum(jnp.where(diagonal, speed_ref[...], 0.0), axis=1, keepdims=True)
    pre = pre_ref[...].astype(F32)
    logit_ref[...] = decay * speed * jax.nn.sigmoid(-pre)


SCALAR = pl.BlockSpec(memory_space=pltpu.SMEM)
WHOLE = pl.BlockSpec(memory_space=pltpu.VMEM)


def on_chip(array):
    return pltpu.with_memory_space_constraint(array, pltpu.VMEM)


def off_chip(array):
    return pltpu.with_memory_space_constraint(array, pltpu.HBM)


def call(kernel, outs, *args, scalars=0, stored=()):
    shapes = [
        (pltpu.HBM if k in stored else pltpu.VMEM)(shape, dtype)
        for k, (shape, dtype) in enumerate(outs)
    ]
    return pl.pallas_call(
        kernel,
        out_shape=shapes,
        in_specs=[SCALAR] * scalars + [WHOLE] * (len(args) - scalars),
        out_specs=[WHOLE] * len(shapes),
        compiler_params=pltpu.CompilerParams(vmem_limit_bytes=24 << 20),
    )(*args)


def inner(scaled, keys, vals, cum, lower):
    gap = cum[:, :, None] - cum[:, None, :]
    weight = jnp.exp(jnp.where(lower, gap, -gap))
    scores = jnp.einsum("ct,cs,cts->ts", scaled, keys, weight)
    return jnp.einsum("ts,vs->vt", scores, vals)


def carried(scaled, cum, fwd_in, bwd_in):
    total = cum[:, -1:]
    return jnp.einsum("ct,cv->vt", scaled * jnp.exp(cum), fwd_in) + jnp.einsum(
        "ct,cv->vt", scaled * jnp.exp(total - cum), bwd_in
    )


def body(
    queries,
    input_key_matrix,
    input_value_matrix,
    decay_preactivation,
    extra_log_decay,
    channel_decay_speed,
    output_weight_matrix,
    stored_expert_rows,
    chosen_expert_index,
    expert_combine_weight,
    cotangent,
    expert_gate_weight,
    expert_up_weight,
    expert_down_weight,
):
    sp = ("z", "x")
    core = lax.axis_index("core")
    core_at = core.reshape(1).astype(jnp.int32)
    place_at = lax.axis_index(sp).reshape(1).astype(jnp.int32)
    speed = channel_decay_speed.reshape(1, KEY_DIM)
    swap = [(0, 1), (1, 0)]

    def exchanged(array, axis):
        return lax.all_to_all(array, axis, split_axis=0, concat_axis=0, tiled=True)

    gate, up, down = expert_gate_weight[0], expert_up_weight[0], expert_down_weight[0]
    gate_blocks = gate.reshape(2 * RING, WIDTH, WIDTH)
    up_blocks = up.reshape(2 * RING, WIDTH, WIDTH)
    send, pick, cum = call(
        dispatch_kernel,
        [((PEERS, PAD, 2 * WIDTH), BF16), ((SLOTS, TOK), BF16), ((KEY_DIM, TOK), F32)],
        off_chip(chosen_expert_index.T),
        off_chip(expert_combine_weight.T),
        off_chip(stored_expert_rows),
        off_chip(cotangent),
        off_chip(input_key_matrix),
        off_chip(input_value_matrix),
        off_chip(decay_preactivation),
        off_chip(extra_log_decay),
        off_chip(speed),
        stored=(1,),
    )
    got = exchanged(send, sp)
    copies, back = call(
        arrival_kernel,
        [((RING, ROWS, 2 * WIDTH), BF16), ((PEERS, PAD, WIDTH), BF16)],
        on_chip(got),
        stored=(0, 1),
    )
    rows = exchanged(copies, "y")
    kept, theirs = call(
        slice_kernel,
        [((3, RING, WIDTH, WIDTH), BF16)] * 2,
        core_at,
        place_at,
        off_chip(gate_blocks),
        off_chip(up_blocks),
        off_chip(down),
        scalars=2,
        stored=(1,),
    )
    swapped = lax.ppermute(theirs, "core", swap)
    own, send = call(
        forward_kernel,
        [((2, ROWS, 3 * WIDTH), F32), ((2, ROWS, 3 * WIDTH), BF16)],
        rows,
        on_chip(kept),
        swapped,
    )
    crossed = lax.ppermute(send, "core", swap)
    partials, grads, hidden = call(
        partial_kernel,
        [
            ((RING, ROWS, WIDTH), BF16),
            ((ROWS, 4 * WIDTH), BF16),
            ((ROWS, 2 * WIDTH), BF16),
        ],
        on_chip(own),
        on_chip(crossed),
        on_chip(kept),
        swapped,
        stored=(1, 2),
    )
    parts = exchanged(partials, "y")
    (send,) = call(
        return_kernel, [((PEERS, PAD, WIDTH), BF16)], on_chip(parts), off_chip(back)
    )
    returned = on_chip(exchanged(send, sp))
    (copies,) = call(
        token_kernel, [((RING, TOK, WIDTH), BF16)], returned, off_chip(pick), off_chip(cotangent)
    )
    row = iota((TOK, TOK), 0)
    cum, queries, key_in, val_in, row, copies = lax.optimization_barrier(
        (cum, queries, input_key_matrix, input_value_matrix, row, copies)
    )
    full_rows = exchanged(copies, "y")
    full_rows = lax.all_gather(full_rows, "core", axis=0, tiled=False)

    state, reach = call(
        state_kernel,
        [((KEY_DIM, WIDTH), F32), ((2, PEERS, KEY_DIM // 2, WIDTH), F32)],
        place_at,
        returned,
        scalars=1,
    )
    scaled = queries.astype(F32) * KEY_DIM ** (-0.5)
    keys = key_in.astype(F32)
    vals = val_in.astype(F32)
    lower = row >= iota((TOK, TOK), 1)
    fwd_in, bwd_in = state[:, :VAL_DIM], state[:, VAL_DIM:]
    inner_out, pull_inner = jax.vjp(
        lambda *args: inner(*args, lower), scaled, keys, vals, cum
    )
    carried_out, pull_carried = jax.vjp(
        lambda s, c: carried(s, c, fwd_in, bwd_in), scaled, cum
    )
    mixed = inner_out + carried_out
    inv_rms = lax.rsqrt(jnp.mean(mixed * mixed, axis=0, keepdims=True) + 1e-06)
    normed = mixed * inv_rms
    normed_t = normed.T
    mix_t = normed_t.astype(BF16)
    mix_twice = jnp.concatenate([mix_t, mix_t], axis=1)
    query_fwd = scaled * jnp.exp(cum)
    query_bwd = scaled * jnp.exp(cum[:, -1:] - cum)
    send, grad_mixed_t = call(
        source_kernel,
        [((PEERS, 3 * KEY_DIM // 2, WIDTH), BF16), ((TOK, VAL_DIM), F32)],
        place_at,
        on_chip(full_rows),
        off_chip(output_weight_matrix.T),
        normed_t,
        inv_rms.reshape(TOK, 1),
        mix_twice,
        query_fwd,
        query_bwd,
        scalars=1,
    )
    got = exchanged(send, sp)
    own, send = call(
        weight_kernel,
        [((3, RING, WIDTH, WIDTH), BF16)] * 2,
        off_chip(rows),
        off_chip(grads),
        off_chip(hidden),
        stored=range(2),
    )
    crossed = lax.ppermute(send, "core", swap)
    grad_gate, grad_up, grad_down = call(
        joined_kernel,
        [
            ((2 * RING, WIDTH, WIDTH), BF16),
            ((2 * RING, WIDTH, WIDTH), BF16),
            ((WIDTH, MODEL), BF16),
        ],
        core_at,
        off_chip(own),
        crossed,
        scalars=1,
        stored=range(3),
    )
    grad_mixed = grad_mixed_t.T
    grad_scaled, grad_keys, grad_vals, grad_cum = pull_inner(grad_mixed)
    grad_scaled_in, grad_cum_in = pull_carried(grad_mixed)
    grad_queries = (grad_scaled + grad_scaled_in) * KEY_DIM ** (-0.5)
    tail_mask = ones_where(iota((TOK, TOK), 0) >= iota((TOK, TOK), 1), F32)
    grad_decay = dot(grad_cum + grad_cum_in, tail_mask, 1, 0, EXACT)
    grad_out_proj, grad_keys, grad_values, grad_logit = call(
        final_kernel,
        [
            ((2 * KEY_DIM, VAL_DIM), F32),
            ((KEY_DIM, TOK), F32),
            ((VAL_DIM, TOK), F32),
            ((KEY_DIM, TOK), F32),
        ],
        on_chip(got),
        reach,
        state,
        cum,
        input_key_matrix,
        input_value_matrix,
        decay_preactivation,
        speed,
        grad_keys,
        grad_vals,
        grad_decay,
        stored=range(4),
    )
    return (
        grad_queries,
        grad_keys,
        grad_values,
        grad_logit,
        grad_out_proj,
        grad_gate.reshape(1, MODEL, WIDTH),
        grad_up.reshape(1, MODEL, WIDTH),
        grad_down[None],
    )


def solution(mesh):
    fine = Mesh(mesh.devices.reshape(8, 4, 8, 2), ("z", "x", "y", "core"))
    sp, tp = ("z", "x"), ("y", "core")
    in_specs = (
        P(tp, sp),
        P(tp, sp),
        P(tp, sp),
        P(tp, sp),
        P(tp, sp),
        P(tp),
        P(None, tp),
        P(sp, tp),
        P(sp, None),
        P(sp, None),
        P(sp, tp),
        P(sp, None, tp),
        P(sp, None, tp),
        P(sp, tp, None),
    )
    out_specs = (
        P(tp, sp),
        P(tp, sp),
        P(tp, sp),
        P(tp, sp),
        P(sp, tp),
        P(sp, None, tp),
        P(sp, None, tp),
        P(sp, tp, None),
    )

    return jax.shard_map(body, mesh=fine, in_specs=in_specs, out_specs=out_specs, check_vma=False)
```

```python
import jax
import jax.numpy as jnp
from jax import lax
from jax.experimental import pallas as pl
from jax.experimental.pallas import tpu as pltpu
from jax.sharding import Mesh
from jax.sharding import PartitionSpec as P


KEY_DIM = 32
VAL_DIM = 64
TOK = 128
PEERS = 32
CAP = 12
PAD = 16
RING = 8
SLOTS = PEERS * PAD
ROWS = PEERS * CAP
LEAD = PEERS * 8
WIDTH = 128
HALF = WIDTH // 2
MODEL = 2048

F32 = jnp.float32
BF16 = jnp.bfloat16
EXACT = lax.Precision.HIGHEST


def dot(a, b, da, db, precision=None):
    return lax.dot_general(
        a, b, (((da,), (db,)), ((), ())), preferred_element_type=F32, precision=precision
    )


def iota(shape, dim):
    return lax.broadcasted_iota(jnp.int32, shape, dim)


def ones_where(mask, dtype=BF16):
    return jnp.where(mask, 1.0, 0.0).astype(dtype)


def split_two(value):
    high = value.astype(BF16).astype(F32)
    return high, (value - high).astype(BF16).astype(F32)


def split_three(value):
    high, rest = split_two(value)
    return high, rest, (value - high - rest).astype(BF16).astype(F32)


def slot_rows(shape, compact_dim):
    row = iota(shape, compact_dim)
    tail = row - LEAD
    lead_at = (row >> 3) * PAD + (row & 7)
    tail_at = (tail >> 2) * PAD + 8 + (tail & 3)
    return jnp.where(row < LEAD, lead_at, tail_at) == iota(shape, 1 - compact_dim)


def row_of_peer(place):
    return iota((PEERS, SLOTS), 1) == iota((PEERS, SLOTS), 0) * PAD + place


def column_of(row_ref, k):
    diagonal = iota((TOK, TOK), 0) == iota((TOK, TOK), 1)
    return jnp.sum(jnp.where(diagonal, row_ref[k : k + 1, :], 0.0), axis=1, keepdims=True)


def swap_halves(value):
    return jnp.concatenate([value[:, HALF:], value[:, :HALF]], axis=1)


def dispatch_kernel(
    ids_ref, share_ref, x_ref, cot_ref, key_ref, val_ref, pre_ref, extra_ref, speed_ref,
    send_ref, token_ref, pick_ref, lead_ref, tail_ref, cum_ref,
):
    expert = iota((PEERS, TOK), 0)
    named = [ids_ref[k : k + 1, :] == expert for k in range(2)]
    row, col = iota((TOK, TOK), 0), iota((TOK, TOK), 1)
    rank = dot(ones_where(named[0] | named[1]), ones_where(row < col), 1, 0)
    place = iota((PEERS, PAD, TOK), 1).astype(F32)
    lead = iota((PEERS, 8, TOK), 1)
    tail = (8 + (lead & 3)).astype(F32)
    lead = lead.astype(F32)
    x, cot = x_ref[...].astype(F32), cot_ref[...].astype(F32)
    token_ref[...] = jnp.concatenate([cot[:, HALF:], x[:, HALF:]], axis=1).astype(BF16)
    picks, rows = [], None
    for k in range(2):
        at = jnp.where(named[k], rank, -1.0)[:, None, :]
        pick = jnp.where(at == place, 1.0, 0.0).reshape(SLOTS, TOK).astype(BF16)
        lead_ref[k] = jnp.where(at == lead, 1.0, 0.0).reshape(LEAD, TOK).astype(BF16)
        tail_ref[k] = jnp.where(at == tail, 1.0, 0.0).reshape(LEAD, TOK).astype(BF16)
        weighted = column_of(share_ref, k) * cot[:, :HALF]
        both = jnp.concatenate([x[:, :HALF], weighted], axis=1).astype(BF16)
        part = dot(pick, both, 1, 0)
        rows = part if rows is None else rows + part
        picks.append(pick)
    pick_ref[...] = picks[0] + picks[1]

    pre = pre_ref[...].astype(F32)
    log_sig = jnp.minimum(pre, 0.0) - jnp.log1p(jnp.exp(-jnp.abs(pre)))
    diagonal = iota((KEY_DIM, KEY_DIM), 0) == iota((KEY_DIM, KEY_DIM), 1)
    speed = jnp.sum(jnp.where(diagonal, speed_ref[...], 0.0), axis=1, keepdims=True)
    decay = speed * log_sig + extra_ref[...]
    cum = dot(decay, ones_where(row <= col, F32), 1, 0, EXACT)
    cum_ref[...] = cum
    total = cum[:, TOK - 1 : TOK]
    keys, vals = key_ref[...].astype(F32), val_ref[...].astype(F32)
    sums = jnp.concatenate(
        [
            dot(keys * jnp.exp(total - cum), vals, 1, 1, EXACT),
            dot(keys * jnp.exp(cum), vals, 1, 1, EXACT),
        ],
        axis=1,
    )
    high, low = split_two(sums)
    lane = iota((KEY_DIM, WIDTH), 1)
    logs = jnp.zeros((KEY_DIM, WIDTH), F32)
    for k, part in enumerate(split_three(total)):
        logs = jnp.where(lane == k, part, logs)
    place = iota((PEERS, PAD, WIDTH), 1)
    block = rows.reshape(PEERS, PAD, WIDTH)
    for k, part in enumerate((high, low, logs)):
        block = jnp.where(place == CAP + k, part[:, None, :], block)
    send_ref[...] = block.astype(BF16)


def spread_kernel(tokens_ref, share_ref, lead_ref, tail_ref, send_ref):
    lane = iota((TOK, WIDTH), 1)
    lead, first, second = 0.0, 0.0, 0.0
    for k in range(2):
        share = jnp.where(lane < HALF, column_of(share_ref, k), 1.0)
        rows = [(share * tokens_ref[y].astype(F32)).astype(BF16) for y in range(RING)]
        low = jnp.concatenate(rows[: RING // 2], axis=1)
        high = jnp.concatenate(rows[RING // 2 :], axis=1)
        lead = lead + dot(lead_ref[k], jnp.concatenate([low, high], axis=1), 1, 0)
        first = first + dot(tail_ref[k], low, 1, 0)
        second = second + dot(tail_ref[k], high, 1, 0)
    width = RING * WIDTH
    send_ref[:, :width] = lead.astype(BF16)
    upper = (iota((LEAD, width // 2), 0) & 7) < 4
    send_ref[:, width:] = jnp.where(upper, first, second).astype(BF16)


def arrival_kernel(got_ref, rows_ref, back_ref):
    got = got_ref[...].reshape(SLOTS, WIDTH)
    rows_ref[...] = dot(ones_where(slot_rows((ROWS, SLOTS), 0)), got, 1, 0).astype(BF16)
    state = dot(ones_where(row_of_peer(CAP) | row_of_peer(CAP + 1)), got, 1, 0)
    logs = dot(ones_where(row_of_peer(CAP + 2)), got, 1, 0)
    log = jnp.sum(logs, axis=1, keepdims=True)
    a, b = iota((PEERS, PEERS), 0), iota((PEERS, PEERS), 1)
    gap_fwd = dot(ones_where(b < a, F32), jnp.where(a > b, log, 0.0), 1, 0, EXACT)
    gap_bwd = dot(ones_where(b > a, F32), jnp.where(a < b, log, 0.0), 1, 0, EXACT)
    fwd = dot(jnp.where(b < a, jnp.exp(gap_fwd), 0.0), state, 1, 0, EXACT)
    bwd = dot(jnp.where(b > a, jnp.exp(gap_bwd), 0.0), state, 1, 0, EXACT)
    lane = iota((PEERS, WIDTH), 1)
    high, low = split_two(jnp.where(lane < VAL_DIM, fwd, bwd))
    peer = iota((PEERS, WIDTH), 0)
    spread = jnp.zeros((PEERS, WIDTH), F32)
    for k, part in enumerate(split_three(log)):
        spread = jnp.where(lane == peer + k * PEERS, part, spread)
    all_logs = jnp.sum(spread, axis=0, keepdims=True)
    place = iota((PEERS, PAD, WIDTH), 1)
    block = jnp.where(place == CAP, high[:, None, :], 0.0)
    block = jnp.where(place == CAP + 1, low[:, None, :], block)
    block = jnp.where(place == CAP + 2, all_logs[:, None, :], block)
    back_ref[...] = block.astype(BF16)


def slice_kernel(core_ref, place_ref, gate_ref, up_ref, down_ref, own_ref, out_ref):
    core = core_ref[0]
    for side, ref in ((core, own_ref), (1 - core, out_ref)):
        for k in range(RING):
            at = 2 * k + side
            ref[0, k] = gate_ref[at]
            ref[1, k] = up_ref[at]
            lanes = pl.ds(pl.multiple_of(at * WIDTH, WIDTH), WIDTH)
            ref[2, k] = swap_halves(down_ref[:, lanes].astype(F32)).astype(BF16)


def forward_kernel(near_ref, far_ref, own_ref, swapped_ref, out_ref, send_ref, rows_ref):
    width = RING * WIDTH
    tail = far_ref[:, width:]
    row, source = iota((LEAD // 2, LEAD), 0), iota((LEAD // 2, LEAD), 1)
    upper = source == (row >> 2) * 8 + (row & 3)
    lower = source == (row >> 2) * 8 + 4 + (row & 3)
    tail = [dot(ones_where(take), tail, 1, 0).astype(BF16) for take in (upper, lower)]
    first = iota((ROWS, WIDTH), 1) < HALF
    for k in range(RING):
        at = slice(k * WIDTH, (k + 1) * WIDTH)
        within = (k % (RING // 2)) * WIDTH
        last = tail[k // (RING // 2)][:, within : within + WIDTH]
        far = jnp.concatenate([far_ref[:, at], last], axis=0).astype(F32)
        near = near_ref[k].astype(F32)
        rows_ref[k, :, :WIDTH] = jnp.where(first, near, far).astype(BF16)
        rows_ref[k, :, WIDTH:] = jnp.where(first, far, near).astype(BF16)
    pre = jnp.zeros((ROWS, 4 * WIDTH), F32)
    grad = jnp.zeros((ROWS, 2 * WIDTH), F32)
    for k in range(0, RING, 2):
        weights, downs = [], []
        for j in (k, k + 1):
            parts = [own_ref[0, j], own_ref[1, j], swapped_ref[0, j], swapped_ref[1, j]]
            weights.append(jnp.concatenate(parts, axis=1))
            downs.append(jnp.concatenate([own_ref[2, j], swapped_ref[2, j]], axis=0))
        x = jnp.concatenate([rows_ref[k, :, :WIDTH], rows_ref[k + 1, :, :WIDTH]], axis=1)
        y = jnp.concatenate([rows_ref[k, :, WIDTH:], rows_ref[k + 1, :, WIDTH:]], axis=1)
        pre = pre + dot(x, jnp.concatenate(weights, axis=0), 1, 0)
        grad = grad + dot(y, jnp.concatenate(downs, axis=1), 1, 1)
    mine = jnp.concatenate([pre[:, : 2 * WIDTH], grad[:, :WIDTH]], axis=1)
    theirs = jnp.concatenate([pre[:, 2 * WIDTH :], grad[:, WIDTH:]], axis=1)
    out_ref[0] = mine
    out_ref[1] = theirs
    send_ref[0] = theirs.astype(BF16)
    send_ref[1] = mine.astype(BF16)


def partial_kernel(
    own_ref, got_ref, kept_ref, swapped_ref, out_ref, grads_ref, hidden_ref
):
    grads = []
    for half in range(2):
        total = own_ref[half] + got_ref[half].astype(F32)
        gate_pre, up_pre = total[:, :WIDTH], total[:, WIDTH : 2 * WIDTH]
        grad_hidden = total[:, 2 * WIDTH :]
        gate_sig = jax.nn.sigmoid(gate_pre)
        gate_act = gate_pre * gate_sig
        hidden_ref[:, half * WIDTH : (half + 1) * WIDTH] = (gate_act * up_pre).astype(BF16)
        slope = gate_sig * (1.0 + gate_pre * (1.0 - gate_sig))
        grads.append((grad_hidden * up_pre * slope).astype(BF16))
        grads.append((grad_hidden * gate_act).astype(BF16))
    grads = jnp.concatenate(grads, axis=1)
    grads_ref[...] = grads
    for k in range(RING):
        weights = jnp.concatenate(
            [kept_ref[0, k], kept_ref[1, k], swapped_ref[0, k], swapped_ref[1, k]], axis=1
        )
        out_ref[k] = dot(grads, weights, 1, 1).astype(BF16)


def weight_kernel(rows_ref, grads_ref, hidden_ref, own_ref, send_ref):
    grads, hidden = grads_ref[...], hidden_ref[...]
    for k in range(RING):
        both = dot(rows_ref[k, :, :WIDTH], grads, 0, 0).astype(BF16)
        down = swap_halves(dot(hidden, rows_ref[k, :, WIDTH:], 0, 0)).astype(BF16)
        for half, ref in enumerate((own_ref, send_ref)):
            at = 2 * half * WIDTH
            ref[0, k] = both[:, at : at + WIDTH]
            ref[1, k] = both[:, at + WIDTH : at + 2 * WIDTH]
            ref[2, k] = down[half * WIDTH : (half + 1) * WIDTH]


def joined_kernel(core_ref, own_ref, got_ref, gate_ref, up_ref, down_ref):
    core = core_ref[0]
    for k in range(RING):
        for side, ref in ((core, own_ref), (1 - core, got_ref)):
            at = 2 * k + side
            gate_ref[at] = ref[0, k]
            up_ref[at] = ref[1, k]
            down_ref[:, pl.ds(pl.multiple_of(at * WIDTH, WIDTH), WIDTH)] = ref[2, k]


def return_kernel(parts_ref, back_ref, send_ref):
    total = parts_ref[0].astype(F32)
    for k in range(1, RING):
        total = total + parts_ref[k].astype(F32)
    rows = dot(ones_where(slot_rows((SLOTS, ROWS), 1)), total.astype(BF16), 1, 0)
    rows = rows.astype(BF16).reshape(PEERS, PAD, WIDTH)
    send_ref[...] = rows + back_ref[...]


def token_kernel(got_ref, pick_ref, cot_ref, copies_ref):
    got = got_ref[...].reshape(SLOTS, WIDTH)
    rows = (cot_ref[...].astype(F32) + dot(pick_ref[...], got, 0, 0)).astype(BF16)
    for k in range(RING):
        copies_ref[k] = rows


def state_kernel(place_ref, got_ref, state_ref, reach_ref):
    got = got_ref[...].reshape(SLOTS, WIDTH)
    state_ref[...] = dot(ones_where(row_of_peer(CAP) | row_of_peer(CAP + 1)), got, 1, 0)
    spread = dot(ones_where(row_of_peer(CAP + 2)), got, 1, 0).astype(BF16)
    lane, peer = iota((WIDTH, PEERS), 0), iota((WIDTH, PEERS), 1)
    fold = (lane == peer) | (lane == peer + PEERS) | (lane == peer + 2 * PEERS)
    logs = dot(spread, ones_where(fold), 1, 0)
    here = place_ref[0]
    a, b = iota((PEERS, PEERS), 0), iota((PEERS, PEERS), 1)
    later = dot(jnp.where(b > here, logs, 0.0), ones_where(a < b, F32), 1, 0, EXACT)
    before = dot(jnp.where(b < here, logs, 0.0), ones_where(a > b, F32), 1, 0, EXACT)
    later = jnp.where(b > here, jnp.exp(later), 0.0)
    before = jnp.where(b < here, jnp.exp(before), 0.0)
    half = KEY_DIM // 2
    first = iota((half, WIDTH), 1) < VAL_DIM
    for k in range(PEERS):
        for side, value in enumerate((later, before)):
            column = value[:, k : k + 1]
            reach_ref[side, k] = jnp.where(first, column[:half], column[half:])


def source_kernel(
    place_ref, rows_ref, weight_ref, normed_ref, inv_ref, mix_ref, query_fwd_ref, query_bwd_ref,
    send_ref, grad_ref,
):
    here = place_ref[0]
    rows = jnp.concatenate([rows_ref[c, k] for k in range(RING) for c in range(2)], axis=1)
    grad = dot(rows, weight_ref[...], 1, 1)
    normed = normed_ref[...]
    mean = jnp.mean(grad * normed, axis=1, keepdims=True)
    grad = inv_ref[...] * (grad - normed * mean)
    grad_ref[...] = grad
    twice = jnp.concatenate([grad, grad], axis=1)
    half = KEY_DIM // 2
    first = iota((half, WIDTH), 1) < VAL_DIM
    states = []
    for ref in (query_fwd_ref, query_bwd_ref):
        state = dot(ref[...], twice, 1, 0, EXACT)
        states.append(jnp.where(first, state[:half], state[half:]))
    lane = iota((KEY_DIM, WIDTH), 1)
    for k in range(2 * RING):
        part = dot(rows[:, k * WIDTH : (k + 1) * WIDTH], mix_ref[...], 0, 0)
        for side in range(2):
            at, peer = side * VAL_DIM, 2 * k + side
            both = jnp.where(lane < VAL_DIM, part[at : at + 32], part[at + 32 : at + 64])
            send_ref[peer, :KEY_DIM] = both.astype(BF16)
            send_ref[peer, KEY_DIM:] = jnp.where(peer < here, states[0], states[1]).astype(BF16)


def final_kernel(
    got_ref, reach_ref, state_ref, cum_ref, key_ref, val_ref, pre_ref, speed_ref,
    keys_mix_ref, vals_mix_ref, decay_mix_ref,
    proj_ref, keys_ref, vals_ref, logit_ref,
):
    proj = got_ref[0, :KEY_DIM].astype(F32)
    flow = got_ref[0, KEY_DIM:].astype(F32)
    packed = [flow * reach_ref[0, 0], flow * reach_ref[1, 0]]
    for k in range(1, PEERS):
        proj = proj + got_ref[k, :KEY_DIM].astype(F32)
        flow = got_ref[k, KEY_DIM:].astype(F32)
        packed = [total + flow * reach_ref[side, k] for side, total in enumerate(packed)]
    flow_fwd, flow_bwd = (
        jnp.concatenate([total[:, :VAL_DIM], total[:, VAL_DIM:]], axis=0) for total in packed
    )
    proj_ref[:KEY_DIM] = proj[:, :VAL_DIM]
    proj_ref[KEY_DIM:] = proj[:, VAL_DIM:]
    cum = cum_ref[...]
    total = cum[:, TOK - 1 : TOK]
    keys, vals = key_ref[...].astype(F32), val_ref[...].astype(F32)
    scale_fwd, scale_bwd = jnp.exp(total - cum), jnp.exp(cum)
    grad_fwd = dot(flow_fwd, vals, 1, 0, EXACT) * scale_fwd
    grad_bwd = dot(flow_bwd, vals, 1, 0, EXACT) * scale_bwd
    keys_ref[...] = keys_mix_ref[...] + grad_fwd + grad_bwd
    vals_ref[...] = (
        vals_mix_ref[...]
        + dot(flow_fwd, keys * scale_fwd, 0, 0, EXACT)
        + dot(flow_bwd, keys * scale_bwd, 0, 0, EXACT)
    )
    state = state_ref[...]
    flow = flow_fwd * state[:, :VAL_DIM] + flow_bwd * state[:, VAL_DIM:]
    factor = jnp.exp(total) * jnp.sum(flow, axis=1, keepdims=True)
    grad_fwd, grad_bwd = grad_fwd * keys, grad_bwd * keys
    at_end = factor + jnp.sum(grad_fwd, axis=1, keepdims=True)
    row, col = iota((TOK, TOK), 0), iota((TOK, TOK), 1)
    tail = dot(grad_bwd - grad_fwd, ones_where(row >= col, F32), 1, 0, EXACT)
    decay = decay_mix_ref[...] + tail + at_end
    diagonal = iota((KEY_DIM, KEY_DIM), 0) == iota((KEY_DIM, KEY_DIM), 1)
    speed = jnp.sum(jnp.where(diagonal, speed_ref[...], 0.0), axis=1, keepdims=True)
    pre = pre_ref[...].astype(F32)
    logit_ref[...] = decay * speed * jax.nn.sigmoid(-pre)


SCALAR = pl.BlockSpec(memory_space=pltpu.SMEM)
WHOLE = pl.BlockSpec(memory_space=pltpu.VMEM)


def on_chip(array):
    return pltpu.with_memory_space_constraint(array, pltpu.VMEM)


def off_chip(array):
    return pltpu.with_memory_space_constraint(array, pltpu.HBM)


def call(kernel, outs, *args, scalars=0, stored=()):
    shapes = [
        (pltpu.HBM if k in stored else pltpu.VMEM)(shape, dtype)
        for k, (shape, dtype) in enumerate(outs)
    ]
    return pl.pallas_call(
        kernel,
        out_shape=shapes,
        in_specs=[SCALAR] * scalars + [WHOLE] * (len(args) - scalars),
        out_specs=[WHOLE] * len(shapes),
        compiler_params=pltpu.CompilerParams(vmem_limit_bytes=24 << 20),
    )(*args)


def inner(scaled, keys, vals, cum, lower):
    gap = cum[:, :, None] - cum[:, None, :]
    weight = jnp.exp(jnp.where(lower, gap, -gap))
    scores = jnp.einsum("ct,cs,cts->ts", scaled, keys, weight)
    return jnp.einsum("ts,vs->vt", scores, vals)


def carried(scaled, cum, fwd_in, bwd_in):
    total = cum[:, -1:]
    return jnp.einsum("ct,cv->vt", scaled * jnp.exp(cum), fwd_in) + jnp.einsum(
        "ct,cv->vt", scaled * jnp.exp(total - cum), bwd_in
    )


def body(
    queries,
    input_key_matrix,
    input_value_matrix,
    decay_preactivation,
    extra_log_decay,
    channel_decay_speed,
    output_weight_matrix,
    stored_expert_rows,
    chosen_expert_index,
    expert_combine_weight,
    cotangent,
    expert_gate_weight,
    expert_up_weight,
    expert_down_weight,
):
    sp = ("z", "x")
    core = lax.axis_index("core")
    core_at = core.reshape(1).astype(jnp.int32)
    place_at = lax.axis_index(sp).reshape(1).astype(jnp.int32)
    speed = channel_decay_speed.reshape(1, KEY_DIM)
    swap = [(0, 1), (1, 0)]

    def exchanged(array, axis):
        return lax.all_to_all(array, axis, split_axis=0, concat_axis=0, tiled=True)

    gate, up, down = expert_gate_weight[0], expert_up_weight[0], expert_down_weight[0]
    gate_blocks = gate.reshape(2 * RING, WIDTH, WIDTH)
    up_blocks = up.reshape(2 * RING, WIDTH, WIDTH)
    ids, share = off_chip(chosen_expert_index.T), off_chip(expert_combine_weight.T)
    send, token, pick, lead, tail, cum = call(
        dispatch_kernel,
        [
            ((PEERS, PAD, WIDTH), BF16),
            ((TOK, WIDTH), BF16),
            ((SLOTS, TOK), BF16),
            ((2, LEAD, TOK), BF16),
            ((2, LEAD, TOK), BF16),
            ((KEY_DIM, TOK), F32),
        ],
        ids,
        share,
        off_chip(stored_expert_rows),
        off_chip(cotangent),
        off_chip(input_key_matrix),
        off_chip(input_value_matrix),
        off_chip(decay_preactivation),
        off_chip(extra_log_decay),
        off_chip(speed),
        stored=(0, 2),
    )
    got = exchanged(send, sp)
    tokens = lax.all_gather(token, "y", axis=0, tiled=False)
    (send,) = call(
        spread_kernel,
        [((LEAD, 12 * WIDTH), BF16)],
        on_chip(tokens),
        share,
        on_chip(lead),
        on_chip(tail),
        stored=(0,),
    )
    far = exchanged(send.reshape(PEERS, 8, 12 * WIDTH), sp).reshape(LEAD, 12 * WIDTH)
    rows, back = call(
        arrival_kernel,
        [((ROWS, WIDTH), BF16), ((PEERS, PAD, WIDTH), BF16)],
        on_chip(got),
        stored=(1,),
    )
    near = lax.all_gather(rows, "y", axis=0, tiled=False)
    kept, theirs = call(
        slice_kernel,
        [((3, RING, WIDTH, WIDTH), BF16)] * 2,
        core_at,
        place_at,
        off_chip(gate_blocks),
        off_chip(up_blocks),
        off_chip(down),
        scalars=2,
        stored=(1,),
    )
    swapped = lax.ppermute(theirs, "core", swap)
    own, send, rows = call(
        forward_kernel,
        [
            ((2, ROWS, 3 * WIDTH), F32),
            ((2, ROWS, 3 * WIDTH), BF16),
            ((RING, ROWS, 2 * WIDTH), BF16),
        ],
        near,
        far,
        on_chip(kept),
        swapped,
    )
    crossed = lax.ppermute(send, "core", swap)
    partials, grads, hidden = call(
        partial_kernel,
        [
            ((RING, ROWS, WIDTH), BF16),
            ((ROWS, 4 * WIDTH), BF16),
            ((ROWS, 2 * WIDTH), BF16),
        ],
        on_chip(own),
        on_chip(crossed),
        on_chip(kept),
        swapped,
        stored=(1, 2),
    )
    parts = exchanged(partials, "y")
    (send,) = call(
        return_kernel, [((PEERS, PAD, WIDTH), BF16)], on_chip(parts), off_chip(back)
    )
    returned = on_chip(exchanged(send, sp))
    (copies,) = call(
        token_kernel, [((RING, TOK, WIDTH), BF16)], returned, off_chip(pick), off_chip(cotangent)
    )
    row = iota((TOK, TOK), 0)
    cum, queries, key_in, val_in, row, copies = lax.optimization_barrier(
        (cum, queries, input_key_matrix, input_value_matrix, row, copies)
    )
    full_rows = exchanged(copies, "y")
    full_rows = lax.all_gather(full_rows, "core", axis=0, tiled=False)

    state, reach = call(
        state_kernel,
        [((KEY_DIM, WIDTH), F32), ((2, PEERS, KEY_DIM // 2, WIDTH), F32)],
        place_at,
        returned,
        scalars=1,
    )
    scaled = queries.astype(F32) * KEY_DIM ** (-0.5)
    keys = key_in.astype(F32)
    vals = val_in.astype(F32)
    lower = row >= iota((TOK, TOK), 1)
    fwd_in, bwd_in = state[:, :VAL_DIM], state[:, VAL_DIM:]
    inner_out, pull_inner = jax.vjp(
        lambda *args: inner(*args, lower), scaled, keys, vals, cum
    )
    carried_out, pull_carried = jax.vjp(
        lambda s, c: carried(s, c, fwd_in, bwd_in), scaled, cum
    )
    mixed = inner_out + carried_out
    inv_rms = lax.rsqrt(jnp.mean(mixed * mixed, axis=0, keepdims=True) + 1e-06)
    normed = mixed * inv_rms
    normed_t = normed.T
    mix_t = normed_t.astype(BF16)
    mix_twice = jnp.concatenate([mix_t, mix_t], axis=1)
    query_fwd = scaled * jnp.exp(cum)
    query_bwd = scaled * jnp.exp(cum[:, -1:] - cum)
    send, grad_mixed_t = call(
        source_kernel,
        [((PEERS, 3 * KEY_DIM // 2, WIDTH), BF16), ((TOK, VAL_DIM), F32)],
        place_at,
        on_chip(full_rows),
        off_chip(output_weight_matrix.T),
        normed_t,
        inv_rms.reshape(TOK, 1),
        mix_twice,
        query_fwd,
        query_bwd,
        scalars=1,
    )
    got = exchanged(send, sp)
    own, send = call(
        weight_kernel,
        [((3, RING, WIDTH, WIDTH), BF16)] * 2,
        off_chip(rows),
        off_chip(grads),
        off_chip(hidden),
        stored=range(2),
    )
    crossed = lax.ppermute(send, "core", swap)
    grad_gate, grad_up, grad_down = call(
        joined_kernel,
        [
            ((2 * RING, WIDTH, WIDTH), BF16),
            ((2 * RING, WIDTH, WIDTH), BF16),
            ((WIDTH, MODEL), BF16),
        ],
        core_at,
        off_chip(own),
        crossed,
        scalars=1,
        stored=range(3),
    )
    grad_mixed = grad_mixed_t.T
    grad_scaled, grad_keys, grad_vals, grad_cum = pull_inner(grad_mixed)
    grad_scaled_in, grad_cum_in = pull_carried(grad_mixed)
    grad_queries = (grad_scaled + grad_scaled_in) * KEY_DIM ** (-0.5)
    tail_mask = ones_where(iota((TOK, TOK), 0) >= iota((TOK, TOK), 1), F32)
    grad_decay = dot(grad_cum + grad_cum_in, tail_mask, 1, 0, EXACT)
    grad_out_proj, grad_keys, grad_values, grad_logit = call(
        final_kernel,
        [
            ((2 * KEY_DIM, VAL_DIM), F32),
            ((KEY_DIM, TOK), F32),
            ((VAL_DIM, TOK), F32),
            ((KEY_DIM, TOK), F32),
        ],
        on_chip(got),
        reach,
        state,
        cum,
        input_key_matrix,
        input_value_matrix,
        decay_preactivation,
        speed,
        grad_keys,
        grad_vals,
        grad_decay,
        stored=range(4),
    )
    return (
        grad_queries,
        grad_keys,
        grad_values,
        grad_logit,
        grad_out_proj,
        grad_gate.reshape(1, MODEL, WIDTH),
        grad_up.reshape(1, MODEL, WIDTH),
        grad_down[None],
    )


def solution(mesh):
    fine = Mesh(mesh.devices.reshape(8, 4, 8, 2), ("z", "x", "y", "core"))
    sp, tp = ("z", "x"), ("y", "core")
    in_specs = (
        P(tp, sp),
        P(tp, sp),
        P(tp, sp),
        P(tp, sp),
        P(tp, sp),
        P(tp),
        P(None, tp),
        P(sp, tp),
        P(sp, None),
        P(sp, None),
        P(sp, tp),
        P(sp, None, tp),
        P(sp, None, tp),
        P(sp, tp, None),
    )
    out_specs = (
        P(tp, sp),
        P(tp, sp),
        P(tp, sp),
        P(tp, sp),
        P(sp, tp),
        P(sp, None, tp),
        P(sp, None, tp),
        P(sp, tp, None),
    )

    return jax.shard_map(body, mesh=fine, in_specs=in_specs, out_specs=out_specs, check_vma=False)
```

```python
import jax
import jax.numpy as jnp
from jax import lax
from jax.experimental import pallas as pl
from jax.experimental.pallas import tpu as pltpu
from jax.sharding import Mesh
from jax.sharding import PartitionSpec as P


KEY_DIM = 32
VAL_DIM = 64
TOK = 128
PEERS = 32
CAP = 12
PAD = 16
RING = 8
SLOTS = PEERS * PAD
ROWS = PEERS * CAP
WIDTH = 128
MODEL = 2048

F32 = jnp.float32
BF16 = jnp.bfloat16
EXACT = lax.Precision.HIGHEST


def dot(a, b, da, db, precision=None):
    return lax.dot_general(
        a, b, (((da,), (db,)), ((), ())), preferred_element_type=F32, precision=precision
    )


def iota(shape, dim):
    return lax.broadcasted_iota(jnp.int32, shape, dim)


def ones_where(mask, dtype=BF16):
    return jnp.where(mask, 1.0, 0.0).astype(dtype)


def split_two(value):
    high = value.astype(BF16).astype(F32)
    return high, (value - high).astype(BF16).astype(F32)


def split_three(value):
    high, rest = split_two(value)
    return high, rest, (value - high - rest).astype(BF16).astype(F32)


def compact_rows(shape, compact_dim):
    row = iota(shape, compact_dim)
    peer = (row * 5462) >> 16
    return peer * PAD + (row - peer * CAP) == iota(shape, 1 - compact_dim)


def row_of_peer(place):
    return iota((PEERS, SLOTS), 1) == iota((PEERS, SLOTS), 0) * PAD + place


def start_all(pairs, sems):
    copies = [
        pltpu.make_async_copy(source, target, sems.at[k]) for k, (source, target) in enumerate(pairs)
    ]
    for copy in copies:
        copy.start()
    return copies


def dispatch_kernel(
    ids_ref, share_ref, x_ref, cot_ref, key_ref, val_ref, pre_ref, extra_ref, speed_ref,
    send_ref, pick_ref, cum_ref,
):
    expert = iota((PEERS, TOK), 0)
    named = [ids_ref[k : k + 1, :] == expert for k in range(2)]
    row, col = iota((TOK, TOK), 0), iota((TOK, TOK), 1)
    rank = dot(ones_where(named[0] | named[1]), ones_where(row < col), 1, 0)
    place = iota((PEERS, PAD, TOK), 1).astype(F32)
    cot = cot_ref[...].astype(F32)
    picks, grads = [], None
    for k in range(2):
        at = jnp.where(named[k], rank, -1.0)
        pick = jnp.where(at[:, None, :] == place, 1.0, 0.0).reshape(SLOTS, TOK).astype(BF16)
        share = jnp.sum(jnp.where(row == col, share_ref[k : k + 1, :], 0.0), axis=1, keepdims=True)
        part = dot(pick, (share * cot).astype(BF16), 1, 0)
        grads = part if grads is None else grads + part
        picks.append(pick)
    pick = picks[0] + picks[1]
    pick_ref[...] = pick
    rows = jnp.concatenate([dot(pick, x_ref[...], 1, 0), grads], axis=1)

    pre = pre_ref[...].astype(F32)
    log_sig = jnp.minimum(pre, 0.0) - jnp.log1p(jnp.exp(-jnp.abs(pre)))
    diagonal = iota((KEY_DIM, KEY_DIM), 0) == iota((KEY_DIM, KEY_DIM), 1)
    speed = jnp.sum(jnp.where(diagonal, speed_ref[...], 0.0), axis=1, keepdims=True)
    decay = speed * log_sig + extra_ref[...]
    cum = dot(decay, ones_where(row <= col, F32), 1, 0, EXACT)
    cum_ref[...] = cum
    total = cum[:, TOK - 1 : TOK]
    keys, vals = key_ref[...].astype(F32), val_ref[...].astype(F32)
    sums = jnp.concatenate(
        [
            dot(keys * jnp.exp(total - cum), vals, 1, 1, EXACT),
            dot(keys * jnp.exp(cum), vals, 1, 1, EXACT),
        ],
        axis=1,
    )
    state = jnp.concatenate(split_two(sums), axis=1)
    lane = iota((KEY_DIM, 2 * WIDTH), 1)
    logs = jnp.zeros((KEY_DIM, 2 * WIDTH), F32)
    for k, part in enumerate(split_three(total)):
        logs = jnp.where(lane == k, part, logs)
    place = iota((PEERS, PAD, 2 * WIDTH), 1)
    block = rows.reshape(PEERS, PAD, 2 * WIDTH)
    block = jnp.where(place == CAP, state[:, None, :], block)
    block = jnp.where(place == CAP + 1, logs[:, None, :], block)
    send_ref[...] = block.astype(BF16)


def arrival_kernel(got_ref, copies_ref, back_ref, rows_ref, sems):
    got = got_ref[...].reshape(SLOTS, 2 * WIDTH)
    rows_ref[...] = dot(ones_where(compact_rows((ROWS, SLOTS), 0)), got, 1, 0).astype(BF16)
    copies = start_all([(rows_ref, copies_ref.at[k]) for k in range(RING)], sems)
    both = dot(ones_where(row_of_peer(CAP)), got, 1, 0)
    state = both[:, :WIDTH] + both[:, WIDTH:]
    logs = dot(ones_where(row_of_peer(CAP + 1)), got, 1, 0)
    log = jnp.sum(logs, axis=1, keepdims=True)
    a, b = iota((PEERS, PEERS), 0), iota((PEERS, PEERS), 1)
    gap_fwd = dot(ones_where(b < a, F32), jnp.where(a > b, log, 0.0), 1, 0, EXACT)
    gap_bwd = dot(ones_where(b > a, F32), jnp.where(a < b, log, 0.0), 1, 0, EXACT)
    fwd = dot(jnp.where(b < a, jnp.exp(gap_fwd), 0.0), state, 1, 0, EXACT)
    bwd = dot(jnp.where(b > a, jnp.exp(gap_bwd), 0.0), state, 1, 0, EXACT)
    lane = iota((PEERS, WIDTH), 1)
    high, low = split_two(jnp.where(lane < VAL_DIM, fwd, bwd))
    peer = iota((PEERS, WIDTH), 0)
    spread = jnp.zeros((PEERS, WIDTH), F32)
    for k, part in enumerate(split_three(log)):
        spread = jnp.where(lane == peer + k * PEERS, part, spread)
    all_logs = jnp.sum(spread, axis=0, keepdims=True)
    place = iota((PEERS, PAD, WIDTH), 1)
    block = jnp.where(place == CAP, high[:, None, :], 0.0)
    block = jnp.where(place == CAP + 1, low[:, None, :], block)
    block = jnp.where(place == CAP + 2, all_logs[:, None, :], block)
    back_ref[...] = block.astype(BF16)
    for copy in copies:
        copy.wait()


def slice_kernel(core_ref, place_ref, gate_ref, up_ref, down_ref, own_ref, out_ref):
    core = core_ref[0]
    for side, ref in ((core, own_ref), (1 - core, out_ref)):
        for k in range(RING):
            at = 2 * k + side
            ref[0, k] = gate_ref[at]
            ref[1, k] = up_ref[at]
            ref[2, k] = down_ref[:, pl.ds(pl.multiple_of(at * WIDTH, WIDTH), WIDTH)]


def forward_kernel(rows_ref, own_ref, swapped_ref, out_ref, send_ref):
    pre = jnp.zeros((ROWS, 4 * WIDTH), F32)
    grad = jnp.zeros((ROWS, 2 * WIDTH), F32)
    for k in range(0, RING, 2):
        weights, downs = [], []
        for j in (k, k + 1):
            parts = [own_ref[0, j], own_ref[1, j], swapped_ref[0, j], swapped_ref[1, j]]
            weights.append(jnp.concatenate(parts, axis=1))
            downs.append(jnp.concatenate([own_ref[2, j], swapped_ref[2, j]], axis=0))
        x = jnp.concatenate([rows_ref[k, :, :WIDTH], rows_ref[k + 1, :, :WIDTH]], axis=1)
        y = jnp.concatenate([rows_ref[k, :, WIDTH:], rows_ref[k + 1, :, WIDTH:]], axis=1)
        pre = pre + dot(x, jnp.concatenate(weights, axis=0), 1, 0)
        grad = grad + dot(y, jnp.concatenate(downs, axis=1), 1, 1)
    mine = jnp.concatenate([pre[:, : 2 * WIDTH], grad[:, :WIDTH]], axis=1)
    theirs = jnp.concatenate([pre[:, 2 * WIDTH :], grad[:, WIDTH:]], axis=1)
    out_ref[0] = mine
    out_ref[1] = theirs
    send_ref[0] = theirs.astype(BF16)
    send_ref[1] = mine.astype(BF16)


def partial_kernel(
    own_ref, got_ref, kept_ref, swapped_ref, out_ref, grads_out, hidden_out,
    grads_ref, hidden_ref, sems,
):
    grads = []
    for half in range(2):
        total = own_ref[half] + got_ref[half].astype(F32)
        gate_pre, up_pre = total[:, :WIDTH], total[:, WIDTH : 2 * WIDTH]
        grad_hidden = total[:, 2 * WIDTH :]
        gate_sig = jax.nn.sigmoid(gate_pre)
        gate_act = gate_pre * gate_sig
        hidden_ref[:, half * WIDTH : (half + 1) * WIDTH] = (gate_act * up_pre).astype(BF16)
        slope = gate_sig * (1.0 + gate_pre * (1.0 - gate_sig))
        grads.append((grad_hidden * up_pre * slope).astype(BF16))
        grads.append((grad_hidden * gate_act).astype(BF16))
    grads_ref[...] = jnp.concatenate(grads, axis=1)
    copies = start_all([(grads_ref, grads_out), (hidden_ref, hidden_out)], sems)
    grads = grads_ref[...]
    for k in range(RING):
        weights = jnp.concatenate(
            [kept_ref[0, k], kept_ref[1, k], swapped_ref[0, k], swapped_ref[1, k]], axis=1
        )
        out_ref[k] = dot(grads, weights, 1, 1).astype(BF16)
    for copy in copies:
        copy.wait()


def weight_kernel(rows_ref, grads_ref, hidden_ref, own_ref, send_ref):
    grads, hidden = grads_ref[...], hidden_ref[...]
    for k in range(RING):
        both = dot(rows_ref[k, :, :WIDTH], grads, 0, 0).astype(BF16)
        down = dot(hidden, rows_ref[k, :, WIDTH:], 0, 0).astype(BF16)
        for half, ref in enumerate((own_ref, send_ref)):
            at = 2 * half * WIDTH
            ref[0, k] = both[:, at : at + WIDTH]
            ref[1, k] = both[:, at + WIDTH : at + 2 * WIDTH]
            ref[2, k] = down[half * WIDTH : (half + 1) * WIDTH]


def joined_kernel(core_ref, own_ref, got_ref, gate_ref, up_ref, down_ref):
    core = core_ref[0]
    for k in range(RING):
        for side, ref in ((core, own_ref), (1 - core, got_ref)):
            at = 2 * k + side
            gate_ref[at] = ref[0, k]
            up_ref[at] = ref[1, k]
            down_ref[:, pl.ds(pl.multiple_of(at * WIDTH, WIDTH), WIDTH)] = ref[2, k]


def return_kernel(parts_ref, back_ref, send_ref):
    total = parts_ref[0].astype(F32)
    for k in range(1, RING):
        total = total + parts_ref[k].astype(F32)
    rows = dot(ones_where(compact_rows((SLOTS, ROWS), 1)), total.astype(BF16), 1, 0)
    rows = rows.astype(BF16).reshape(PEERS, PAD, WIDTH)
    send_ref[...] = rows + back_ref[...]


def token_kernel(got_ref, pick_ref, cot_ref, copies_ref, rows_ref, sems):
    got = got_ref[...].reshape(SLOTS, WIDTH)
    rows_ref[...] = (cot_ref[...].astype(F32) + dot(pick_ref[...], got, 0, 0)).astype(BF16)
    for copy in start_all([(rows_ref, copies_ref.at[k]) for k in range(RING)], sems):
        copy.wait()


def state_kernel(place_ref, got_ref, state_ref, reach_ref):
    got = got_ref[...].reshape(SLOTS, WIDTH)
    state_ref[...] = dot(ones_where(row_of_peer(CAP) | row_of_peer(CAP + 1)), got, 1, 0)
    spread = dot(ones_where(row_of_peer(CAP + 2)), got, 1, 0).astype(BF16)
    lane, peer = iota((WIDTH, PEERS), 0), iota((WIDTH, PEERS), 1)
    fold = (lane == peer) | (lane == peer + PEERS) | (lane == peer + 2 * PEERS)
    logs = dot(spread, ones_where(fold), 1, 0)
    here = place_ref[0]
    a, b = iota((PEERS, PEERS), 0), iota((PEERS, PEERS), 1)
    later = dot(jnp.where(b > here, logs, 0.0), ones_where(a < b, F32), 1, 0, EXACT)
    before = dot(jnp.where(b < here, logs, 0.0), ones_where(a > b, F32), 1, 0, EXACT)
    later = jnp.where(b > here, jnp.exp(later), 0.0)
    before = jnp.where(b < here, jnp.exp(before), 0.0)
    half = KEY_DIM // 2
    first = iota((half, WIDTH), 1) < VAL_DIM
    for k in range(PEERS):
        for side, value in enumerate((later, before)):
            column = value[:, k : k + 1]
            reach_ref[side, k] = jnp.where(first, column[:half], column[half:])


def source_kernel(
    place_ref, rows_ref, weight_ref, normed_ref, inv_ref, mix_ref, query_fwd_ref, query_bwd_ref,
    send_ref, grad_ref, proj_ref, state_ref, sems,
):
    here = place_ref[0]
    rows = jnp.concatenate([rows_ref[c, k] for k in range(RING) for c in range(2)], axis=1)
    lane = iota((KEY_DIM, WIDTH), 1)
    for k in range(2 * RING):
        part = dot(rows[:, k * WIDTH : (k + 1) * WIDTH], mix_ref[...], 0, 0)
        for side in range(2):
            at = side * VAL_DIM
            both = jnp.where(lane < VAL_DIM, part[at : at + 32], part[at + 32 : at + 64])
            proj_ref[2 * k + side] = both.astype(BF16)
    first_part = pltpu.make_async_copy(proj_ref, send_ref.at[:, :KEY_DIM], sems.at[0])
    first_part.start()
    grad = dot(rows, weight_ref[...], 1, 1)
    normed = normed_ref[...]
    mean = jnp.mean(grad * normed, axis=1, keepdims=True)
    grad = inv_ref[...] * (grad - normed * mean)
    grad_ref[...] = grad
    twice = jnp.concatenate([grad, grad], axis=1)
    half = KEY_DIM // 2
    first = iota((half, WIDTH), 1) < VAL_DIM
    states = []
    for ref in (query_fwd_ref, query_bwd_ref):
        state = dot(ref[...], twice, 1, 0, EXACT)
        states.append(jnp.where(first, state[:half], state[half:]))
    for peer in range(PEERS):
        state_ref[peer] = jnp.where(peer < here, states[0], states[1]).astype(BF16)
    second_part = pltpu.make_async_copy(state_ref, send_ref.at[:, KEY_DIM:], sems.at[1])
    second_part.start()
    first_part.wait()
    second_part.wait()


def final_kernel(
    got_ref, reach_ref, state_ref, cum_ref, key_ref, val_ref, pre_ref, speed_ref,
    keys_mix_ref, vals_mix_ref, decay_mix_ref,
    proj_ref, keys_ref, vals_ref, logit_ref,
):
    proj = got_ref[0, :KEY_DIM].astype(F32)
    flow = got_ref[0, KEY_DIM:].astype(F32)
    packed = [flow * reach_ref[0, 0], flow * reach_ref[1, 0]]
    for k in range(1, PEERS):
        proj = proj + got_ref[k, :KEY_DIM].astype(F32)
        flow = got_ref[k, KEY_DIM:].astype(F32)
        packed = [total + flow * reach_ref[side, k] for side, total in enumerate(packed)]
    flow_fwd, flow_bwd = (
        jnp.concatenate([total[:, :VAL_DIM], total[:, VAL_DIM:]], axis=0) for total in packed
    )
    proj_ref[:KEY_DIM] = proj[:, :VAL_DIM]
    proj_ref[KEY_DIM:] = proj[:, VAL_DIM:]
    cum = cum_ref[...]
    total = cum[:, TOK - 1 : TOK]
    keys, vals = key_ref[...].astype(F32), val_ref[...].astype(F32)
    scale_fwd, scale_bwd = jnp.exp(total - cum), jnp.exp(cum)
    grad_fwd = dot(flow_fwd, vals, 1, 0, EXACT) * scale_fwd
    grad_bwd = dot(flow_bwd, vals, 1, 0, EXACT) * scale_bwd
    keys_ref[...] = keys_mix_ref[...] + grad_fwd + grad_bwd
    vals_ref[...] = (
        vals_mix_ref[...]
        + dot(flow_fwd, keys * scale_fwd, 0, 0, EXACT)
        + dot(flow_bwd, keys * scale_bwd, 0, 0, EXACT)
    )
    state = state_ref[...]
    flow = flow_fwd * state[:, :VAL_DIM] + flow_bwd * state[:, VAL_DIM:]
    factor = jnp.exp(total) * jnp.sum(flow, axis=1, keepdims=True)
    grad_fwd, grad_bwd = grad_fwd * keys, grad_bwd * keys
    at_end = factor + jnp.sum(grad_fwd, axis=1, keepdims=True)
    row, col = iota((TOK, TOK), 0), iota((TOK, TOK), 1)
    tail = dot(grad_bwd - grad_fwd, ones_where(row >= col, F32), 1, 0, EXACT)
    decay = decay_mix_ref[...] + tail + at_end
    diagonal = iota((KEY_DIM, KEY_DIM), 0) == iota((KEY_DIM, KEY_DIM), 1)
    speed = jnp.sum(jnp.where(diagonal, speed_ref[...], 0.0), axis=1, keepdims=True)
    pre = pre_ref[...].astype(F32)
    logit_ref[...] = decay * speed * jax.nn.sigmoid(-pre)


SCALAR = pl.BlockSpec(memory_space=pltpu.SMEM)
WHOLE = pl.BlockSpec(memory_space=pltpu.VMEM)
OUTSIDE = pl.BlockSpec(memory_space=pltpu.HBM)


def on_chip(array):
    return pltpu.with_memory_space_constraint(array, pltpu.VMEM)


def off_chip(array):
    return pltpu.with_memory_space_constraint(array, pltpu.HBM)


def call(kernel, outs, *args, scalars=0, stored=(), manual=(), scratch=()):
    shapes = [
        (pltpu.HBM if k in stored else pltpu.VMEM)(shape, dtype)
        for k, (shape, dtype) in enumerate(outs)
    ]
    return pl.pallas_call(
        kernel,
        out_shape=shapes,
        in_specs=[SCALAR] * scalars + [WHOLE] * (len(args) - scalars),
        out_specs=[OUTSIDE if k in manual else WHOLE for k in range(len(shapes))],
        scratch_shapes=list(scratch),
        compiler_params=pltpu.CompilerParams(vmem_limit_bytes=24 << 20),
    )(*args)


def inner(scaled, keys, vals, cum, lower):
    gap = cum[:, :, None] - cum[:, None, :]
    weight = jnp.exp(jnp.where(lower, gap, -gap))
    scores = jnp.einsum("ct,cs,cts->ts", scaled, keys, weight)
    return jnp.einsum("ts,vs->vt", scores, vals)


def carried(scaled, cum, fwd_in, bwd_in):
    total = cum[:, -1:]
    return jnp.einsum("ct,cv->vt", scaled * jnp.exp(cum), fwd_in) + jnp.einsum(
        "ct,cv->vt", scaled * jnp.exp(total - cum), bwd_in
    )


def body(
    queries,
    input_key_matrix,
    input_value_matrix,
    decay_preactivation,
    extra_log_decay,
    channel_decay_speed,
    output_weight_matrix,
    stored_expert_rows,
    chosen_expert_index,
    expert_combine_weight,
    cotangent,
    expert_gate_weight,
    expert_up_weight,
    expert_down_weight,
):
    sp = ("z", "x")
    core = lax.axis_index("core")
    core_at = core.reshape(1).astype(jnp.int32)
    place_at = lax.axis_index(sp).reshape(1).astype(jnp.int32)
    speed = channel_decay_speed.reshape(1, KEY_DIM)
    swap = [(0, 1), (1, 0)]

    def exchanged(array, axis):
        return lax.all_to_all(array, axis, split_axis=0, concat_axis=0, tiled=True)

    gate, up, down = expert_gate_weight[0], expert_up_weight[0], expert_down_weight[0]
    gate_blocks = gate.reshape(2 * RING, WIDTH, WIDTH)
    up_blocks = up.reshape(2 * RING, WIDTH, WIDTH)
    send, pick, cum = call(
        dispatch_kernel,
        [((PEERS, PAD, 2 * WIDTH), BF16), ((SLOTS, TOK), BF16), ((KEY_DIM, TOK), F32)],
        off_chip(chosen_expert_index.T),
        off_chip(expert_combine_weight.T),
        off_chip(stored_expert_rows),
        off_chip(cotangent),
        off_chip(input_key_matrix),
        off_chip(input_value_matrix),
        off_chip(decay_preactivation),
        off_chip(extra_log_decay),
        off_chip(speed),
        stored=(1,),
    )
    got = exchanged(send, sp)
    copies, back = call(
        arrival_kernel,
        [((RING, ROWS, 2 * WIDTH), BF16), ((PEERS, PAD, WIDTH), BF16)],
        on_chip(got),
        stored=(0, 1),
        manual=(0,),
        scratch=(pltpu.VMEM((ROWS, 2 * WIDTH), BF16), pltpu.SemaphoreType.DMA((RING,))),
    )
    rows = exchanged(copies, "y")
    kept, theirs = call(
        slice_kernel,
        [((3, RING, WIDTH, WIDTH), BF16)] * 2,
        core_at,
        place_at,
        off_chip(gate_blocks),
        off_chip(up_blocks),
        off_chip(down),
        scalars=2,
        stored=(1,),
    )
    swapped = lax.ppermute(theirs, "core", swap)
    own, send = call(
        forward_kernel,
        [((2, ROWS, 3 * WIDTH), F32), ((2, ROWS, 3 * WIDTH), BF16)],
        rows,
        on_chip(kept),
        swapped,
    )
    crossed = lax.ppermute(send, "core", swap)
    partials, grads, hidden = call(
        partial_kernel,
        [
            ((RING, ROWS, WIDTH), BF16),
            ((ROWS, 4 * WIDTH), BF16),
            ((ROWS, 2 * WIDTH), BF16),
        ],
        on_chip(own),
        on_chip(crossed),
        on_chip(kept),
        swapped,
        stored=(1, 2),
        manual=(1, 2),
        scratch=(
            pltpu.VMEM((ROWS, 4 * WIDTH), BF16),
            pltpu.VMEM((ROWS, 2 * WIDTH), BF16),
            pltpu.SemaphoreType.DMA((2,)),
        ),
    )
    parts = exchanged(partials, "y")
    (send,) = call(
        return_kernel, [((PEERS, PAD, WIDTH), BF16)], on_chip(parts), off_chip(back)
    )
    returned = on_chip(exchanged(send, sp))
    (copies,) = call(
        token_kernel,
        [((RING, TOK, WIDTH), BF16)],
        returned,
        off_chip(pick),
        off_chip(cotangent),
        stored=(0,),
        manual=(0,),
        scratch=(pltpu.VMEM((TOK, WIDTH), BF16), pltpu.SemaphoreType.DMA((RING,))),
    )
    row = iota((TOK, TOK), 0)
    cum, queries, key_in, val_in, row, copies = lax.optimization_barrier(
        (cum, queries, input_key_matrix, input_value_matrix, row, copies)
    )
    full_rows = exchanged(copies, "y")
    full_rows = lax.all_gather(full_rows, "core", axis=0, tiled=False)

    state, reach = call(
        state_kernel,
        [((KEY_DIM, WIDTH), F32), ((2, PEERS, KEY_DIM // 2, WIDTH), F32)],
        place_at,
        returned,
        scalars=1,
    )
    scaled = queries.astype(F32) * KEY_DIM ** (-0.5)
    keys = key_in.astype(F32)
    vals = val_in.astype(F32)
    lower = row >= iota((TOK, TOK), 1)
    fwd_in, bwd_in = state[:, :VAL_DIM], state[:, VAL_DIM:]
    inner_out, pull_inner = jax.vjp(
        lambda *args: inner(*args, lower), scaled, keys, vals, cum
    )
    carried_out, pull_carried = jax.vjp(
        lambda s, c: carried(s, c, fwd_in, bwd_in), scaled, cum
    )
    mixed = inner_out + carried_out
    inv_rms = lax.rsqrt(jnp.mean(mixed * mixed, axis=0, keepdims=True) + 1e-06)
    normed = mixed * inv_rms
    normed_t = normed.T
    mix_t = normed_t.astype(BF16)
    mix_twice = jnp.concatenate([mix_t, mix_t], axis=1)
    query_fwd = scaled * jnp.exp(cum)
    query_bwd = scaled * jnp.exp(cum[:, -1:] - cum)
    send, grad_mixed_t = call(
        source_kernel,
        [((PEERS, 3 * KEY_DIM // 2, WIDTH), BF16), ((TOK, VAL_DIM), F32)],
        place_at,
        on_chip(full_rows),
        off_chip(output_weight_matrix.T),
        normed_t,
        inv_rms.reshape(TOK, 1),
        mix_twice,
        query_fwd,
        query_bwd,
        scalars=1,
        stored=(0,),
        manual=(0,),
        scratch=(
            pltpu.VMEM((PEERS, KEY_DIM, WIDTH), BF16),
            pltpu.VMEM((PEERS, KEY_DIM // 2, WIDTH), BF16),
            pltpu.SemaphoreType.DMA((2,)),
        ),
    )
    got = exchanged(send, sp)
    own, send = call(
        weight_kernel,
        [((3, RING, WIDTH, WIDTH), BF16)] * 2,
        off_chip(rows),
        off_chip(grads),
        off_chip(hidden),
        stored=range(2),
    )
    crossed = lax.ppermute(send, "core", swap)
    grad_gate, grad_up, grad_down = call(
        joined_kernel,
        [
            ((2 * RING, WIDTH, WIDTH), BF16),
            ((2 * RING, WIDTH, WIDTH), BF16),
            ((WIDTH, MODEL), BF16),
        ],
        core_at,
        off_chip(own),
        crossed,
        scalars=1,
        stored=range(3),
    )
    grad_mixed = grad_mixed_t.T
    grad_scaled, grad_keys, grad_vals, grad_cum = pull_inner(grad_mixed)
    grad_scaled_in, grad_cum_in = pull_carried(grad_mixed)
    grad_queries = (grad_scaled + grad_scaled_in) * KEY_DIM ** (-0.5)
    tail_mask = ones_where(iota((TOK, TOK), 0) >= iota((TOK, TOK), 1), F32)
    grad_decay = dot(grad_cum + grad_cum_in, tail_mask, 1, 0, EXACT)
    grad_out_proj, grad_keys, grad_values, grad_logit = call(
        final_kernel,
        [
            ((2 * KEY_DIM, VAL_DIM), F32),
            ((KEY_DIM, TOK), F32),
            ((VAL_DIM, TOK), F32),
            ((KEY_DIM, TOK), F32),
        ],
        on_chip(got),
        reach,
        state,
        cum,
        input_key_matrix,
        input_value_matrix,
        decay_preactivation,
        speed,
        grad_keys,
        grad_vals,
        grad_decay,
        stored=range(4),
    )
    return (
        grad_queries,
        grad_keys,
        grad_values,
        grad_logit,
        grad_out_proj,
        grad_gate.reshape(1, MODEL, WIDTH),
        grad_up.reshape(1, MODEL, WIDTH),
        grad_down[None],
    )


def solution(mesh):
    fine = Mesh(mesh.devices.reshape(8, 4, 8, 2), ("z", "x", "y", "core"))
    sp, tp = ("z", "x"), ("y", "core")
    in_specs = (
        P(tp, sp),
        P(tp, sp),
        P(tp, sp),
        P(tp, sp),
        P(tp, sp),
        P(tp),
        P(None, tp),
        P(sp, tp),
        P(sp, None),
        P(sp, None),
        P(sp, tp),
        P(sp, None, tp),
        P(sp, None, tp),
        P(sp, tp, None),
    )
    out_specs = (
        P(tp, sp),
        P(tp, sp),
        P(tp, sp),
        P(tp, sp),
        P(sp, tp),
        P(sp, None, tp),
        P(sp, None, tp),
        P(sp, tp, None),
    )

    return jax.shard_map(body, mesh=fine, in_specs=in_specs, out_specs=out_specs, check_vma=False)
```

```python
import jax
import jax.numpy as jnp
from jax import lax
from jax.experimental import pallas as pl
from jax.experimental.pallas import tpu as pltpu
from jax.sharding import Mesh
from jax.sharding import PartitionSpec as P


KEY_DIM = 32
VAL_DIM = 64
TOK = 128
PEERS = 32
CAP = 12
PAD = 16
RING = 8
SLOTS = PEERS * PAD
ROWS = PEERS * CAP
WIDTH = 128
MODEL = 2048

F32 = jnp.float32
BF16 = jnp.bfloat16
EXACT = lax.Precision.HIGHEST


def dot(a, b, da, db, precision=None):
    return lax.dot_general(
        a, b, (((da,), (db,)), ((), ())), preferred_element_type=F32, precision=precision
    )


def iota(shape, dim):
    return lax.broadcasted_iota(jnp.int32, shape, dim)


def ones_where(mask, dtype=BF16):
    return jnp.where(mask, 1.0, 0.0).astype(dtype)


def split_two(value):
    high = value.astype(BF16).astype(F32)
    return high, (value - high).astype(BF16).astype(F32)


def split_three(value):
    high, rest = split_two(value)
    return high, rest, (value - high - rest).astype(BF16).astype(F32)


def compact_rows(shape, compact_dim):
    row = iota(shape, compact_dim)
    peer = (row * 5462) >> 16
    return peer * PAD + (row - peer * CAP) == iota(shape, 1 - compact_dim)


def row_of_peer(place):
    return iota((PEERS, SLOTS), 1) == iota((PEERS, SLOTS), 0) * PAD + place


def dispatch_kernel(
    ids_ref, share_ref, x_ref, cot_ref, key_ref, val_ref, pre_ref, extra_ref, speed_ref,
    send_ref, pick_ref, cum_ref,
):
    expert = iota((PEERS, TOK), 0)
    named = [ids_ref[k : k + 1, :] == expert for k in range(2)]
    row, col = iota((TOK, TOK), 0), iota((TOK, TOK), 1)
    rank = dot(ones_where(named[0] | named[1]), ones_where(row < col), 1, 0)
    place = iota((PEERS, PAD, TOK), 1).astype(F32)
    cot = cot_ref[...].astype(F32)
    picks, grads = [], None
    for k in range(2):
        at = jnp.where(named[k], rank, -1.0)
        pick = jnp.where(at[:, None, :] == place, 1.0, 0.0).reshape(SLOTS, TOK).astype(BF16)
        share = jnp.sum(jnp.where(row == col, share_ref[k : k + 1, :], 0.0), axis=1, keepdims=True)
        part = dot(pick, (share * cot).astype(BF16), 1, 0)
        grads = part if grads is None else grads + part
        picks.append(pick)
    pick = picks[0] + picks[1]
    pick_ref[...] = pick
    rows = jnp.concatenate([dot(pick, x_ref[...], 1, 0), grads], axis=1)

    pre = pre_ref[...].astype(F32)
    log_sig = jnp.minimum(pre, 0.0) - jnp.log1p(jnp.exp(-jnp.abs(pre)))
    diagonal = iota((KEY_DIM, KEY_DIM), 0) == iota((KEY_DIM, KEY_DIM), 1)
    speed = jnp.sum(jnp.where(diagonal, speed_ref[...], 0.0), axis=1, keepdims=True)
    decay = speed * log_sig + extra_ref[...]
    cum = dot(decay, ones_where(row <= col, F32), 1, 0, EXACT)
    cum_ref[...] = cum
    total = cum[:, TOK - 1 : TOK]
    keys, vals = key_ref[...].astype(F32), val_ref[...].astype(F32)
    sums = jnp.concatenate(
        [
            dot(keys * jnp.exp(total - cum), vals, 1, 1, EXACT),
            dot(keys * jnp.exp(cum), vals, 1, 1, EXACT),
        ],
        axis=1,
    )
    state = jnp.concatenate(split_two(sums), axis=1)
    lane = iota((KEY_DIM, 2 * WIDTH), 1)
    logs = jnp.zeros((KEY_DIM, 2 * WIDTH), F32)
    for k, part in enumerate(split_three(total)):
        logs = jnp.where(lane == k, part, logs)
    place = iota((PEERS, PAD, 2 * WIDTH), 1)
    block = rows.reshape(PEERS, PAD, 2 * WIDTH)
    block = jnp.where(place == CAP, state[:, None, :], block)
    block = jnp.where(place == CAP + 1, logs[:, None, :], block)
    send_ref[...] = block.astype(BF16)


def arrival_kernel(got_ref, rows_ref, back_ref):
    got = got_ref[...].reshape(SLOTS, 2 * WIDTH)
    rows_ref[...] = dot(ones_where(compact_rows((ROWS, SLOTS), 0)), got, 1, 0).astype(BF16)
    both = dot(ones_where(row_of_peer(CAP)), got, 1, 0)
    state = both[:, :WIDTH] + both[:, WIDTH:]
    logs = dot(ones_where(row_of_peer(CAP + 1)), got, 1, 0)
    log = jnp.sum(logs, axis=1, keepdims=True)
    a, b = iota((PEERS, PEERS), 0), iota((PEERS, PEERS), 1)
    gap_fwd = dot(ones_where(b < a, F32), jnp.where(a > b, log, 0.0), 1, 0, EXACT)
    gap_bwd = dot(ones_where(b > a, F32), jnp.where(a < b, log, 0.0), 1, 0, EXACT)
    fwd = dot(jnp.where(b < a, jnp.exp(gap_fwd), 0.0), state, 1, 0, EXACT)
    bwd = dot(jnp.where(b > a, jnp.exp(gap_bwd), 0.0), state, 1, 0, EXACT)
    lane = iota((PEERS, WIDTH), 1)
    high, low = split_two(jnp.where(lane < VAL_DIM, fwd, bwd))
    peer = iota((PEERS, WIDTH), 0)
    spread = jnp.zeros((PEERS, WIDTH), F32)
    for k, part in enumerate(split_three(log)):
        spread = jnp.where(lane == peer + k * PEERS, part, spread)
    all_logs = jnp.sum(spread, axis=0, keepdims=True)
    place = iota((PEERS, PAD, WIDTH), 1)
    block = jnp.where(place == CAP, high[:, None, :], 0.0)
    block = jnp.where(place == CAP + 1, low[:, None, :], block)
    block = jnp.where(place == CAP + 2, all_logs[:, None, :], block)
    back_ref[...] = block.astype(BF16)


def slice_kernel(
    core_ref, place_ref, ring_ref, gate_ref, up_ref, down_ref, proj_ref, own_ref, out_ref, near_ref
):
    near_ref[...] = proj_ref[...]
    core = core_ref[0]
    for side, ref in ((core, own_ref), (1 - core, out_ref)):
        for k in range(RING):
            at = 2 * k + side
            ref[0, k] = gate_ref[at]
            ref[1, k] = up_ref[at]
            ref[2, k] = down_ref[:, pl.ds(pl.multiple_of(at * WIDTH, WIDTH), WIDTH)]


def sender(here, distance):
    return lax.rem(here + RING - distance, RING)


def forward_kernel(here_ref, *refs):
    rows, (own_ref, swapped_ref, out_ref, send_ref) = refs[:RING], refs[RING:]
    here = here_ref[0]
    pre = jnp.zeros((ROWS, 4 * WIDTH), F32)
    grad = jnp.zeros((ROWS, 2 * WIDTH), F32)
    for k in range(0, RING, 2):
        weights, downs = [], []
        for j in (sender(here, k), sender(here, k + 1)):
            parts = [own_ref[0, j], own_ref[1, j], swapped_ref[0, j], swapped_ref[1, j]]
            weights.append(jnp.concatenate(parts, axis=1))
            downs.append(jnp.concatenate([own_ref[2, j], swapped_ref[2, j]], axis=0))
        x = jnp.concatenate([rows[k][:, :WIDTH], rows[k + 1][:, :WIDTH]], axis=1)
        y = jnp.concatenate([rows[k][:, WIDTH:], rows[k + 1][:, WIDTH:]], axis=1)
        pre = pre + dot(x, jnp.concatenate(weights, axis=0), 1, 0)
        grad = grad + dot(y, jnp.concatenate(downs, axis=1), 1, 1)
    mine = jnp.concatenate([pre[:, : 2 * WIDTH], grad[:, :WIDTH]], axis=1)
    theirs = jnp.concatenate([pre[:, 2 * WIDTH :], grad[:, WIDTH:]], axis=1)
    out_ref[0] = mine
    out_ref[1] = theirs
    send_ref[0] = theirs.astype(BF16)
    send_ref[1] = mine.astype(BF16)


def partial_kernel(
    own_ref, got_ref, kept_ref, swapped_ref, out_ref, grads_ref, hidden_ref
):
    grads = []
    for half in range(2):
        total = own_ref[half] + got_ref[half].astype(F32)
        gate_pre, up_pre = total[:, :WIDTH], total[:, WIDTH : 2 * WIDTH]
        grad_hidden = total[:, 2 * WIDTH :]
        gate_sig = jax.nn.sigmoid(gate_pre)
        gate_act = gate_pre * gate_sig
        hidden_ref[:, half * WIDTH : (half + 1) * WIDTH] = (gate_act * up_pre).astype(BF16)
        slope = gate_sig * (1.0 + gate_pre * (1.0 - gate_sig))
        grads.append((grad_hidden * up_pre * slope).astype(BF16))
        grads.append((grad_hidden * gate_act).astype(BF16))
    grads = jnp.concatenate(grads, axis=1)
    grads_ref[...] = grads
    for k in range(RING):
        weights = jnp.concatenate(
            [kept_ref[0, k], kept_ref[1, k], swapped_ref[0, k], swapped_ref[1, k]], axis=1
        )
        out_ref[k] = dot(grads, weights, 1, 1).astype(BF16)


def weight_kernel(here_ref, *refs):
    rows, (grads_ref, hidden_ref, own_ref, send_ref) = refs[:RING], refs[RING:]
    grads, hidden = grads_ref[...], hidden_ref[...]
    for k in range(RING):
        j = sender(here_ref[0], k)
        both = dot(rows[k][:, :WIDTH], grads, 0, 0).astype(BF16)
        down = dot(hidden, rows[k][:, WIDTH:], 0, 0).astype(BF16)
        for half, ref in enumerate((own_ref, send_ref)):
            at = 2 * half * WIDTH
            ref[0, j] = both[:, at : at + WIDTH]
            ref[1, j] = both[:, at + WIDTH : at + 2 * WIDTH]
            ref[2, j] = down[half * WIDTH : (half + 1) * WIDTH]


def joined_kernel(core_ref, own_ref, got_ref, gate_ref, up_ref, down_ref):
    core = core_ref[0]
    for k in range(RING):
        for side, ref in ((core, own_ref), (1 - core, got_ref)):
            at = 2 * k + side
            gate_ref[at] = ref[0, k]
            up_ref[at] = ref[1, k]
            down_ref[:, pl.ds(pl.multiple_of(at * WIDTH, WIDTH), WIDTH)] = ref[2, k]


def return_kernel(parts_ref, back_ref, send_ref):
    total = parts_ref[0].astype(F32)
    for k in range(1, RING):
        total = total + parts_ref[k].astype(F32)
    rows = dot(ones_where(compact_rows((SLOTS, ROWS), 1)), total.astype(BF16), 1, 0)
    rows = rows.astype(BF16).reshape(PEERS, PAD, WIDTH)
    send_ref[...] = rows + back_ref[...]


def token_kernel(got_ref, pick_ref, cot_ref, copies_ref):
    got = got_ref[...].reshape(SLOTS, WIDTH)
    rows = (cot_ref[...].astype(F32) + dot(pick_ref[...], got, 0, 0)).astype(BF16)
    for k in range(RING):
        copies_ref[k] = rows


def state_kernel(place_ref, got_ref, state_ref, reach_ref):
    got = got_ref[...].reshape(SLOTS, WIDTH)
    state_ref[...] = dot(ones_where(row_of_peer(CAP) | row_of_peer(CAP + 1)), got, 1, 0)
    spread = dot(ones_where(row_of_peer(CAP + 2)), got, 1, 0).astype(BF16)
    lane, peer = iota((WIDTH, PEERS), 0), iota((WIDTH, PEERS), 1)
    fold = (lane == peer) | (lane == peer + PEERS) | (lane == peer + 2 * PEERS)
    logs = dot(spread, ones_where(fold), 1, 0)
    here = place_ref[0]
    a, b = iota((PEERS, PEERS), 0), iota((PEERS, PEERS), 1)
    later = dot(jnp.where(b > here, logs, 0.0), ones_where(a < b, F32), 1, 0, EXACT)
    before = dot(jnp.where(b < here, logs, 0.0), ones_where(a > b, F32), 1, 0, EXACT)
    later = jnp.where(b > here, jnp.exp(later), 0.0)
    before = jnp.where(b < here, jnp.exp(before), 0.0)
    half = KEY_DIM // 2
    first = iota((half, WIDTH), 1) < VAL_DIM
    for k in range(PEERS):
        for side, value in enumerate((later, before)):
            column = value[:, k : k + 1]
            reach_ref[side, k] = jnp.where(first, column[:half], column[half:])


def source_kernel(
    place_ref, rows_ref, weight_ref, normed_ref, inv_ref, mix_ref, query_fwd_ref, query_bwd_ref,
    send_ref, grad_ref, proj_ref, state_ref, sems,
):
    here = place_ref[0]
    rows = jnp.concatenate([rows_ref[c, k] for k in range(RING) for c in range(2)], axis=1)
    lane = iota((KEY_DIM, WIDTH), 1)
    for k in range(2 * RING):
        part = dot(rows[:, k * WIDTH : (k + 1) * WIDTH], mix_ref[...], 0, 0)
        for side in range(2):
            at = side * VAL_DIM
            both = jnp.where(lane < VAL_DIM, part[at : at + 32], part[at + 32 : at + 64])
            proj_ref[2 * k + side] = both.astype(BF16)
    first_part = pltpu.make_async_copy(proj_ref, send_ref.at[:, :KEY_DIM], sems.at[0])
    first_part.start()
    grad = dot(rows, weight_ref[...], 1, 1)
    normed = normed_ref[...]
    mean = jnp.mean(grad * normed, axis=1, keepdims=True)
    grad = inv_ref[...] * (grad - normed * mean)
    grad_ref[...] = grad
    twice = jnp.concatenate([grad, grad], axis=1)
    half = KEY_DIM // 2
    first = iota((half, WIDTH), 1) < VAL_DIM
    states = []
    for ref in (query_fwd_ref, query_bwd_ref):
        state = dot(ref[...], twice, 1, 0, EXACT)
        states.append(jnp.where(first, state[:half], state[half:]))
    for peer in range(PEERS):
        state_ref[peer] = jnp.where(peer < here, states[0], states[1]).astype(BF16)
    second_part = pltpu.make_async_copy(state_ref, send_ref.at[:, KEY_DIM:], sems.at[1])
    second_part.start()
    first_part.wait()
    second_part.wait()


def final_kernel(
    got_ref, reach_ref, state_ref, cum_ref, key_ref, val_ref, pre_ref, speed_ref,
    keys_mix_ref, vals_mix_ref, decay_mix_ref,
    proj_ref, keys_ref, vals_ref, logit_ref,
):
    proj = got_ref[0, :KEY_DIM].astype(F32)
    flow = got_ref[0, KEY_DIM:].astype(F32)
    packed = [flow * reach_ref[0, 0], flow * reach_ref[1, 0]]
    for k in range(1, PEERS):
        proj = proj + got_ref[k, :KEY_DIM].astype(F32)
        flow = got_ref[k, KEY_DIM:].astype(F32)
        packed = [total + flow * reach_ref[side, k] for side, total in enumerate(packed)]
    flow_fwd, flow_bwd = (
        jnp.concatenate([total[:, :VAL_DIM], total[:, VAL_DIM:]], axis=0) for total in packed
    )
    proj_ref[:KEY_DIM] = proj[:, :VAL_DIM]
    proj_ref[KEY_DIM:] = proj[:, VAL_DIM:]
    cum = cum_ref[...]
    total = cum[:, TOK - 1 : TOK]
    keys, vals = key_ref[...].astype(F32), val_ref[...].astype(F32)
    scale_fwd, scale_bwd = jnp.exp(total - cum), jnp.exp(cum)
    grad_fwd = dot(flow_fwd, vals, 1, 0, EXACT) * scale_fwd
    grad_bwd = dot(flow_bwd, vals, 1, 0, EXACT) * scale_bwd
    keys_ref[...] = keys_mix_ref[...] + grad_fwd + grad_bwd
    vals_ref[...] = (
        vals_mix_ref[...]
        + dot(flow_fwd, keys * scale_fwd, 0, 0, EXACT)
        + dot(flow_bwd, keys * scale_bwd, 0, 0, EXACT)
    )
    state = state_ref[...]
    flow = flow_fwd * state[:, :VAL_DIM] + flow_bwd * state[:, VAL_DIM:]
    factor = jnp.exp(total) * jnp.sum(flow, axis=1, keepdims=True)
    grad_fwd, grad_bwd = grad_fwd * keys, grad_bwd * keys
    at_end = factor + jnp.sum(grad_fwd, axis=1, keepdims=True)
    row, col = iota((TOK, TOK), 0), iota((TOK, TOK), 1)
    tail = dot(grad_bwd - grad_fwd, ones_where(row >= col, F32), 1, 0, EXACT)
    decay = decay_mix_ref[...] + tail + at_end
    diagonal = iota((KEY_DIM, KEY_DIM), 0) == iota((KEY_DIM, KEY_DIM), 1)
    speed = jnp.sum(jnp.where(diagonal, speed_ref[...], 0.0), axis=1, keepdims=True)
    pre = pre_ref[...].astype(F32)
    logit_ref[...] = decay * speed * jax.nn.sigmoid(-pre)


SCALAR = pl.BlockSpec(memory_space=pltpu.SMEM)
WHOLE = pl.BlockSpec(memory_space=pltpu.VMEM)
OUTSIDE = pl.BlockSpec(memory_space=pltpu.HBM)


def on_chip(array):
    return pltpu.with_memory_space_constraint(array, pltpu.VMEM)


def off_chip(array):
    return pltpu.with_memory_space_constraint(array, pltpu.HBM)


def call(kernel, outs, *args, scalars=0, stored=(), manual=(), scratch=()):
    shapes = [
        (pltpu.HBM if k in stored else pltpu.VMEM)(shape, dtype)
        for k, (shape, dtype) in enumerate(outs)
    ]
    return pl.pallas_call(
        kernel,
        out_shape=shapes,
        in_specs=[SCALAR] * scalars + [WHOLE] * (len(args) - scalars),
        out_specs=[OUTSIDE if k in manual else WHOLE for k in range(len(shapes))],
        scratch_shapes=list(scratch),
        compiler_params=pltpu.CompilerParams(vmem_limit_bytes=24 << 20),
    )(*args)


def inner(scaled, keys, vals, cum, lower):
    gap = cum[:, :, None] - cum[:, None, :]
    weight = jnp.exp(jnp.where(lower, gap, -gap))
    scores = jnp.einsum("ct,cs,cts->ts", scaled, keys, weight)
    return jnp.einsum("ts,vs->vt", scores, vals)


def carried(scaled, cum, fwd_in, bwd_in):
    total = cum[:, -1:]
    return jnp.einsum("ct,cv->vt", scaled * jnp.exp(cum), fwd_in) + jnp.einsum(
        "ct,cv->vt", scaled * jnp.exp(total - cum), bwd_in
    )


def body(
    queries,
    input_key_matrix,
    input_value_matrix,
    decay_preactivation,
    extra_log_decay,
    channel_decay_speed,
    output_weight_matrix,
    stored_expert_rows,
    chosen_expert_index,
    expert_combine_weight,
    cotangent,
    expert_gate_weight,
    expert_up_weight,
    expert_down_weight,
):
    sp = ("z", "x")
    core = lax.axis_index("core")
    core_at = core.reshape(1).astype(jnp.int32)
    place_at = lax.axis_index(sp).reshape(1).astype(jnp.int32)
    ring_at = lax.axis_index("y").reshape(1).astype(jnp.int32)
    speed = channel_decay_speed.reshape(1, KEY_DIM)
    swap = [(0, 1), (1, 0)]

    def exchanged(array, axis):
        return lax.all_to_all(array, axis, split_axis=0, concat_axis=0, tiled=True)

    gate, up, down = expert_gate_weight[0], expert_up_weight[0], expert_down_weight[0]
    gate_blocks = gate.reshape(2 * RING, WIDTH, WIDTH)
    up_blocks = up.reshape(2 * RING, WIDTH, WIDTH)
    send, pick, cum = call(
        dispatch_kernel,
        [((PEERS, PAD, 2 * WIDTH), BF16), ((SLOTS, TOK), BF16), ((KEY_DIM, TOK), F32)],
        off_chip(chosen_expert_index.T),
        off_chip(expert_combine_weight.T),
        off_chip(stored_expert_rows),
        off_chip(cotangent),
        off_chip(input_key_matrix),
        off_chip(input_value_matrix),
        off_chip(decay_preactivation),
        off_chip(extra_log_decay),
        off_chip(speed),
        stored=(1,),
    )
    got = exchanged(send, sp)
    kept, theirs, proj = call(
        slice_kernel,
        [((3, RING, WIDTH, WIDTH), BF16)] * 2 + [((VAL_DIM, MODEL), BF16)],
        core_at,
        place_at,
        ring_at,
        off_chip(gate_blocks),
        off_chip(up_blocks),
        off_chip(down),
        off_chip(output_weight_matrix.T),
        scalars=3,
        stored=(1,),
    )
    swapped = lax.ppermute(theirs, "core", swap)
    rows, back = call(
        arrival_kernel,
        [((ROWS, 2 * WIDTH), BF16), ((PEERS, PAD, WIDTH), BF16)],
        on_chip(got),
        stored=(1,),
    )
    shards = {0: rows}
    for distance in (4, 3, 5, 2, 6, 1, 7):
        shards[distance] = lax.ppermute(
            rows, "y", [(k, (k + distance) % RING) for k in range(RING)]
        )
    shards = [on_chip(shards[distance]) for distance in range(RING)]
    own, send = call(
        forward_kernel,
        [((2, ROWS, 3 * WIDTH), F32), ((2, ROWS, 3 * WIDTH), BF16)],
        ring_at,
        *shards,
        on_chip(kept),
        swapped,
        scalars=1,
    )
    crossed = lax.ppermute(send, "core", swap)
    partials, grads, hidden = call(
        partial_kernel,
        [
            ((RING, ROWS, WIDTH), BF16),
            ((ROWS, 4 * WIDTH), BF16),
            ((ROWS, 2 * WIDTH), BF16),
        ],
        on_chip(own),
        on_chip(crossed),
        on_chip(kept),
        swapped,
    )
    parts = exchanged(partials, "y")
    (send,) = call(
        return_kernel, [((PEERS, PAD, WIDTH), BF16)], on_chip(parts), on_chip(back)
    )
    returned = on_chip(exchanged(send, sp))
    (copies,) = call(
        token_kernel,
        [((RING, TOK, WIDTH), BF16)],
        returned,
        on_chip(pick),
        cotangent,
        stored=(0,),
    )
    row = iota((TOK, TOK), 0)
    cum, queries, key_in, val_in, row, copies = lax.optimization_barrier(
        (cum, queries, input_key_matrix, input_value_matrix, row, copies)
    )
    full_rows = exchanged(copies, "y")
    full_rows = lax.all_gather(full_rows, "core", axis=0, tiled=False)

    state, reach = call(
        state_kernel,
        [((KEY_DIM, WIDTH), F32), ((2, PEERS, KEY_DIM // 2, WIDTH), F32)],
        place_at,
        returned,
        scalars=1,
    )
    scaled = queries.astype(F32) * KEY_DIM ** (-0.5)
    keys = key_in.astype(F32)
    vals = val_in.astype(F32)
    lower = row >= iota((TOK, TOK), 1)
    fwd_in, bwd_in = state[:, :VAL_DIM], state[:, VAL_DIM:]
    inner_out, pull_inner = jax.vjp(
        lambda *args: inner(*args, lower), scaled, keys, vals, cum
    )
    carried_out, pull_carried = jax.vjp(
        lambda s, c: carried(s, c, fwd_in, bwd_in), scaled, cum
    )
    mixed = inner_out + carried_out
    inv_rms = lax.rsqrt(jnp.mean(mixed * mixed, axis=0, keepdims=True) + 1e-06)
    normed = mixed * inv_rms
    normed_t = normed.T
    mix_t = normed_t.astype(BF16)
    mix_twice = jnp.concatenate([mix_t, mix_t], axis=1)
    query_fwd = scaled * jnp.exp(cum)
    query_bwd = scaled * jnp.exp(cum[:, -1:] - cum)
    send, grad_mixed_t = call(
        source_kernel,
        [((PEERS, 3 * KEY_DIM // 2, WIDTH), BF16), ((TOK, VAL_DIM), F32)],
        place_at,
        on_chip(full_rows),
        on_chip(proj),
        normed_t,
        inv_rms.reshape(TOK, 1),
        mix_twice,
        query_fwd,
        query_bwd,
        scalars=1,
        stored=(0,),
        manual=(0,),
        scratch=(
            pltpu.VMEM((PEERS, KEY_DIM, WIDTH), BF16),
            pltpu.VMEM((PEERS, KEY_DIM // 2, WIDTH), BF16),
            pltpu.SemaphoreType.DMA((2,)),
        ),
    )
    got = exchanged(send, sp)
    own, send = call(
        weight_kernel,
        [((3, RING, WIDTH, WIDTH), BF16)] * 2,
        ring_at,
        *shards,
        on_chip(grads),
        on_chip(hidden),
        scalars=1,
    )
    crossed = lax.ppermute(send, "core", swap)
    grad_gate, grad_up, grad_down = call(
        joined_kernel,
        [
            ((2 * RING, WIDTH, WIDTH), BF16),
            ((2 * RING, WIDTH, WIDTH), BF16),
            ((WIDTH, MODEL), BF16),
        ],
        core_at,
        on_chip(own),
        on_chip(crossed),
        scalars=1,
        stored=range(3),
    )
    grad_mixed = grad_mixed_t.T
    grad_scaled, grad_keys, grad_vals, grad_cum = pull_inner(grad_mixed)
    grad_scaled_in, grad_cum_in = pull_carried(grad_mixed)
    grad_queries = (grad_scaled + grad_scaled_in) * KEY_DIM ** (-0.5)
    tail_mask = ones_where(iota((TOK, TOK), 0) >= iota((TOK, TOK), 1), F32)
    grad_decay = dot(grad_cum + grad_cum_in, tail_mask, 1, 0, EXACT)
    grad_out_proj, grad_keys, grad_values, grad_logit = call(
        final_kernel,
        [
            ((2 * KEY_DIM, VAL_DIM), F32),
            ((KEY_DIM, TOK), F32),
            ((VAL_DIM, TOK), F32),
            ((KEY_DIM, TOK), F32),
        ],
        on_chip(got),
        reach,
        state,
        cum,
        input_key_matrix,
        input_value_matrix,
        decay_preactivation,
        speed,
        grad_keys,
        grad_vals,
        grad_decay,
        stored=range(4),
    )
    return (
        grad_queries,
        grad_keys,
        grad_values,
        grad_logit,
        grad_out_proj,
        grad_gate.reshape(1, MODEL, WIDTH),
        grad_up.reshape(1, MODEL, WIDTH),
        grad_down[None],
    )


def solution(mesh):
    fine = Mesh(mesh.devices.reshape(8, 4, 8, 2), ("z", "x", "y", "core"))
    sp, tp = ("z", "x"), ("y", "core")
    in_specs = (
        P(tp, sp),
        P(tp, sp),
        P(tp, sp),
        P(tp, sp),
        P(tp, sp),
        P(tp),
        P(None, tp),
        P(sp, tp),
        P(sp, None),
        P(sp, None),
        P(sp, tp),
        P(sp, None, tp),
        P(sp, None, tp),
        P(sp, tp, None),
    )
    out_specs = (
        P(tp, sp),
        P(tp, sp),
        P(tp, sp),
        P(tp, sp),
        P(sp, tp),
        P(sp, None, tp),
        P(sp, None, tp),
        P(sp, tp, None),
    )

    return jax.shard_map(
        body, mesh=fine, in_specs=in_specs, out_specs=out_specs, check_vma=False
    )
```

```python
import jax
import jax.numpy as jnp
from jax import lax
from jax.experimental import pallas as pl
from jax.experimental.pallas import tpu as pltpu
from jax.sharding import Mesh
from jax.sharding import PartitionSpec as P


KEY_DIM = 32
VAL_DIM = 64
TOK = 128
PEERS = 32
CAP = 12
PAD = 16
RING = 8
SLOTS = PEERS * PAD
ROWS = PEERS * CAP
WIDTH = 128
MODEL = 2048

F32 = jnp.float32
BF16 = jnp.bfloat16
EXACT = lax.Precision.HIGHEST


def dot(a, b, da, db, precision=None):
    return lax.dot_general(
        a, b, (((da,), (db,)), ((), ())), preferred_element_type=F32, precision=precision
    )


def iota(shape, dim):
    return lax.broadcasted_iota(jnp.int32, shape, dim)


def ones_where(mask, dtype=BF16):
    return jnp.where(mask, 1.0, 0.0).astype(dtype)


def split_two(value):
    high = value.astype(BF16).astype(F32)
    return high, (value - high).astype(BF16).astype(F32)


def split_three(value):
    high, rest = split_two(value)
    return high, rest, (value - high - rest).astype(BF16).astype(F32)


def compact_rows(shape, compact_dim):
    row = iota(shape, compact_dim)
    peer = (row * 5462) >> 16
    return peer * PAD + (row - peer * CAP) == iota(shape, 1 - compact_dim)


def row_of_peer(place):
    return iota((PEERS, SLOTS), 1) == iota((PEERS, SLOTS), 0) * PAD + place


def dispatch_kernel(
    ids_ref, share_ref, x_ref, cot_ref, key_ref, val_ref, pre_ref, extra_ref, speed_ref,
    send_ref, pick_ref, cum_ref,
):
    expert = iota((PEERS, TOK), 0)
    named = [ids_ref[k : k + 1, :] == expert for k in range(2)]
    row, col = iota((TOK, TOK), 0), iota((TOK, TOK), 1)
    rank = dot(ones_where(named[0] | named[1]), ones_where(row < col), 1, 0)
    place = iota((PEERS, PAD, TOK), 1).astype(F32)
    cot = cot_ref[...].astype(F32)
    picks, grads = [], None
    for k in range(2):
        at = jnp.where(named[k], rank, -1.0)
        pick = jnp.where(at[:, None, :] == place, 1.0, 0.0).reshape(SLOTS, TOK).astype(BF16)
        share = jnp.sum(jnp.where(row == col, share_ref[k : k + 1, :], 0.0), axis=1, keepdims=True)
        part = dot(pick, (share * cot).astype(BF16), 1, 0)
        grads = part if grads is None else grads + part
        picks.append(pick)
    pick = picks[0] + picks[1]
    pick_ref[...] = pick
    rows = jnp.concatenate([dot(pick, x_ref[...], 1, 0), grads], axis=1)

    pre = pre_ref[...].astype(F32)
    log_sig = jnp.minimum(pre, 0.0) - jnp.log1p(jnp.exp(-jnp.abs(pre)))
    diagonal = iota((KEY_DIM, KEY_DIM), 0) == iota((KEY_DIM, KEY_DIM), 1)
    speed = jnp.sum(jnp.where(diagonal, speed_ref[...], 0.0), axis=1, keepdims=True)
    decay = speed * log_sig + extra_ref[...]
    cum = dot(decay, ones_where(row <= col, F32), 1, 0, EXACT)
    cum_ref[...] = cum
    total = cum[:, TOK - 1 : TOK]
    keys, vals = key_ref[...].astype(F32), val_ref[...].astype(F32)
    sums = jnp.concatenate(
        [
            dot(keys * jnp.exp(total - cum), vals, 1, 1, EXACT),
            dot(keys * jnp.exp(cum), vals, 1, 1, EXACT),
        ],
        axis=1,
    )
    state = jnp.concatenate(split_two(sums), axis=1)
    lane = iota((KEY_DIM, 2 * WIDTH), 1)
    logs = jnp.zeros((KEY_DIM, 2 * WIDTH), F32)
    for k, part in enumerate(split_three(total)):
        logs = jnp.where(lane == k, part, logs)
    place = iota((PEERS, PAD, 2 * WIDTH), 1)
    block = rows.reshape(PEERS, PAD, 2 * WIDTH)
    block = jnp.where(place == CAP, state[:, None, :], block)
    block = jnp.where(place == CAP + 1, logs[:, None, :], block)
    send_ref[...] = block.astype(BF16)


def arrival_kernel(got_ref, copies_ref, back_ref):
    got = got_ref[...].reshape(SLOTS, 2 * WIDTH)
    rows = dot(ones_where(compact_rows((ROWS, SLOTS), 0)), got, 1, 0).astype(BF16)
    for k in range(RING):
        copies_ref[k] = rows
    both = dot(ones_where(row_of_peer(CAP)), got, 1, 0)
    state = both[:, :WIDTH] + both[:, WIDTH:]
    logs = dot(ones_where(row_of_peer(CAP + 1)), got, 1, 0)
    log = jnp.sum(logs, axis=1, keepdims=True)
    a, b = iota((PEERS, PEERS), 0), iota((PEERS, PEERS), 1)
    gap_fwd = dot(ones_where(b < a, F32), jnp.where(a > b, log, 0.0), 1, 0, EXACT)
    gap_bwd = dot(ones_where(b > a, F32), jnp.where(a < b, log, 0.0), 1, 0, EXACT)
    fwd = dot(jnp.where(b < a, jnp.exp(gap_fwd), 0.0), state, 1, 0, EXACT)
    bwd = dot(jnp.where(b > a, jnp.exp(gap_bwd), 0.0), state, 1, 0, EXACT)
    lane = iota((PEERS, WIDTH), 1)
    high, low = split_two(jnp.where(lane < VAL_DIM, fwd, bwd))
    peer = iota((PEERS, WIDTH), 0)
    spread = jnp.zeros((PEERS, WIDTH), F32)
    for k, part in enumerate(split_three(log)):
        spread = jnp.where(lane == peer + k * PEERS, part, spread)
    all_logs = jnp.sum(spread, axis=0, keepdims=True)
    place = iota((PEERS, PAD, WIDTH), 1)
    block = jnp.where(place == CAP, high[:, None, :], 0.0)
    block = jnp.where(place == CAP + 1, low[:, None, :], block)
    block = jnp.where(place == CAP + 2, all_logs[:, None, :], block)
    back_ref[...] = block.astype(BF16)


def slice_kernel(
    core_ref, place_ref, gate_ref, up_ref, down_ref, proj_ref, own_ref, out_ref, near_ref
):
    near_ref[...] = proj_ref[...]
    core = core_ref[0]
    for side, ref in ((core, own_ref), (1 - core, out_ref)):
        for k in range(RING):
            at = 2 * k + side
            ref[0, k] = gate_ref[at]
            ref[1, k] = up_ref[at]
            ref[2, k] = down_ref[:, pl.ds(pl.multiple_of(at * WIDTH, WIDTH), WIDTH)]


def forward_kernel(rows_ref, own_ref, swapped_ref, out_ref, send_ref):
    pre = jnp.zeros((ROWS, 4 * WIDTH), F32)
    grad = jnp.zeros((ROWS, 2 * WIDTH), F32)
    for k in range(0, RING, 2):
        weights, downs = [], []
        for j in (k, k + 1):
            parts = [own_ref[0, j], own_ref[1, j], swapped_ref[0, j], swapped_ref[1, j]]
            weights.append(jnp.concatenate(parts, axis=1))
            downs.append(jnp.concatenate([own_ref[2, j], swapped_ref[2, j]], axis=0))
        x = jnp.concatenate([rows_ref[k, :, :WIDTH], rows_ref[k + 1, :, :WIDTH]], axis=1)
        y = jnp.concatenate([rows_ref[k, :, WIDTH:], rows_ref[k + 1, :, WIDTH:]], axis=1)
        pre = pre + dot(x, jnp.concatenate(weights, axis=0), 1, 0)
        grad = grad + dot(y, jnp.concatenate(downs, axis=1), 1, 1)
    mine = jnp.concatenate([pre[:, : 2 * WIDTH], grad[:, :WIDTH]], axis=1)
    theirs = jnp.concatenate([pre[:, 2 * WIDTH :], grad[:, WIDTH:]], axis=1)
    out_ref[0] = mine
    out_ref[1] = theirs
    send_ref[0] = theirs.astype(BF16)
    send_ref[1] = mine.astype(BF16)


def partial_kernel(
    own_ref, got_ref, kept_ref, swapped_ref, out_ref, grads_ref, hidden_ref
):
    grads = []
    for half in range(2):
        total = own_ref[half] + got_ref[half].astype(F32)
        gate_pre, up_pre = total[:, :WIDTH], total[:, WIDTH : 2 * WIDTH]
        grad_hidden = total[:, 2 * WIDTH :]
        gate_sig = jax.nn.sigmoid(gate_pre)
        gate_act = gate_pre * gate_sig
        hidden_ref[:, half * WIDTH : (half + 1) * WIDTH] = (gate_act * up_pre).astype(BF16)
        slope = gate_sig * (1.0 + gate_pre * (1.0 - gate_sig))
        grads.append((grad_hidden * up_pre * slope).astype(BF16))
        grads.append((grad_hidden * gate_act).astype(BF16))
    grads = jnp.concatenate(grads, axis=1)
    grads_ref[...] = grads
    for k in range(RING):
        weights = jnp.concatenate(
            [kept_ref[0, k], kept_ref[1, k], swapped_ref[0, k], swapped_ref[1, k]], axis=1
        )
        out_ref[k] = dot(grads, weights, 1, 1).astype(BF16)


def weight_kernel(rows_ref, grads_ref, hidden_ref, own_ref, send_ref):
    grads, hidden = grads_ref[...], hidden_ref[...]
    for k in range(RING):
        both = dot(rows_ref[k, :, :WIDTH], grads, 0, 0).astype(BF16)
        down = dot(hidden, rows_ref[k, :, WIDTH:], 0, 0).astype(BF16)
        for half, ref in enumerate((own_ref, send_ref)):
            at = 2 * half * WIDTH
            ref[0, k] = both[:, at : at + WIDTH]
            ref[1, k] = both[:, at + WIDTH : at + 2 * WIDTH]
            ref[2, k] = down[half * WIDTH : (half + 1) * WIDTH]


def joined_kernel(core_ref, own_ref, got_ref, gate_ref, up_ref, down_ref):
    core = core_ref[0]
    for k in range(RING):
        for side, ref in ((core, own_ref), (1 - core, got_ref)):
            at = 2 * k + side
            gate_ref[at] = ref[0, k]
            up_ref[at] = ref[1, k]
            down_ref[:, pl.ds(pl.multiple_of(at * WIDTH, WIDTH), WIDTH)] = ref[2, k]


def return_kernel(parts_ref, back_ref, send_ref):
    total = parts_ref[0].astype(F32)
    for k in range(1, RING):
        total = total + parts_ref[k].astype(F32)
    rows = dot(ones_where(compact_rows((SLOTS, ROWS), 1)), total.astype(BF16), 1, 0)
    rows = rows.astype(BF16).reshape(PEERS, PAD, WIDTH)
    send_ref[...] = rows + back_ref[...]


def token_kernel(got_ref, pick_ref, cot_ref, copies_ref):
    got = got_ref[...].reshape(SLOTS, WIDTH)
    rows = (cot_ref[...].astype(F32) + dot(pick_ref[...], got, 0, 0)).astype(BF16)
    for k in range(RING):
        copies_ref[k] = rows


def state_kernel(place_ref, got_ref, state_ref, reach_ref):
    got = got_ref[...].reshape(SLOTS, WIDTH)
    state_ref[...] = dot(ones_where(row_of_peer(CAP) | row_of_peer(CAP + 1)), got, 1, 0)
    spread = dot(ones_where(row_of_peer(CAP + 2)), got, 1, 0).astype(BF16)
    lane, peer = iota((WIDTH, PEERS), 0), iota((WIDTH, PEERS), 1)
    fold = (lane == peer) | (lane == peer + PEERS) | (lane == peer + 2 * PEERS)
    logs = dot(spread, ones_where(fold), 1, 0)
    here = place_ref[0]
    a, b = iota((PEERS, PEERS), 0), iota((PEERS, PEERS), 1)
    later = dot(jnp.where(b > here, logs, 0.0), ones_where(a < b, F32), 1, 0, EXACT)
    before = dot(jnp.where(b < here, logs, 0.0), ones_where(a > b, F32), 1, 0, EXACT)
    later = jnp.where(b > here, jnp.exp(later), 0.0)
    before = jnp.where(b < here, jnp.exp(before), 0.0)
    half = KEY_DIM // 2
    first = iota((half, WIDTH), 1) < VAL_DIM
    for k in range(PEERS):
        for side, value in enumerate((later, before)):
            column = value[:, k : k + 1]
            reach_ref[side, k] = jnp.where(first, column[:half], column[half:])


def source_kernel(
    place_ref, rows_ref, weight_ref, normed_ref, inv_ref, mix_ref, query_fwd_ref, query_bwd_ref,
    send_ref, grad_ref, proj_ref, state_ref, sems,
):
    here = place_ref[0]
    rows = jnp.concatenate([rows_ref[c, k] for k in range(RING) for c in range(2)], axis=1)
    lane = iota((KEY_DIM, WIDTH), 1)
    for k in range(2 * RING):
        part = dot(rows[:, k * WIDTH : (k + 1) * WIDTH], mix_ref[...], 0, 0)
        for side in range(2):
            at = side * VAL_DIM
            both = jnp.where(lane < VAL_DIM, part[at : at + 32], part[at + 32 : at + 64])
            proj_ref[2 * k + side] = both.astype(BF16)
    first_part = pltpu.make_async_copy(proj_ref, send_ref.at[:, :KEY_DIM], sems.at[0])
    first_part.start()
    grad = dot(rows, weight_ref[...], 1, 1)
    normed = normed_ref[...]
    mean = jnp.mean(grad * normed, axis=1, keepdims=True)
    grad = inv_ref[...] * (grad - normed * mean)
    grad_ref[...] = grad
    twice = jnp.concatenate([grad, grad], axis=1)
    half = KEY_DIM // 2
    first = iota((half, WIDTH), 1) < VAL_DIM
    states = []
    for ref in (query_fwd_ref, query_bwd_ref):
        state = dot(ref[...], twice, 1, 0, EXACT)
        states.append(jnp.where(first, state[:half], state[half:]))
    for peer in range(PEERS):
        state_ref[peer] = jnp.where(peer < here, states[0], states[1]).astype(BF16)
    second_part = pltpu.make_async_copy(state_ref, send_ref.at[:, KEY_DIM:], sems.at[1])
    second_part.start()
    first_part.wait()
    second_part.wait()


def final_kernel(
    got_ref, reach_ref, state_ref, cum_ref, key_ref, val_ref, pre_ref, speed_ref,
    keys_mix_ref, vals_mix_ref, decay_mix_ref,
    proj_ref, keys_ref, vals_ref, logit_ref,
):
    proj = got_ref[0, :KEY_DIM].astype(F32)
    flow = got_ref[0, KEY_DIM:].astype(F32)
    packed = [flow * reach_ref[0, 0], flow * reach_ref[1, 0]]
    for k in range(1, PEERS):
        proj = proj + got_ref[k, :KEY_DIM].astype(F32)
        flow = got_ref[k, KEY_DIM:].astype(F32)
        packed = [total + flow * reach_ref[side, k] for side, total in enumerate(packed)]
    flow_fwd, flow_bwd = (
        jnp.concatenate([total[:, :VAL_DIM], total[:, VAL_DIM:]], axis=0) for total in packed
    )
    proj_ref[:KEY_DIM] = proj[:, :VAL_DIM]
    proj_ref[KEY_DIM:] = proj[:, VAL_DIM:]
    cum = cum_ref[...]
    total = cum[:, TOK - 1 : TOK]
    keys, vals = key_ref[...].astype(F32), val_ref[...].astype(F32)
    scale_fwd, scale_bwd = jnp.exp(total - cum), jnp.exp(cum)
    grad_fwd = dot(flow_fwd, vals, 1, 0, EXACT) * scale_fwd
    grad_bwd = dot(flow_bwd, vals, 1, 0, EXACT) * scale_bwd
    keys_ref[...] = keys_mix_ref[...] + grad_fwd + grad_bwd
    vals_ref[...] = (
        vals_mix_ref[...]
        + dot(flow_fwd, keys * scale_fwd, 0, 0, EXACT)
        + dot(flow_bwd, keys * scale_bwd, 0, 0, EXACT)
    )
    state = state_ref[...]
    flow = flow_fwd * state[:, :VAL_DIM] + flow_bwd * state[:, VAL_DIM:]
    factor = jnp.exp(total) * jnp.sum(flow, axis=1, keepdims=True)
    grad_fwd, grad_bwd = grad_fwd * keys, grad_bwd * keys
    at_end = factor + jnp.sum(grad_fwd, axis=1, keepdims=True)
    row, col = iota((TOK, TOK), 0), iota((TOK, TOK), 1)
    tail = dot(grad_bwd - grad_fwd, ones_where(row >= col, F32), 1, 0, EXACT)
    decay = decay_mix_ref[...] + tail + at_end
    diagonal = iota((KEY_DIM, KEY_DIM), 0) == iota((KEY_DIM, KEY_DIM), 1)
    speed = jnp.sum(jnp.where(diagonal, speed_ref[...], 0.0), axis=1, keepdims=True)
    pre = pre_ref[...].astype(F32)
    logit_ref[...] = decay * speed * jax.nn.sigmoid(-pre)


SCALAR = pl.BlockSpec(memory_space=pltpu.SMEM)
WHOLE = pl.BlockSpec(memory_space=pltpu.VMEM)
OUTSIDE = pl.BlockSpec(memory_space=pltpu.HBM)


def on_chip(array):
    return pltpu.with_memory_space_constraint(array, pltpu.VMEM)


def off_chip(array):
    return pltpu.with_memory_space_constraint(array, pltpu.HBM)


def call(kernel, outs, *args, scalars=0, stored=(), manual=(), scratch=()):
    shapes = [
        (pltpu.HBM if k in stored else pltpu.VMEM)(shape, dtype)
        for k, (shape, dtype) in enumerate(outs)
    ]
    return pl.pallas_call(
        kernel,
        out_shape=shapes,
        in_specs=[SCALAR] * scalars + [WHOLE] * (len(args) - scalars),
        out_specs=[OUTSIDE if k in manual else WHOLE for k in range(len(shapes))],
        scratch_shapes=list(scratch),
        compiler_params=pltpu.CompilerParams(vmem_limit_bytes=24 << 20),
    )(*args)


def inner(scaled, keys, vals, cum, lower):
    gap = cum[:, :, None] - cum[:, None, :]
    weight = jnp.exp(jnp.where(lower, gap, -gap))
    scores = jnp.einsum("ct,cs,cts->ts", scaled, keys, weight)
    return jnp.einsum("ts,vs->vt", scores, vals)


def carried(scaled, cum, fwd_in, bwd_in):
    total = cum[:, -1:]
    return jnp.einsum("ct,cv->vt", scaled * jnp.exp(cum), fwd_in) + jnp.einsum(
        "ct,cv->vt", scaled * jnp.exp(total - cum), bwd_in
    )


def body(
    queries,
    input_key_matrix,
    input_value_matrix,
    decay_preactivation,
    extra_log_decay,
    channel_decay_speed,
    output_weight_matrix,
    stored_expert_rows,
    chosen_expert_index,
    expert_combine_weight,
    cotangent,
    expert_gate_weight,
    expert_up_weight,
    expert_down_weight,
):
    sp = ("z", "x")
    core = lax.axis_index("core")
    core_at = core.reshape(1).astype(jnp.int32)
    place_at = lax.axis_index(sp).reshape(1).astype(jnp.int32)
    speed = channel_decay_speed.reshape(1, KEY_DIM)
    swap = [(0, 1), (1, 0)]

    def exchanged(array, axis):
        return lax.all_to_all(array, axis, split_axis=0, concat_axis=0, tiled=True)

    gate, up, down = expert_gate_weight[0], expert_up_weight[0], expert_down_weight[0]
    gate_blocks = gate.reshape(2 * RING, WIDTH, WIDTH)
    up_blocks = up.reshape(2 * RING, WIDTH, WIDTH)
    send, pick, cum = call(
        dispatch_kernel,
        [((PEERS, PAD, 2 * WIDTH), BF16), ((SLOTS, TOK), BF16), ((KEY_DIM, TOK), F32)],
        off_chip(chosen_expert_index.T),
        off_chip(expert_combine_weight.T),
        off_chip(stored_expert_rows),
        off_chip(cotangent),
        off_chip(input_key_matrix),
        off_chip(input_value_matrix),
        off_chip(decay_preactivation),
        off_chip(extra_log_decay),
        off_chip(speed),
        stored=(1,),
    )
    got = exchanged(send, sp)
    kept, theirs, proj = call(
        slice_kernel,
        [((3, RING, WIDTH, WIDTH), BF16)] * 2 + [((VAL_DIM, MODEL), BF16)],
        core_at,
        place_at,
        off_chip(gate_blocks),
        off_chip(up_blocks),
        off_chip(down),
        off_chip(output_weight_matrix.T),
        scalars=2,
        stored=(1,),
    )
    swapped = lax.ppermute(theirs, "core", swap)
    copies, back = call(
        arrival_kernel,
        [((RING, ROWS, 2 * WIDTH), BF16), ((PEERS, PAD, WIDTH), BF16)],
        on_chip(got),
        stored=(1,),
    )
    rows = exchanged(copies, "y")
    own, send = call(
        forward_kernel,
        [((2, ROWS, 3 * WIDTH), F32), ((2, ROWS, 3 * WIDTH), BF16)],
        rows,
        on_chip(kept),
        swapped,
    )
    crossed = lax.ppermute(send, "core", swap)
    partials, grads, hidden = call(
        partial_kernel,
        [
            ((RING, ROWS, WIDTH), BF16),
            ((ROWS, 4 * WIDTH), BF16),
            ((ROWS, 2 * WIDTH), BF16),
        ],
        on_chip(own),
        on_chip(crossed),
        on_chip(kept),
        swapped,
    )
    parts = exchanged(partials, "y")
    (send,) = call(
        return_kernel, [((PEERS, PAD, WIDTH), BF16)], on_chip(parts), on_chip(back)
    )
    returned = on_chip(exchanged(send, sp))
    (copies,) = call(
        token_kernel,
        [((RING, TOK, WIDTH), BF16)],
        returned,
        on_chip(pick),
        cotangent,
        stored=(0,),
    )
    row = iota((TOK, TOK), 0)
    cum, queries, key_in, val_in, row, copies = lax.optimization_barrier(
        (cum, queries, input_key_matrix, input_value_matrix, row, copies)
    )
    full_rows = exchanged(copies, "y")
    full_rows = lax.all_gather(full_rows, "core", axis=0, tiled=False)

    state, reach = call(
        state_kernel,
        [((KEY_DIM, WIDTH), F32), ((2, PEERS, KEY_DIM // 2, WIDTH), F32)],
        place_at,
        returned,
        scalars=1,
    )
    scaled = queries.astype(F32) * KEY_DIM ** (-0.5)
    keys = key_in.astype(F32)
    vals = val_in.astype(F32)
    lower = row >= iota((TOK, TOK), 1)
    fwd_in, bwd_in = state[:, :VAL_DIM], state[:, VAL_DIM:]
    inner_out, pull_inner = jax.vjp(
        lambda *args: inner(*args, lower), scaled, keys, vals, cum
    )
    carried_out, pull_carried = jax.vjp(
        lambda s, c: carried(s, c, fwd_in, bwd_in), scaled, cum
    )
    mixed = inner_out + carried_out
    inv_rms = lax.rsqrt(jnp.mean(mixed * mixed, axis=0, keepdims=True) + 1e-06)
    normed = mixed * inv_rms
    normed_t = normed.T
    mix_t = normed_t.astype(BF16)
    mix_twice = jnp.concatenate([mix_t, mix_t], axis=1)
    query_fwd = scaled * jnp.exp(cum)
    query_bwd = scaled * jnp.exp(cum[:, -1:] - cum)
    send, grad_mixed_t = call(
        source_kernel,
        [((PEERS, 3 * KEY_DIM // 2, WIDTH), BF16), ((TOK, VAL_DIM), F32)],
        place_at,
        on_chip(full_rows),
        on_chip(proj),
        normed_t,
        inv_rms.reshape(TOK, 1),
        mix_twice,
        query_fwd,
        query_bwd,
        scalars=1,
        stored=(0,),
        manual=(0,),
        scratch=(
            pltpu.VMEM((PEERS, KEY_DIM, WIDTH), BF16),
            pltpu.VMEM((PEERS, KEY_DIM // 2, WIDTH), BF16),
            pltpu.SemaphoreType.DMA((2,)),
        ),
    )
    got = exchanged(send, sp)
    own, send = call(
        weight_kernel,
        [((3, RING, WIDTH, WIDTH), BF16)] * 2,
        on_chip(rows),
        on_chip(grads),
        on_chip(hidden),
    )
    crossed = lax.ppermute(send, "core", swap)
    grad_gate, grad_up, grad_down = call(
        joined_kernel,
        [
            ((2 * RING, WIDTH, WIDTH), BF16),
            ((2 * RING, WIDTH, WIDTH), BF16),
            ((WIDTH, MODEL), BF16),
        ],
        core_at,
        on_chip(own),
        on_chip(crossed),
        scalars=1,
        stored=range(3),
    )
    grad_mixed = grad_mixed_t.T
    grad_scaled, grad_keys, grad_vals, grad_cum = pull_inner(grad_mixed)
    grad_scaled_in, grad_cum_in = pull_carried(grad_mixed)
    grad_queries = (grad_scaled + grad_scaled_in) * KEY_DIM ** (-0.5)
    tail_mask = ones_where(iota((TOK, TOK), 0) >= iota((TOK, TOK), 1), F32)
    grad_decay = dot(grad_cum + grad_cum_in, tail_mask, 1, 0, EXACT)
    grad_out_proj, grad_keys, grad_values, grad_logit = call(
        final_kernel,
        [
            ((2 * KEY_DIM, VAL_DIM), F32),
            ((KEY_DIM, TOK), F32),
            ((VAL_DIM, TOK), F32),
            ((KEY_DIM, TOK), F32),
        ],
        on_chip(got),
        reach,
        state,
        cum,
        input_key_matrix,
        input_value_matrix,
        decay_preactivation,
        speed,
        grad_keys,
        grad_vals,
        grad_decay,
        stored=range(4),
    )
    return (
        grad_queries,
        grad_keys,
        grad_values,
        grad_logit,
        grad_out_proj,
        grad_gate.reshape(1, MODEL, WIDTH),
        grad_up.reshape(1, MODEL, WIDTH),
        grad_down[None],
    )


def solution(mesh):
    fine = Mesh(mesh.devices.reshape(8, 4, 8, 2), ("z", "x", "y", "core"))
    sp, tp = ("z", "x"), ("y", "core")
    in_specs = (
        P(tp, sp),
        P(tp, sp),
        P(tp, sp),
        P(tp, sp),
        P(tp, sp),
        P(tp),
        P(None, tp),
        P(sp, tp),
        P(sp, None),
        P(sp, None),
        P(sp, tp),
        P(sp, None, tp),
        P(sp, None, tp),
        P(sp, tp, None),
    )
    out_specs = (
        P(tp, sp),
        P(tp, sp),
        P(tp, sp),
        P(tp, sp),
        P(sp, tp),
        P(sp, None, tp),
        P(sp, None, tp),
        P(sp, tp, None),
    )

    return jax.shard_map(body, mesh=fine, in_specs=in_specs, out_specs=out_specs, check_vma=False)
```
